32 devices in a mesh: sp: 8 (over z, y), tp: 4 (over x, core).
Axes of the slice: x: 2, y: 2, z: 4, core: 2. Of those that a mesh axis runs over, the one named last changes fastest.
Arguments:
- tokens: bfloat16 [3072, 2048], P('sp', 'tp'), may hold values from -6 to 6
- norm_gain: float32 [3, 2048], replicated, may hold values from 0.1 to 1.9
- w_value: bfloat16 [3, 2048, 1024], P(None, 'sp', 'tp'), may hold values from -0.125 to 0.125
- w_gate: bfloat16 [3, 2048, 1024], P(None, 'sp', 'tp'), may hold values from -0.125 to 0.125
- conv_taps: float32 [3, 31, 1024], P(None, None, 'tp'), may hold values from -2.4 to 2.4
- conv_bias: float32 [3, 1024], P(None, 'tp'), may hold values from -3 to 3
- ln_gain: float32 [3, 1024], P(None, 'tp'), may hold values from 0.1 to 1.9
- ln_shift: float32 [3, 1024], P(None, 'tp'), may hold values from -3 to 3
- w_out: bfloat16 [3, 1024, 2048], P(None, 'tp', 'sp'), may hold values from -0.1875 to 0.1875
Outputs:
- stream: bfloat16 [3072, 2048], P('sp', 'tp')
The draws below stay inside these ranges and needn't reach their ends.
All inputs are finite; a program needn't handle non-finite values.
Results may differ from the reference program's by a relative error of at most 0.015.
Values may be sent and summed in bfloat16 or wider, within the bound.
A program may use at most 64 MiB of HBM per device.

```python
import jax
import jax.numpy as jnp
from jax import lax

D = 2048
CONV_CH = 1024
KERNEL = 31
LAYERS = 3
TOKENS = 3072
N_TP = 4


def draw_conv_taps(key, part):
    first_key, second_key, third_key = jax.random.split(key, 3)
    groups = (CONV_CH + 127) // 128
    group_scale = jnp.exp(jax.random.uniform(second_key, (LAYERS, 1, groups), jnp.float32, -1.0, 1.0))
    group_scale = jnp.repeat(group_scale, 128, axis=2)[:, :, :CONV_CH]
    channel_scale = jnp.exp(jax.random.uniform(third_key, (LAYERS, 1, CONV_CH), jnp.float32, -0.2, 0.2))
    raw_taps = jnp.clip(jax.random.normal(first_key, (LAYERS, KERNEL, CONV_CH), jnp.float32), -4.0, 4.0)
    return (raw_taps * group_scale * channel_scale / jnp.sqrt(float(KERNEL))).astype(jnp.float32)


def steps_of(rng, extent, cuts, smallest, top_value):
    gain = 1.0
    for position, parts in cuts:
        heights = jax.random.uniform(jax.random.fold_in(jax.random.fold_in(rng, 6), position), (parts,), jnp.float32, smallest / len(cuts), top_value / len(cuts))
        gain = gain * jnp.repeat(jnp.exp(heights), extent[position] // parts).reshape((-1,) + (1,) * (len(extent) - 1 - position))
    return gain


def scatter_about(rng, shape, scale, most, shards=(), dtype=jnp.bfloat16):
    level = steps_of(rng, shape, shards, -0.22, 0.18) if shards else 1.0
    result = jax.random.normal(rng, shape, jnp.float32) * scale * level
    return jnp.minimum(jnp.maximum(result, -most), most).astype(dtype)


def setup_inputs(seed: int = 0) -> dict:
    key_list = jax.random.split(jax.random.key(seed), 10)
    return {
        "tokens": scatter_about(key_list[0], (TOKENS, D), 1.0, 6.0, ((0, 8), (1, 4))),
        "norm_gain": jnp.clip(1.0 + 0.18 * jax.random.normal(key_list[1], (LAYERS, D), jnp.float32), 0.1, 1.9),
        "w_value": scatter_about(key_list[2], (LAYERS, D, CONV_CH), D ** -0.5, 0.125, ((1, 8), (2, 4))),
        "w_gate": scatter_about(key_list[3], (LAYERS, D, CONV_CH), D ** -0.5, 0.125, ((1, 8), (2, 4))),
        "conv_taps": draw_conv_taps(jax.random.fold_in(key_list[9], 71), 0),
        "conv_bias": scatter_about(key_list[5], (LAYERS, CONV_CH), 0.5, 3.0, ((1, 4),), jnp.float32),
        "ln_gain": jnp.clip(1.0 + 0.18 * jax.random.normal(key_list[6], (LAYERS, CONV_CH), jnp.float32), 0.1, 1.9),
        "ln_shift": scatter_about(key_list[7], (LAYERS, CONV_CH), 0.5, 3.0, ((1, 4),), jnp.float32),
        "w_out": scatter_about(key_list[8], (LAYERS, CONV_CH, D), CONV_CH ** -0.5, 0.1875, ((1, 4), (2, 8))),
    }


norm_floor = 0.01

def reference(tokens, norm_gain, w_value, w_gate, conv_taps, conv_bias, ln_gain, ln_shift, w_out):
    stream = tokens
    reach = KERNEL // 2
    block_width = CONV_CH // N_TP
    for layer_index in range(LAYERS):
        stream_f32 = stream.astype(jnp.float32)
        scale_rows = lax.rsqrt(lax.optimization_barrier(jnp.mean(stream_f32 * stream_f32, axis=-1, keepdims=True)) + norm_floor)
        normed = (stream_f32 * scale_rows * norm_gain[layer_index]).astype(jnp.bfloat16)
        value_rows = jnp.dot(normed, w_value[layer_index], preferred_element_type=jnp.float32)
        gate_rows = jnp.dot(normed, w_gate[layer_index], preferred_element_type=jnp.float32)
        gated_input = (value_rows * jax.nn.sigmoid(gate_rows)).astype(jnp.bfloat16)
        padded = jnp.pad(gated_input, ((reach, reach), (0, 0))).astype(jnp.float32)
        convolved = jnp.zeros((TOKENS, CONV_CH), jnp.float32) + conv_bias[layer_index]
        for offset in range(KERNEL):
            convolved = convolved + conv_taps[layer_index, offset] * padded[offset:offset + TOKENS]
        average = lax.optimization_barrier(jnp.mean(convolved, axis=-1, keepdims=True))
        spread = lax.optimization_barrier(jnp.mean(convolved * convolved, axis=-1, keepdims=True)) - average * average
        activated = jax.nn.silu((convolved - average) * lax.rsqrt(spread + norm_floor) * ln_gain[layer_index] + ln_shift[layer_index]).astype(jnp.bfloat16)
        summed = jnp.zeros((TOKENS, D), jnp.float32)
        for block_index in range(N_TP):
            first = block_index * block_width
            partial_block = jnp.dot(activated[:, first:first + block_width], w_out[layer_index, first:first + block_width], preferred_element_type=jnp.float32).astype(jnp.bfloat16)
            partial_block = lax.optimization_barrier(partial_block)
            summed = summed + partial_block.astype(jnp.float32)
        stream = (stream_f32 + summed).astype(jnp.bfloat16)
    return stream
```

```python
import functools

import jax
import jax.numpy as jnp
from jax import lax
from jax.experimental import pallas as pl
from jax.experimental.pallas import tpu as pltpu
from jax.sharding import PartitionSpec as P

MESH = pl.DeviceIdType.MESH

norm_floor = 0.01


def with_halo(array, sides, width):
    for axis, dim in sides:
        size, length = (lax.axis_size(axis), array.shape[dim])
        up = [(i, (i + 1) % size) for i in range(size - 1)]
        down = [(j, i) for i, j in up]
        last = lax.slice_in_dim(array, length - width, length, axis=dim)
        first = lax.slice_in_dim(array, 0, width, axis=dim)
        before = lax.ppermute(last, axis, up)
        after = lax.ppermute(first, axis, down)
        array = jnp.concatenate([before, array, after], axis=dim)
    return array


def body(tokens, norm_gain, w_value, w_gate, conv_taps, conv_bias, ln_gain, ln_shift, w_out):
    stream = tokens
    layer_count = w_value.shape[0]
    reach = conv_taps.shape[1] // 2
    local_channels = w_value.shape[2]
    channels = local_channels * lax.axis_size("tp")
    tok_rows = tokens.shape[0]
    whole_value, whole_gate = (
        lax.all_gather(w_value, "sp", axis=1, tiled=True),
        lax.all_gather(w_gate, "sp", axis=1, tiled=True),
    )
    whole_out = lax.all_gather(w_out, "sp", axis=2, tiled=True)
    for layer_index in range(layer_count):
        whole_rows = lax.all_gather(stream, "tp", axis=1, tiled=True)
        rows_f32 = whole_rows.astype(jnp.float32)
        scale_rows = lax.rsqrt(jnp.mean(rows_f32 * rows_f32, axis=-1, keepdims=True) + norm_floor)
        normed = (rows_f32 * scale_rows * norm_gain[layer_index]).astype(jnp.bfloat16)
        value_rows = jnp.dot(normed, whole_value[layer_index], preferred_element_type=jnp.float32)
        gate_rows = jnp.dot(normed, whole_gate[layer_index], preferred_element_type=jnp.float32)
        gated_input = (value_rows * jax.nn.sigmoid(gate_rows)).astype(jnp.bfloat16)
        padded = with_halo(gated_input, (("sp", 0),), reach)
        padded = padded.astype(jnp.float32)
        convolved = jnp.zeros((tok_rows, local_channels), jnp.float32) + conv_bias[layer_index]
        for offset in range(2 * reach + 1):
            convolved = (
                convolved + conv_taps[layer_index, offset] * padded[offset : offset + tok_rows]
            )
        moments = lax.psum(
            (
                jnp.sum(convolved, axis=-1, keepdims=True),
                jnp.sum(convolved * convolved, axis=-1, keepdims=True),
            ),
            "tp",
        )
        average = moments[0] / channels
        spread = moments[1] / channels - average * average
        activated = jax.nn.silu(
            (convolved - average) * lax.rsqrt(spread + norm_floor) * ln_gain[layer_index]
            + ln_shift[layer_index]
        ).astype(jnp.bfloat16)
        partial_rows = jnp.dot(
            activated, whole_out[layer_index], preferred_element_type=jnp.float32
        )
        summed = lax.psum_scatter(
            partial_rows.astype(jnp.bfloat16), "tp", scatter_dimension=1, tiled=True
        ).astype(jnp.float32)
        stream = (stream.astype(jnp.float32) + summed).astype(jnp.bfloat16)
    return stream


def fused(
    dims,
    tok, gain_in, wv_in, wg_in, wo_in, taps_in, bias_in, lng_in, lns_in,
    out,
    wvg, wo, taps, bias, lng, lns, stream, normed, gated, cv, cv2, act, resid,
    loc_sem, pre_send, pre_recv, z_send, z_recv, d_send, d_recv,
    a_send, a_recv, b_send, b_recv, r_send, r_recv, o_send, o_recv,
    tok_send, tok_recv, zh_send, zh_recv, hp_send, hp_recv, ih_send, ih_recv,
    par_send, par_recv, ln_send, ln_recv,
    ca_send, ca_recv, cb_send, cb_recv, cr_send, cr_recv,
    l_send, l_recv, p_send, p_recv, res_send, res_recv,
):
    n, tp, layers, ntaps, rows, width, chans = dims
    planes = n // 2
    feats = width // tp
    lch = chans // tp
    krows = width // n
    ocols = width // n
    reach = ntaps // 2
    grain = 16
    halo = grain * layers
    window = rows + 2 * halo
    slots = 2 * planes - 1
    last = layers - 1
    lanes = 128
    per_side = lch // lanes
    per_out = feats // ocols

    sp = lax.axis_index("sp")
    t = lax.axis_index("tp")
    z, y = sp // 2, lax.rem(sp, 2)
    x, h = t // 2, lax.rem(t, 2)
    xn, yn, hn = 1 - x, 1 - y, 1 - h
    same = 1 - (y + h - 2 * y * h)
    spn = 2 * z + yn
    has_up, has_down = 1 - (z + 1) // planes, jnp.minimum(z, 1)

    partner = (sp, 2 * x + hn)
    xdev = (sp, 2 * xn + h)
    ydev = (spn, t)
    ax, ay = hn * xn + h * x, hn * y + h * yn
    bx, by = hn * x + h * xn, hn * yn + h * y
    adev = (2 * z + ay, 2 * ax + h)
    bdev = (2 * z + by, 2 * bx + h)

    def rcopy(src, dst, ssem, rsem, dev):
        return pltpu.make_async_remote_copy(
            src_ref=src, dst_ref=dst, send_sem=ssem, recv_sem=rsem,
            device_id=dev, device_id_type=MESH)

    def arrived(ref, ssem, rsem):
        rcopy(ref, ref, ssem, rsem, partner).wait_recv()

    def when(flag):
        return pl.when(flag == 1)

    def vblock(l, k, zs, c):
        r = pl.ds(pl.multiple_of((2 * zs + c) * krows, krows), krows)
        return wvg.at[l, k, r, :]

    def oblock(l, zs, yy, cb):
        r = pl.ds(pl.multiple_of(cb * lch, lch), lch)
        return wo.at[l, 2 * zs + yy, r, :]

    def item(l, k, zs):
        return vblock(l, k, zs, h) if k < 2 else oblock(l, zs, y, t)

    def local_copy(l, k):
        src = (wv_in, wg_in, wo_in)[k].at[l]
        return pltpu.make_async_copy(src, item(l, k, z), loc_sem.at[3 * l + k])

    def pre_copy(l, k):
        src = (wv_in, wg_in)[k].at[l]
        i = 2 * l + k
        return rcopy(src, vblock(l, k, z, y), pre_send.at[i], pre_recv.at[i], (spn, 2 * x + hn))

    def z_copy(l, k, d, s):
        zs = z - s if d == 0 else z + s
        ref = item(l, k, zs)
        i = ((d * layers + l) * 3 + k) * (planes - 1) + s
        return rcopy(ref, ref, z_send.at[i], z_recv.at[i], (sp + (2 if d == 0 else -2), t))

    def z_wait(l, k, d, s):
        zs = z - s if d == 0 else z + s
        i = ((d * layers + l) * 3 + k) * (planes - 1) + s - 1
        arrived(item(l, k, zs), z_send.at[i], z_recv.at[i])

    def d_copy(l, k, src_kind, slot, ref):
        i = ((l * 3 + k) * slots + slot) if src_kind == 0 else (
            layers * 3 * slots + ((l * 3) + src_kind - 1) * slots + slot)
        return rcopy(ref, ref, d_send.at[i], d_recv.at[2 * l + k // 2], partner)

    def a_copy(l, slot, zs):
        ref, i = oblock(l, zs, y, t), l * slots + slot
        return rcopy(ref, ref, a_send.at[i], a_recv.at[i], adev)

    def b_copy(l, slot, zs):
        ref, i = oblock(l, zs, y, t), l * slots + slot
        return rcopy(ref, ref, b_send.at[i], b_recv.at[i], bdev)

    def r_copy(l, slot, zs):
        ref, i = oblock(l, zs, ay, 2 * ax + h), l * slots + slot
        return rcopy(ref, ref, r_send.at[i], r_recv.at[i], bdev)

    def o_copy(slot, rel, zs):
        ref, i = oblock(last, zs, y, t), 2 * slot + rel
        return rcopy(ref, ref, o_send.at[i], o_recv.at[2 * t + rel],
                     (sp if rel == 0 else spn, zs))

    def differs(a, b):
        return jnp.minimum(jnp.abs(a - b), 1)

    def spread(l, k, slot, zs):
        if k < 2:
            d_copy(l, k, 0, slot, item(l, k, zs)).start()
        elif l < last:
            a_copy(l, slot, zs).start()
            b_copy(l, slot, zs).start()
            d_copy(l, k, 0, slot, item(l, k, zs)).start()
        else:
            when(differs(zs, t))(lambda: o_copy(slot, 0, zs).start())
            o_copy(slot, 1, zs).start()

    def spread_sent(l, k, slot, zs):
        if k < 2:
            d_copy(l, k, 0, slot, item(l, k, zs)).wait_send()
        elif l < last:
            a_copy(l, slot, zs).wait_send()
            b_copy(l, slot, zs).wait_send()
            d_copy(l, k, 0, slot, item(l, k, zs)).wait_send()
        else:
            when(differs(zs, t))(lambda: o_copy(slot, 0, zs).wait_send())
            o_copy(slot, 1, zs).wait_send()

    def own_start(l, k):
        if k < 2:
            when(same)(lambda: local_copy(l, k).wait())

            @when(1 - same)
            def _():
                i = 2 * l + k
                arrived(item(l, k, z), pre_send.at[i], pre_recv.at[i])
        else:
            local_copy(l, k).wait()
        when(has_up)(lambda: z_copy(l, k, 0, 0).start())
        when(has_down)(lambda: z_copy(l, k, 1, 0).start())
        spread(l, k, 0, z)

    def below(s):
        return jnp.minimum(z // s, 1)

    def above(s):
        return jnp.minimum((planes - 1 - z) // s, 1)

    def groups(s):
        if s == 0:
            return [(None, 0, z)]
        return [(below(s), 2 * s - 1, z - s), (above(s), 2 * s, z + s)]

    def guarded(flag, f):
        if flag is None:
            f()
        else:
            when(flag)(f)

    def z_recv_step(l, k, s):
        for d, (flag, slot, zs) in enumerate(groups(s)):
            def go(d=d, slot=slot, zs=zs):
                z_wait(l, k, d, s)
                if s < planes - 1:
                    when((has_up, has_down)[d])(lambda: z_copy(l, k, d, s).start())
                spread(l, k, slot, zs)
            guarded(flag, go)

    def a_step(l, s):
        for flag, slot, zs in groups(s):
            def go(slot=slot, zs=zs):
                i = l * slots + slot
                ref = oblock(l, zs, ay, 2 * ax + h)
                arrived(ref, a_send.at[i], a_recv.at[i])
                r_copy(l, slot, zs).start()
                d_copy(l, 2, 1, slot, ref).start()
            guarded(flag, go)

    def b_step(l, s):
        for flag, slot, zs in groups(s):
            def go(slot=slot, zs=zs):
                i = l * slots + slot
                ref = oblock(l, zs, by, 2 * bx + h)
                arrived(ref, b_send.at[i], b_recv.at[i])
                d_copy(l, 2, 2, slot, ref).start()
            guarded(flag, go)

    def r_step(l, s):
        for flag, slot, zs in groups(s):
            def go(slot=slot, zs=zs):
                i = l * slots + slot
                ref = oblock(l, zs, yn, 2 * xn + h)
                arrived(ref, r_send.at[i], r_recv.at[i])
                d_copy(l, 2, 3, slot, ref).start()
            guarded(flag, go)

    def need_v(l):
        arrived(wvg.at[l, :, pl.ds(0, width // 2), :], d_send.at[0], d_recv.at[2 * l])

    def need_o(l):
        arrived(wo.at[l, pl.ds(0, planes)], d_send.at[0], d_recv.at[2 * l + 1])

    def need_last():
        for j in range(tp):
            other = lax.rem(t + j, tp)
            for rel in range(2):
                if j or rel:
                    i = 2 * other + rel
                    arrived(oblock(last, t, y if rel == 0 else yn, other), o_send.at[0], o_recv.at[i])

    def weights_sent():
        for l in range(layers):
            for k in range(3):
                if k < 2:
                    when(1 - same)(lambda l=l, k=k: pre_copy(l, k).wait_send())
                for s in range(planes - 1):
                    for d, flag in enumerate((has_up, has_down)):
                        ok = flag if s == 0 else flag * (below(s), above(s))[d]
                        when(ok)(lambda l=l, k=k, d=d, s=s: z_copy(l, k, d, s).wait_send())
                for s in range(planes):
                    for flag, slot, zs in groups(s):
                        guarded(flag, lambda l=l, k=k, slot=slot, zs=zs: spread_sent(l, k, slot, zs))

    def plane_sent():
        for l in range(last):
            for s in range(planes):
                for flag, slot, zs in groups(s):
                    def go(l=l, slot=slot, zs=zs):
                        r_copy(l, slot, zs).wait_send()
                        d_copy(l, 2, 1, slot, oblock(l, zs, ay, 2 * ax + h)).wait_send()
                        d_copy(l, 2, 2, slot, oblock(l, zs, by, 2 * bx + h)).wait_send()
                        d_copy(l, 2, 3, slot, oblock(l, zs, yn, 2 * xn + h)).wait_send()
                    guarded(flag, go)

    def cols(owner):
        return pl.ds(pl.multiple_of(owner * feats, feats), feats)

    def mcols(owner):
        return stream.at[pl.ds(halo, rows), cols(owner)]

    tcols = cols(t)

    def tok_copy(j):
        dev = ((sp, 2 * x + y), (sp, 2 * xn + y), (spn, 2 * x + y))[j]
        return rcopy(tok, mcols(t), tok_send.at[j], tok_recv.at[t], dev)

    rt = same * (2 * xn) + (1 - same) * (2 * x + 1)
    rsp = same * spn + (1 - same) * sp
    rtp = same * t + (1 - same) * (2 * xn + h)

    def tok_pass():
        return rcopy(mcols(rt), mcols(rt), tok_send.at[3], tok_recv.at[rt], (rsp, rtp))

    def tok_starts():
        when(1 - same)(lambda: tok_copy(0).start())
        tok_copy(1).start()
        tok_copy(2).start()

        @when(same)
        def _():
            stream[pl.ds(halo, rows), tcols] = tok[...]

    def tok_relay():
        arrived(mcols(rt), tok_send.at[3], tok_recv.at[rt])
        tok_pass().start()

    def tok_waits():
        for j in range(1, tp):
            other = lax.rem(rt + j, tp)
            ok = 1 - same * (1 - differs(other, t))
            when(ok)(lambda other=other: arrived(mcols(other), tok_send.at[3], tok_recv.at[other]))

    zh_to = y * has_up + yn * has_down
    zh_from = hn * has_down + h * has_up

    def edge(owner_cols, side):
        r = pl.ds(pl.multiple_of(side * (halo + rows), grain), halo)
        return stream.at[r, owner_cols]

    def zh_copy():
        src = tok.at[pl.ds(pl.multiple_of(y * (rows - halo), grain), halo), :]
        return rcopy(src, edge(tcols, yn), zh_send.at[0], zh_recv.at[t],
                     (sp + 4 * y - 2, 2 * x + yn))

    def half_cols(xx):
        return pl.ds(pl.multiple_of(xx * 2 * feats, feats), 2 * feats)

    def hp_copy(j):
        ref = edge(half_cols(xn if j == 2 else x), h)
        return rcopy(ref, ref, hp_send.at[j], hp_recv.at[j], xdev if j == 0 else ydev)

    def halo_pass():
        @when(zh_from * (1 - same))
        def _():
            for c in range(2):
                arrived(edge(cols(2 * x + c), h), zh_send.at[0], zh_recv.at[2 * x + c])
            hp_copy(0).start()
            hp_copy(1).start()

        @when(1 - zh_from)
        def _():
            stream[pl.ds(pl.multiple_of(h * (halo + rows), grain), halo), :] = jnp.zeros((halo, width), jnp.bfloat16)

    def halo_pass_on():
        @when(zh_from * (1 - same))
        def _():
            arrived(edge(half_cols(xn), h), hp_send.at[0], hp_recv.at[0])
            hp_copy(2).start()

    def halo_waits():
        @when(zh_from * same)
        def _():
            arrived(edge(half_cols(x), h), hp_send.at[0], hp_recv.at[1])
            arrived(edge(half_cols(xn), h), hp_send.at[0], hp_recv.at[2])

    def ih_copy():
        src = stream.at[pl.ds(pl.multiple_of(hn * rows + h * halo, grain), halo), :]
        dst = stream.at[pl.ds(pl.multiple_of(h * (halo + rows), grain), halo), :]
        return rcopy(src, dst, ih_send.at[0], ih_recv.at[0], partner)

    def ih_wait():
        ref = stream.at[pl.ds(pl.multiple_of(hn * (halo + rows), grain), halo), :]
        arrived(ref, ih_send.at[0], ih_recv.at[0])

    def par_copy(i):
        a, b = ((taps_in, taps), (bias_in, bias))[i]
        return rcopy(a, b, par_send.at[i], par_recv.at[i], partner)

    def ln_copy(i, j):
        a, b = ((lng_in, lng), (lns_in, lns))[i]
        return rcopy(a, b.at[t], ln_send.at[3 * i + j - 1], ln_recv.at[tp * i + t],
                     (sp, lax.rem(t + j, tp)))

    def params_start():
        for i in range(2):
            when(same)(lambda i=i: par_copy(i).start())
            for j in range(1, tp):
                ln_copy(i, j).start()

        @when(same)
        def _():
            taps[...] = taps_in[...]
            bias[...] = bias_in[...]
        lng[t] = lng_in[...]
        lns[t] = lns_in[...]

    def params_wait():
        for i, ref in enumerate((taps, bias)):
            when(1 - same)(lambda i=i, ref=ref: arrived(ref, par_send.at[i], par_recv.at[i]))
        for i, ref in enumerate((lng, lns)):
            for j in range(1, tp):
                other = lax.rem(t + j, tp)
                arrived(ref.at[other], ln_send.at[0], ln_recv.at[tp * i + other])

    def small_sent():
        when(1 - same)(lambda: tok_copy(0).wait_send())
        tok_copy(1).wait_send()
        tok_copy(2).wait_send()
        when(zh_to)(lambda: zh_copy().wait_send())
        for i in range(2):
            when(same)(lambda i=i: par_copy(i).wait_send())
            for j in range(1, tp):
                ln_copy(i, j).wait_send()

    def stream_sent():
        tok_pass().wait_send()

        @when(zh_from * (1 - same))
        def _():
            for j in range(3):
                hp_copy(j).wait_send()
        ih_copy().wait_send()

    cb_own = 2 * x + y
    cb_a, cb_b, cb_d = 2 * ax + ay, 2 * bx + by, 2 * xn + yn

    def piece(l, i):
        size = (window - 2 * grain * (l + 1)) // 2
        return i * size, size

    def cblock(l, i, cb):
        r0, size = piece(l, i)
        return cv.at[l, cb, pl.ds(r0, size), :]

    def cv_copy(l, i, j):
        ref = cblock(l, i, cb_a if j == 2 else cb_own)
        s, r = ((ca_send, ca_recv), (cb_send, cb_recv), (cr_send, cr_recv))[j]
        return rcopy(ref, ref, s.at[2 * l + i], r.at[2 * l + i], adev if j == 0 else bdev)

    def cv_start(l, i):
        cv_copy(l, i, 0).start()
        cv_copy(l, i, 1).start()

    def cv_relay(l, i):
        arrived(cblock(l, i, cb_a), ca_send.at[2 * l + i], ca_recv.at[2 * l + i])
        cv_copy(l, i, 2).start()

    def cv_waits(l, i):
        arrived(cblock(l, i, cb_b), cb_send.at[2 * l + i], cb_recv.at[2 * l + i])
        arrived(cblock(l, i, cb_d), cr_send.at[2 * l + i], cr_recv.at[2 * l + i])

    def lblock(i, cb):
        r0, size = piece(last, i)
        return cv2.at[cb, pl.ds(r0, size), :]

    def l_copy(i, j):
        src, cb, dev = (
            (cblock(last, i, cb_own), cb_own, ydev),
            (cblock(last, i, cb_own), cb_own, xdev),
            (lblock(i, 2 * x + yn), 2 * x + yn, xdev),
        )[j]
        return rcopy(src, lblock(i, cb), l_send.at[3 * i + j], l_recv.at[3 * i + j], dev)

    def p_copy(i, j):
        cb = (cb_own, 2 * x + yn, 2 * xn + y, 2 * xn + yn)[j]
        src = cblock(last, i, cb) if j == 0 else lblock(i, cb)
        return rcopy(src, lblock(i, cb), p_send.at[tp * i + j], p_recv.at[tp * i + j], partner)

    def last_start(i):
        r0, size = piece(last, i)
        when(1 - same)(lambda: l_copy(i, 0).start())

        @when(same)
        def _():
            l_copy(i, 1).start()
            p_copy(i, 0).start()
            cv2[cb_own, r0:r0 + size, :] = cv[last, cb_own, r0:r0 + size, :]

    def last_relay(i):
        @when(same)
        def _():
            arrived(lblock(i, 2 * x + yn), l_send.at[0], l_recv.at[3 * i])
            l_copy(i, 2).start()
            p_copy(i, 1).start()

    def last_waits(i):
        @when(same)
        def _():
            for j in (1, 2):
                cb = 2 * xn + (y if j == 1 else yn)
                arrived(lblock(i, cb), l_send.at[0], l_recv.at[3 * i + j])
                p_copy(i, j + 1).start()

        @when(1 - same)
        def _():
            for j, cb in enumerate((2 * x + yn, 2 * x + y, 2 * xn + yn, 2 * xn + y)):
                arrived(lblock(i, cb), p_send.at[0], p_recv.at[tp * i + j])

    def conv_sent():
        for i in range(2):
            for l in range(last):
                for j in range(3):
                    cv_copy(l, i, j).wait_send()
            when(1 - same)(lambda i=i: l_copy(i, 0).wait_send())

            @when(same)
            def _(i=i):
                l_copy(i, 1).wait_send()
                l_copy(i, 2).wait_send()
                for j in range(tp):
                    p_copy(i, j).wait_send()

    def res_copy():
        src = stream.at[pl.ds(halo, rows), cols(2 * x + hn)]
        return rcopy(src, resid, res_send.at[0], res_recv.at[0], partner)

    def res_start():
        @when(same)
        def _():
            res_copy().start()
            resid[...] = stream[pl.ds(halo, rows), tcols]

    def res_wait():
        when(1 - same)(lambda: arrived(resid, res_send.at[0], res_recv.at[0]))

    first_row = (2 * z + h) * rows - halo
    total_rows = n * rows

    def normalize(layer, w0, size):
        def step(i, carry):
            r = pl.ds(pl.multiple_of(w0 + i * grain, grain), grain)
            v = stream[r, :].astype(jnp.float32)
            scale = lax.rsqrt(jnp.mean(v * v, axis=-1, keepdims=True) + norm_floor)
            normed[r, :] = (v * scale * gain_in[layer:layer + 1, :]).astype(jnp.bfloat16)
            return carry

        lax.fori_loop(0, size // grain, step, 0)

    def project(layer, w0, size):
        value = jnp.dot(normed[w0:w0 + size, :], wvg[layer, 0], preferred_element_type=jnp.float32)
        gate = jnp.dot(normed[w0:w0 + size, :], wvg[layer, 1], preferred_element_type=jnp.float32)
        g = (value * jax.nn.sigmoid(gate)).astype(jnp.bfloat16).astype(jnp.float32)
        row = lax.broadcasted_iota(jnp.int32, (size, lch), 0) + (first_row + w0)
        g = jnp.where(jnp.logical_and(row >= 0, row < total_rows), g, 0.0)
        for b in range(per_side):
            gated[b, w0:w0 + size, :] = g[:, b * lanes:(b + 1) * lanes]

    def convolve(layer, i):
        r0, size = piece(layer, i)
        start = grain * (layer + 1)
        cut = -(-size // 2 // grain) * grain
        for c0, part in ((r0, cut), (r0 + cut, size - cut)):
            def lane_block(b, carry, c0=c0, part=part):
                lane = pl.ds(pl.multiple_of(b * lanes, lanes), lanes)
                total = jnp.zeros((part, lanes), jnp.float32) + bias[layer:layer + 1, lane]
                for k in range(ntaps):
                    first = start + c0 + k - reach
                    total = total + taps[layer, k:k + 1, lane] * gated[b, first:first + part, :]
                cv[layer, cb_own, c0:c0 + part, lane] = total.astype(jnp.bfloat16)
                return carry

            lax.fori_loop(0, per_side, lane_block, 0)

    def activate(layer, i):
        r0, size = piece(layer, i)

        def step(j, carry):
            r = pl.ds(pl.multiple_of(r0 + j * grain, grain), grain)
            src = [(cv[layer, b, r, :] if layer < last else cv2[b, r, :]).astype(jnp.float32) for b in range(tp)]
            s1 = sum(jnp.sum(v, axis=-1, keepdims=True) for v in src)
            s2 = sum(jnp.sum(v * v, axis=-1, keepdims=True) for v in src)
            average = s1 / chans
            spread_ = s2 / chans - average * average
            scale = lax.rsqrt(spread_ + norm_floor)
            for b, v in enumerate(src):
                u = (v - average) * scale * lng[b, layer:layer + 1, :] + lns[b, layer:layer + 1, :]
                act[r, b * lch:(b + 1) * lch] = (u / (1.0 + jnp.exp(-u))).astype(jnp.bfloat16)
            return carry

        lax.fori_loop(0, size // grain, step, 0)

    def expand(layer, i):
        r0, size = piece(layer, i)
        w0 = grain * (layer + 1) + r0

        def step(j, carry):
            c = pl.ds(pl.multiple_of(j * ocols, ocols), ocols)
            add = jnp.dot(act[r0:r0 + size, :], wo[layer, j], preferred_element_type=jnp.float32)
            stream[w0:w0 + size, c] = (stream[w0:w0 + size, c].astype(jnp.float32) + add).astype(jnp.bfloat16)
            return carry

        lax.fori_loop(0, n, step, 0)

    def finish(i):
        r0, size = piece(last, i)
        for j in range(per_out):
            c = slice(j * ocols, (j + 1) * ocols)
            add = jnp.dot(act[r0:r0 + size, :], wo[last, per_out * t + j], preferred_element_type=jnp.float32)
            out[r0:r0 + size, c] = (resid[r0:r0 + size, c].astype(jnp.float32) + add).astype(jnp.bfloat16)

    barrier = pltpu.get_barrier_semaphore()
    for l in range(layers):
        for k in range(3):
            if k < 2:
                when(same)(lambda l=l, k=k: local_copy(l, k).start())
            else:
                local_copy(l, k).start()
    for ds in range(2):
        for j in range(tp):
            if ds or j:
                pl.semaphore_signal(barrier, inc=1, device_id=((sp, spn)[ds], lax.rem(t + j, tp)), device_id_type=MESH)
    for flag, step in ((has_up, 2), (has_down, -2)):
        @when(flag)
        def _(step=step):
            for c in range(2):
                pl.semaphore_signal(barrier, inc=1, device_id=(sp + step, 2 * x + c), device_id_type=MESH)
    pl.semaphore_wait(barrier, 2 * tp - 1 + 2 * (has_up + has_down))

    def pre_start(l):
        for k in range(2):
            when(1 - same)(lambda k=k: pre_copy(l, k).start())

    pre_start(0)
    when(zh_to)(lambda: zh_copy().start())
    tok_starts()
    params_start()
    own_start(0, 0)
    own_start(0, 1)
    pre_start(1)
    pre_start(2)
    z_recv_step(0, 0, 1)
    z_recv_step(0, 1, 1)
    halo_pass()
    tok_relay()
    halo_pass_on()
    z_recv_step(0, 0, 2)
    z_recv_step(0, 1, 2)
    own_start(0, 2)
    tok_waits()
    ih_copy().start()
    halo_waits()
    ih_wait()
    normalize(0, 0, window)
    params_wait()
    z_recv_step(0, 0, 3)
    z_recv_step(0, 1, 3)
    need_v(0)

    for layer in range(layers):
        w0 = grain * layer
        half = (window - 2 * w0) // 2
        for i in range(2):
            project(layer, w0 + i * half, half)
        if layer < last:
            own_start(layer + 1, 0)
            own_start(layer + 1, 1)
            for i in range(2):
                convolve(layer, i)
                cv_start(layer, i)
            z_recv_step(layer, 2, 1)
            a_step(layer, 0)
            cv_relay(layer, 0)
            cv_relay(layer, 1)
            z_recv_step(layer, 2, 2)
            a_step(layer, 1)
            b_step(layer, 0)
            z_recv_step(layer, 2, 3)
            z_recv_step(layer + 1, 0, 1)
            z_recv_step(layer + 1, 1, 1)
            for i in range(2):
                cv_waits(layer, i)
                activate(layer, i)
            a_step(layer, 2)
            b_step(layer, 1)
            r_step(layer, 0)
            z_recv_step(layer + 1, 0, 2)
            z_recv_step(layer + 1, 1, 2)
            own_start(layer + 1, 2)
            a_step(layer, 3)
            b_step(layer, 2)
            r_step(layer, 1)
            b_step(layer, 3)
            r_step(layer, 2)
            r_step(layer, 3)
            need_o(layer)
            if layer == 0:
                stream_sent()
            for i in range(2):
                expand(layer, i)
            if layer + 1 == last:
                res_start()
            normalize(layer + 1, grain * (layer + 1), window - 2 * grain * (layer + 1))
            z_recv_step(layer + 1, 0, 3)
            z_recv_step(layer + 1, 1, 3)
            need_v(layer + 1)
        else:
            z_recv_step(last, 2, 1)
            for i in range(2):
                convolve(last, i)
                last_start(i)
            for i in range(2):
                last_relay(i)
            z_recv_step(last, 2, 2)
            for i in range(2):
                last_waits(i)
            z_recv_step(last, 2, 3)
            res_wait()
            for i in range(2):
                activate(last, i)
            need_last()
            for i in range(2):
                finish(i)
    weights_sent()
    plane_sent()
    small_sent()
    conv_sent()
    when(same)(lambda: res_copy().wait_send())


def fused_call(mesh, *args):
    tokens, norm_gain, w_value, w_gate, conv_taps, conv_bias, ln_gain, ln_shift, w_out = args
    n, tp = mesh.shape["sp"], mesh.shape["tp"]
    layers, ntaps, lch = conv_taps.shape
    rows, feats = tokens.shape
    width, chans = feats * tp, lch * tp
    planes = n // 2
    slots = 2 * planes - 1
    halo = 16 * layers
    window = rows + 2 * halo
    most = window - 32
    dims = (n, tp, layers, ntaps, rows, width, chans)
    vmem = pl.BlockSpec(memory_space=pltpu.VMEM)
    anys = pl.BlockSpec(memory_space=pl.ANY)
    bf, f32 = jnp.bfloat16, jnp.float32
    dma = lambda k: pltpu.SemaphoreType.DMA((k,))
    pairs = lambda k: [dma(k), dma(k)]
    wide = (layers - 1) * slots
    return pl.pallas_call(
        functools.partial(fused, dims),
        out_shape=jax.ShapeDtypeStruct((rows, feats), bf),
        in_specs=[vmem, vmem, anys, anys, anys, vmem, vmem, vmem, vmem],
        out_specs=vmem,
        scratch_shapes=[
            pltpu.VMEM((layers, 2, width, lch), bf),
            pltpu.VMEM((layers, n, chans, width // n), bf),
            pltpu.VMEM(conv_taps.shape, f32),
            pltpu.VMEM(conv_bias.shape, f32),
            pltpu.VMEM((tp,) + ln_gain.shape, f32),
            pltpu.VMEM((tp,) + ln_shift.shape, f32),
            pltpu.VMEM((window, width), bf),
            pltpu.VMEM((window, width), bf),
            pltpu.VMEM((lch // 128, window, 128), f32),
            pltpu.VMEM((layers, tp, most, lch), bf),
            pltpu.VMEM((tp, rows, lch), bf),
            pltpu.VMEM((most, chans), bf),
            pltpu.VMEM((rows, feats), bf),
            dma(3 * layers),
            *pairs(2 * layers),
            *pairs(2 * layers * 3 * (planes - 1)),
            dma(layers * 3 * slots * 2), dma(2 * layers),
            *pairs(wide), *pairs(wide), *pairs(wide),
            *pairs(2 * slots),
            *pairs(tp), *pairs(tp), *pairs(3), *pairs(1),
            *pairs(2), dma(6), dma(2 * tp),
            *pairs(2 * layers), *pairs(2 * layers), *pairs(2 * layers),
            *pairs(6), *pairs(2 * tp), *pairs(1),
        ],
        compiler_params=pltpu.CompilerParams(
            collective_id=0, has_side_effects=True, vmem_limit_bytes=60 * 1024 * 1024),
    )(tokens, norm_gain, w_value, w_gate, w_out, conv_taps, conv_bias, ln_gain, ln_shift)


def fits(mesh, tokens, conv_taps, w_out):
    n, tp = mesh.shape["sp"], mesh.shape["tp"]
    layers, ntaps, lch = conv_taps.shape
    rows, feats = tokens.shape
    return (tp == 4 and n == 2 * tp and ntaps % 2 == 1 and ntaps // 2 < 16 and layers > 1
            and w_out.shape[2] % 128 == 0 and lch % 128 == 0 and feats % 128 == 0
            and feats == 2 * w_out.shape[2]
            and rows % 32 == 0 and rows >= 32 * layers and rows <= 512
            and layers * w_out.shape[1] * w_out.shape[2] * n * 12 <= 20 * 1024 * 1024)


def solution(mesh):
    placed = (
        P("sp", "tp"),
        P(),
        P(None, "sp", "tp"),
        P(None, "sp", "tp"),
        P(None, None, "tp"),
        P(None, "tp"),
        P(None, "tp"),
        P(None, "tp"),
        P(None, "tp", "sp"),
    )

    def run(*args):
        if fits(mesh, args[0], args[4], args[8]):
            return fused_call(mesh, *args)
        return body(*args)

    return jax.shard_map(run, mesh=mesh, in_specs=placed, out_specs=P("sp", "tp"), check_vma=False)
```

```python
import functools

import jax
import jax.numpy as jnp
from jax import lax
from jax.experimental import pallas as pl
from jax.experimental.pallas import tpu as pltpu
from jax.sharding import PartitionSpec as P

MESH = pl.DeviceIdType.MESH

norm_floor = 0.01


def with_halo(array, sides, width):
    for axis, dim in sides:
        size, length = (lax.axis_size(axis), array.shape[dim])
        up = [(i, (i + 1) % size) for i in range(size - 1)]
        down = [(j, i) for i, j in up]
        last = lax.slice_in_dim(array, length - width, length, axis=dim)
        first = lax.slice_in_dim(array, 0, width, axis=dim)
        before = lax.ppermute(last, axis, up)
        after = lax.ppermute(first, axis, down)
        array = jnp.concatenate([before, array, after], axis=dim)
    return array


def body(tokens, norm_gain, w_value, w_gate, conv_taps, conv_bias, ln_gain, ln_shift, w_out):
    stream = tokens
    layer_count = w_value.shape[0]
    reach = conv_taps.shape[1] // 2
    local_channels = w_value.shape[2]
    channels = local_channels * lax.axis_size("tp")
    tok_rows = tokens.shape[0]
    whole_value, whole_gate = (
        lax.all_gather(w_value, "sp", axis=1, tiled=True),
        lax.all_gather(w_gate, "sp", axis=1, tiled=True),
    )
    whole_out = lax.all_gather(w_out, "sp", axis=2, tiled=True)
    for layer_index in range(layer_count):
        whole_rows = lax.all_gather(stream, "tp", axis=1, tiled=True)
        rows_f32 = whole_rows.astype(jnp.float32)
        scale_rows = lax.rsqrt(jnp.mean(rows_f32 * rows_f32, axis=-1, keepdims=True) + norm_floor)
        normed = (rows_f32 * scale_rows * norm_gain[layer_index]).astype(jnp.bfloat16)
        value_rows = jnp.dot(normed, whole_value[layer_index], preferred_element_type=jnp.float32)
        gate_rows = jnp.dot(normed, whole_gate[layer_index], preferred_element_type=jnp.float32)
        gated_input = (value_rows * jax.nn.sigmoid(gate_rows)).astype(jnp.bfloat16)
        padded = with_halo(gated_input, (("sp", 0),), reach)
        padded = padded.astype(jnp.float32)
        convolved = jnp.zeros((tok_rows, local_channels), jnp.float32) + conv_bias[layer_index]
        for offset in range(2 * reach + 1):
            convolved = (
                convolved + conv_taps[layer_index, offset] * padded[offset : offset + tok_rows]
            )
        moments = lax.psum(
            (
                jnp.sum(convolved, axis=-1, keepdims=True),
                jnp.sum(convolved * convolved, axis=-1, keepdims=True),
            ),
            "tp",
        )
        average = moments[0] / channels
        spread = moments[1] / channels - average * average
        activated = jax.nn.silu(
            (convolved - average) * lax.rsqrt(spread + norm_floor) * ln_gain[layer_index]
            + ln_shift[layer_index]
        ).astype(jnp.bfloat16)
        partial_rows = jnp.dot(
            activated, whole_out[layer_index], preferred_element_type=jnp.float32
        )
        summed = lax.psum_scatter(
            partial_rows.astype(jnp.bfloat16), "tp", scatter_dimension=1, tiled=True
        ).astype(jnp.float32)
        stream = (stream.astype(jnp.float32) + summed).astype(jnp.bfloat16)
    return stream


def fused(
    dims,
    tok, gain_in, wv_in, wg_in, wo_in, taps_in, bias_in, lng_in, lns_in,
    out,
    wvg, wo, taps, bias, lng, lns, stream, normed, gated, cv, cv2, act, resid, rowa, rowb,
    loc_sem, pre_send, pre_recv, z_send, z_recv, d_send, d_recv,
    a_send, a_recv, b_send, b_recv, r_send, r_recv, o_send, o_recv,
    tok_send, tok_recv, zh_send, zh_recv, hp_send, hp_recv, ih_send, ih_recv,
    par_send, par_recv, ln_send, ln_recv,
    ca_send, ca_recv, cb_send, cb_recv, cr_send, cr_recv,
    l_send, l_recv, p_send, p_recv, res_send, res_recv,
):
    n, tp, layers, ntaps, rows, width, chans = dims
    planes = n // 2
    feats = width // tp
    lch = chans // tp
    krows = width // n
    ocols = width // n
    reach = ntaps // 2
    grain = 16
    halo = grain * layers
    window = rows + 2 * halo
    slots = 2 * planes - 1
    last = layers - 1
    lanes = 128
    per_side = lch // lanes
    per_out = feats // ocols
    swapped = 1

    sp = lax.axis_index("sp")
    t = lax.axis_index("tp")
    z, y = sp // 2, lax.rem(sp, 2)
    x, h = t // 2, lax.rem(t, 2)
    xn, yn, hn = 1 - x, 1 - y, 1 - h
    same = 1 - (y + h - 2 * y * h)
    spn = 2 * z + yn
    has_up, has_down = 1 - (z + 1) // planes, jnp.minimum(z, 1)

    partner = (sp, 2 * x + hn)
    xdev = (sp, 2 * xn + h)
    ydev = (spn, t)
    ax, ay = hn * xn + h * x, hn * y + h * yn
    bx, by = hn * x + h * xn, hn * yn + h * y
    adev = (2 * z + ay, 2 * ax + h)
    bdev = (2 * z + by, 2 * bx + h)

    def route(slot):
        if (slot + 1) // 2 < swapped:
            return (x, yn), ydev, (xn, y), xdev
        return (ax, ay), adev, (bx, by), bdev

    def rcopy(src, dst, ssem, rsem, dev):
        return pltpu.make_async_remote_copy(
            src_ref=src, dst_ref=dst, send_sem=ssem, recv_sem=rsem,
            device_id=dev, device_id_type=MESH)

    def arrived(ref, ssem, rsem):
        rcopy(ref, ref, ssem, rsem, partner).wait_recv()

    def when(flag):
        return pl.when(flag == 1)

    def vblock(l, k, zs, c):
        r = pl.ds(pl.multiple_of((2 * zs + c) * krows, krows), krows)
        return wvg.at[l, k, r, :]

    def oblock(l, zs, yy, cb):
        r = pl.ds(pl.multiple_of(cb * lch, lch), lch)
        return wo.at[l, 2 * zs + yy, r, :]

    def item(l, k, zs):
        return vblock(l, k, zs, h) if k < 2 else oblock(l, zs, y, t)

    def local_copy(l, k):
        src = (wv_in, wg_in, wo_in)[k].at[l]
        return pltpu.make_async_copy(src, item(l, k, z), loc_sem.at[3 * l + k])

    def pre_copy(l, k):
        src = (wv_in, wg_in)[k].at[l]
        i = 2 * l + k
        return rcopy(src, vblock(l, k, z, y), pre_send.at[i], pre_recv.at[i], (spn, 2 * x + hn))

    def z_copy(l, k, d, s):
        zs = z - s if d == 0 else z + s
        ref = item(l, k, zs)
        i = ((d * layers + l) * 3 + k) * (planes - 1) + s
        return rcopy(ref, ref, z_send.at[i], z_recv.at[i], (sp + (2 if d == 0 else -2), t))

    def z_wait(l, k, d, s):
        zs = z - s if d == 0 else z + s
        i = ((d * layers + l) * 3 + k) * (planes - 1) + s - 1
        arrived(item(l, k, zs), z_send.at[i], z_recv.at[i])

    def d_copy(l, k, src_kind, slot, ref):
        i = ((l * 3 + k) * slots + slot) if src_kind == 0 else (
            layers * 3 * slots + ((l * 3) + src_kind - 1) * slots + slot)
        return rcopy(ref, ref, d_send.at[i], d_recv.at[l if k < 2 else layers + l * slots + slot], partner)

    def a_copy(l, slot, zs):
        ref, i = oblock(l, zs, y, t), l * slots + slot
        return rcopy(ref, ref, a_send.at[i], a_recv.at[i], route(slot)[1])

    def b_copy(l, slot, zs):
        ref, i = oblock(l, zs, y, t), l * slots + slot
        return rcopy(ref, ref, b_send.at[i], b_recv.at[i], route(slot)[3])

    def from_a(l, slot, zs):
        px, py = route(slot)[0]
        return oblock(l, zs, py, 2 * px + h)

    def from_b(l, slot, zs):
        px, py = route(slot)[2]
        return oblock(l, zs, py, 2 * px + h)

    def r_copy(l, slot, zs):
        ref, i = from_a(l, slot, zs), l * slots + slot
        return rcopy(ref, ref, r_send.at[i], r_recv.at[i], route(slot)[3])

    def o_copy(slot, rel, zs):
        ref, i = oblock(last, zs, y, t), 2 * slot + rel
        return rcopy(ref, ref, o_send.at[i], o_recv.at[2 * t + rel],
                     (sp if rel == 0 else spn, zs))

    def differs(a, b):
        return jnp.minimum(jnp.abs(a - b), 1)

    def to_partner(l, k, slot, zs):
        if k < 2 or l < last:
            d_copy(l, k, 0, slot, item(l, k, zs)).start()

    def spread(l, s):
        for flag, slot, zs in groups(s):
            def go(slot=slot, zs=zs):
                if l < last:
                    a_copy(l, slot, zs).start()
                    b_copy(l, slot, zs).start()
                else:
                    when(differs(zs, t))(lambda: o_copy(slot, 0, zs).start())
                    o_copy(slot, 1, zs).start()
            guarded(flag, go)

    def spread_sent(l, k, slot, zs):
        if k < 2:
            d_copy(l, k, 0, slot, item(l, k, zs)).wait_send()
        elif l < last:
            a_copy(l, slot, zs).wait_send()
            b_copy(l, slot, zs).wait_send()
            d_copy(l, k, 0, slot, item(l, k, zs)).wait_send()
        else:
            when(differs(zs, t))(lambda: o_copy(slot, 0, zs).wait_send())
            o_copy(slot, 1, zs).wait_send()

    def own_start(l, k):
        if k < 2:
            when(same)(lambda: local_copy(l, k).wait())

            @when(1 - same)
            def _():
                i = 2 * l + k
                arrived(item(l, k, z), pre_send.at[i], pre_recv.at[i])
        else:
            local_copy(l, k).wait()
        when(has_up)(lambda: z_copy(l, k, 0, 0).start())
        when(has_down)(lambda: z_copy(l, k, 1, 0).start())
        to_partner(l, k, 0, z)

    def below(s):
        return jnp.minimum(z // s, 1)

    def above(s):
        return jnp.minimum((planes - 1 - z) // s, 1)

    def groups(s):
        if s == 0:
            return [(None, 0, z)]
        return [(below(s), 2 * s - 1, z - s), (above(s), 2 * s, z + s)]

    def guarded(flag, f):
        if flag is None:
            f()
        else:
            when(flag)(f)

    def z_recv_step(l, k, s):
        for d, (flag, slot, zs) in enumerate(groups(s)):
            def go(d=d, slot=slot, zs=zs):
                z_wait(l, k, d, s)
                if s < planes - 1:
                    when((has_up, has_down)[d])(lambda: z_copy(l, k, d, s).start())
                to_partner(l, k, slot, zs)
            guarded(flag, go)

    def a_step(l, s):
        for flag, slot, zs in groups(s):
            def go(slot=slot, zs=zs):
                i = l * slots + slot
                ref = from_a(l, slot, zs)
                arrived(ref, a_send.at[i], a_recv.at[i])
                r_copy(l, slot, zs).start()
                d_copy(l, 2, 1, slot, ref).start()
            guarded(flag, go)

    def b_step(l, s):
        for flag, slot, zs in groups(s):
            def go(slot=slot, zs=zs):
                i = l * slots + slot
                ref = from_b(l, slot, zs)
                arrived(ref, b_send.at[i], b_recv.at[i])
                d_copy(l, 2, 2, slot, ref).start()
            guarded(flag, go)

    def r_step(l, s):
        for flag, slot, zs in groups(s):
            def go(slot=slot, zs=zs):
                i = l * slots + slot
                ref = oblock(l, zs, yn, 2 * xn + h)
                arrived(ref, r_send.at[i], r_recv.at[i])
                d_copy(l, 2, 3, slot, ref).start()
            guarded(flag, go)

    def need_v(l):
        arrived(wvg.at[l, :, pl.ds(0, width // 2), :], d_send.at[0], d_recv.at[l])

    def need_last():
        for j in range(tp):
            other = lax.rem(t + j, tp)
            for rel in range(2):
                if j or rel:
                    i = 2 * other + rel
                    arrived(oblock(last, t, y if rel == 0 else yn, other), o_send.at[0], o_recv.at[i])

    def weights_sent():
        for l in range(layers):
            for k in range(3):
                if k < 2:
                    when(1 - same)(lambda l=l, k=k: pre_copy(l, k).wait_send())
                for s in range(planes - 1):
                    for d, flag in enumerate((has_up, has_down)):
                        ok = flag if s == 0 else flag * (below(s), above(s))[d]
                        when(ok)(lambda l=l, k=k, d=d, s=s: z_copy(l, k, d, s).wait_send())
                for s in range(planes):
                    for flag, slot, zs in groups(s):
                        guarded(flag, lambda l=l, k=k, slot=slot, zs=zs: spread_sent(l, k, slot, zs))

    def plane_sent():
        for l in range(last):
            for s in range(planes):
                for flag, slot, zs in groups(s):
                    def go(l=l, slot=slot, zs=zs):
                        r_copy(l, slot, zs).wait_send()
                        d_copy(l, 2, 1, slot, from_a(l, slot, zs)).wait_send()
                        d_copy(l, 2, 2, slot, from_b(l, slot, zs)).wait_send()
                        d_copy(l, 2, 3, slot, oblock(l, zs, yn, 2 * xn + h)).wait_send()
                    guarded(flag, go)

    def cols(owner):
        return pl.ds(pl.multiple_of(owner * feats, feats), feats)

    def mcols(owner):
        return stream.at[pl.ds(halo, rows), cols(owner)]

    tcols = cols(t)

    def tok_copy(j):
        dev = ((sp, 2 * x + y), (sp, 2 * xn + y), (spn, 2 * x + y))[j]
        return rcopy(tok, mcols(t), tok_send.at[j], tok_recv.at[t], dev)

    half_rows = rows // 2

    def hcols(owner, part):
        return stream.at[pl.ds(halo + part * half_rows, half_rows), cols(owner)]

    def tok_pass(j):
        if j == 0:
            ref, i, dev, k = hcols(2 * xn + yn, 0), 2 * xn + yn, ydev, 3
        elif j == 1:
            ref, i, dev, k = mcols(2 * x + yn), 2 * x + yn, xdev, 3
        else:
            ref, i, dev, k = hcols(2 * x + y, 1), tp, xdev, 4
        return rcopy(ref, ref, tok_send.at[k], tok_recv.at[i], dev)

    def tok_starts():
        when(1 - same)(lambda: tok_copy(0).start())
        tok_copy(1).start()

        @when(same)
        def _():
            stream[pl.ds(halo, rows), tcols] = tok[...]

    def tok_arrived(ref, i):
        arrived(ref, tok_send.at[3], tok_recv.at[i])

    def tok_relay():
        @when(same)
        def _():
            tok_arrived(mcols(2 * xn + yn), 2 * xn + yn)
            tok_pass(0).start()

        @when(1 - same)
        def _():
            tok_arrived(mcols(2 * x + yn), 2 * x + yn)
            tok_pass(1).start()

    def tok_relay_late():
        @when(1 - same)
        def _():
            tok_arrived(mcols(2 * x + y), 2 * x + y)
            tok_pass(2).start()

    def tok_waits():
        @when(same)
        def _():
            tok_arrived(mcols(2 * x + hn), 2 * x + hn)
            tok_arrived(mcols(2 * xn + y), 2 * xn + y)

        @when(1 - same)
        def _():
            tok_arrived(mcols(2 * xn + yn), 2 * xn + yn)
            tok_arrived(hcols(2 * xn + y, 0), 2 * xn + y)
            tok_arrived(hcols(2 * xn + y, 1), tp)

    zh_to = y * has_up + yn * has_down
    zh_from = hn * has_down + h * has_up

    def edge(owner_cols, side):
        r = pl.ds(pl.multiple_of(side * (halo + rows), grain), halo)
        return stream.at[r, owner_cols]

    def zh_copy():
        src = tok.at[pl.ds(pl.multiple_of(y * (rows - halo), grain), halo), :]
        return rcopy(src, edge(tcols, yn), zh_send.at[0], zh_recv.at[t],
                     (sp + 4 * y - 2, 2 * x + yn))

    def half_cols(xx):
        return pl.ds(pl.multiple_of(xx * 2 * feats, feats), 2 * feats)

    def hp_copy(j):
        ref = edge(half_cols(xn if j == 2 else x), h)
        return rcopy(ref, ref, hp_send.at[j], hp_recv.at[j], xdev if j == 0 else ydev)

    def halo_pass():
        @when(zh_from * (1 - same))
        def _():
            for c in range(2):
                arrived(edge(cols(2 * x + c), h), zh_send.at[0], zh_recv.at[2 * x + c])
            hp_copy(0).start()
            hp_copy(1).start()

        @when(1 - zh_from)
        def _():
            stream[pl.ds(pl.multiple_of(h * (halo + rows), grain), halo), :] = jnp.zeros((halo, width), jnp.bfloat16)

    def halo_pass_on():
        @when(zh_from * (1 - same))
        def _():
            arrived(edge(half_cols(xn), h), hp_send.at[0], hp_recv.at[0])
            hp_copy(2).start()

    def halo_waits():
        @when(zh_from * same)
        def _():
            arrived(edge(half_cols(x), h), hp_send.at[0], hp_recv.at[1])
            arrived(edge(half_cols(xn), h), hp_send.at[0], hp_recv.at[2])

    def ih_copy():
        src = stream.at[pl.ds(pl.multiple_of(hn * rows + h * halo, grain), halo), :]
        dst = stream.at[pl.ds(pl.multiple_of(h * (halo + rows), grain), halo), :]
        return rcopy(src, dst, ih_send.at[0], ih_recv.at[0], partner)

    def ih_wait():
        ref = stream.at[pl.ds(pl.multiple_of(hn * (halo + rows), grain), halo), :]
        arrived(ref, ih_send.at[0], ih_recv.at[0])

    def par_copy(i):
        a, b = ((taps_in, taps), (bias_in, bias))[i]
        return rcopy(a, b, par_send.at[i], par_recv.at[i], partner)

    def ln_copy(i, j):
        a, b = ((lng_in, lng), (lns_in, lns))[i]
        return rcopy(a, b.at[t], ln_send.at[3 * i + j - 1], ln_recv.at[tp * i + t],
                     (sp, lax.rem(t + j, tp)))

    def params_start():
        for i in range(2):
            when(same)(lambda i=i: par_copy(i).start())
            for j in range(1, tp):
                ln_copy(i, j).start()

        @when(same)
        def _():
            taps[...] = taps_in[...]
            bias[...] = bias_in[...]
        lng[t] = lng_in[...]
        lns[t] = lns_in[...]

    def params_wait():
        for i, ref in enumerate((taps, bias)):
            when(1 - same)(lambda i=i, ref=ref: arrived(ref, par_send.at[i], par_recv.at[i]))
        for i, ref in enumerate((lng, lns)):
            for j in range(1, tp):
                other = lax.rem(t + j, tp)
                arrived(ref.at[other], ln_send.at[0], ln_recv.at[tp * i + other])

    def small_sent():
        when(1 - same)(lambda: tok_copy(0).wait_send())
        tok_copy(1).wait_send()
        tok_copy(2).wait_send()
        when(zh_to)(lambda: zh_copy().wait_send())
        for i in range(2):
            when(same)(lambda i=i: par_copy(i).wait_send())
            for j in range(1, tp):
                ln_copy(i, j).wait_send()

    def stream_sent():
        when(same)(lambda: tok_pass(0).wait_send())

        @when(1 - same)
        def _():
            tok_pass(1).wait_send()
            tok_pass(2).wait_send()

        @when(zh_from * (1 - same))
        def _():
            for j in range(3):
                hp_copy(j).wait_send()
        ih_copy().wait_send()

    cb_own = 2 * x + y
    cb_a, cb_b, cb_d = 2 * ax + ay, 2 * bx + by, 2 * xn + yn

    def piece(l, i):
        total = window - 2 * grain * (l + 1)
        first = total - rows // 2
        return i * first, total - first if i else first

    def cblock(l, i, cb):
        r0, size = piece(l, i)
        return cv.at[l, cb, pl.ds(r0, size), :]

    def cv_copy(l, i, j):
        ref = cblock(l, i, cb_a if j == 2 else cb_own)
        s, r = ((ca_send, ca_recv), (cb_send, cb_recv), (cr_send, cr_recv))[j]
        return rcopy(ref, ref, s.at[2 * l + i], r.at[2 * l + i], adev if j == 0 else bdev)

    def cv_start(l, i):
        cv_copy(l, i, 0).start()
        cv_copy(l, i, 1).start()

    def cv_relay(l, i):
        arrived(cblock(l, i, cb_a), ca_send.at[2 * l + i], ca_recv.at[2 * l + i])
        cv_copy(l, i, 2).start()

    def cv_waits(l, i):
        arrived(cblock(l, i, cb_b), cb_send.at[2 * l + i], cb_recv.at[2 * l + i])
        arrived(cblock(l, i, cb_d), cr_send.at[2 * l + i], cr_recv.at[2 * l + i])

    def lblock(i, cb):
        r0, size = piece(last, i)
        return cv2.at[cb, pl.ds(r0, size), :]

    def l_copy(i, j):
        src, cb, dev = (
            (cblock(last, i, cb_own), cb_own, ydev),
            (cblock(last, i, cb_own), cb_own, xdev),
            (lblock(i, 2 * x + yn), 2 * x + yn, xdev),
        )[j]
        return rcopy(src, lblock(i, cb), l_send.at[3 * i + j], l_recv.at[3 * i + j], dev)

    def p_copy(i, j):
        cb = (cb_own, 2 * x + yn, 2 * xn + y, 2 * xn + yn)[j]
        src = cblock(last, i, cb) if j == 0 else lblock(i, cb)
        return rcopy(src, lblock(i, cb), p_send.at[tp * i + j], p_recv.at[tp * i + j], partner)

    def last_start(i):
        r0, size = piece(last, i)
        when(1 - same)(lambda: l_copy(i, 0).start())

        @when(same)
        def _():
            l_copy(i, 1).start()
            p_copy(i, 0).start()
            cv2[cb_own, r0:r0 + size, :] = cv[last, cb_own, r0:r0 + size, :]

    def last_relay(i):
        @when(same)
        def _():
            arrived(lblock(i, 2 * x + yn), l_send.at[0], l_recv.at[3 * i])
            l_copy(i, 2).start()
            p_copy(i, 1).start()

    def last_waits(i):
        @when(same)
        def _():
            for j in (1, 2):
                cb = 2 * xn + (y if j == 1 else yn)
                arrived(lblock(i, cb), l_send.at[0], l_recv.at[3 * i + j])
                p_copy(i, j + 1).start()

        @when(1 - same)
        def _():
            for j, cb in enumerate((2 * x + yn, 2 * x + y, 2 * xn + yn, 2 * xn + y)):
                arrived(lblock(i, cb), p_send.at[0], p_recv.at[tp * i + j])

    def conv_sent():
        for i in range(2):
            for l in range(last):
                for j in range(3):
                    cv_copy(l, i, j).wait_send()
            when(1 - same)(lambda i=i: l_copy(i, 0).wait_send())

            @when(same)
            def _(i=i):
                l_copy(i, 1).wait_send()
                l_copy(i, 2).wait_send()
                for j in range(tp):
                    p_copy(i, j).wait_send()

    def res_copy():
        src = stream.at[pl.ds(halo, rows), cols(2 * x + hn)]
        return rcopy(src, resid, res_send.at[0], res_recv.at[0], partner)

    def res_start():
        @when(same)
        def _():
            res_copy().start()
            resid[...] = stream[pl.ds(halo, rows), tcols]

    def res_wait():
        when(1 - same)(lambda: arrived(resid, res_send.at[0], res_recv.at[0]))

    first_row = (2 * z + h) * rows - halo
    total_rows = n * rows

    def over_rows(start, size, block, f):
        def step(i, carry):
            f(pl.ds(pl.multiple_of(start + i * block, grain), block))
            return carry

        lax.fori_loop(0, size // block, step, 0)

    def chunk(layer, i):
        r0, size = piece(layer - 1, i)
        return grain * layer + r0, size

    def normalize(layer, i):
        w0, size = chunk(layer, i)
        block = 2 * grain

        def squares(r):
            total = jnp.zeros((block, lanes), jnp.float32)
            for c in range(width // lanes):
                v = stream[r, c * lanes:(c + 1) * lanes].astype(jnp.float32)
                total = total + v * v
            rowa[r, :] = total

        def scaled(r):
            scale = rowa[r, :]
            for c in range(width // lanes):
                lane = slice(c * lanes, (c + 1) * lanes)
                v = stream[r, lane].astype(jnp.float32)
                normed[r, lane] = (v * scale * gain_in[layer:layer + 1, lane]).astype(jnp.bfloat16)

        over_rows(w0, size, block, squares)
        mean = jnp.sum(rowa[w0:w0 + size, :], axis=-1, keepdims=True) / width
        rowa[w0:w0 + size, :] = jnp.broadcast_to(lax.rsqrt(mean + norm_floor), (size, lanes))
        over_rows(w0, size, block, scaled)

    def project(layer, i):
        w0, size = chunk(layer, i)
        value = jnp.dot(normed[w0:w0 + size, :], wvg[layer, 0], preferred_element_type=jnp.float32)
        gate = jnp.dot(normed[w0:w0 + size, :], wvg[layer, 1], preferred_element_type=jnp.float32)
        g = (value * (0.5 + 0.5 * jnp.tanh(0.5 * gate))).astype(jnp.bfloat16).astype(jnp.float32)
        row = lax.broadcasted_iota(jnp.int32, (size, lch), 0) + (first_row + w0)
        g = jnp.where(jnp.logical_and(row >= 0, row < total_rows), g, 0.0)
        for b in range(per_side):
            gated[b, w0:w0 + size, :] = g[:, b * lanes:(b + 1) * lanes]

    def convolve(layer, i):
        r0, size = piece(layer, i)
        start = grain * (layer + 1)
        cut = -(-size // 2 // grain) * grain
        for c0, part in ((r0, cut), (r0 + cut, size - cut)):
            def lane_block(b, carry, c0=c0, part=part):
                lane = pl.ds(pl.multiple_of(b * lanes, lanes), lanes)
                total = jnp.zeros((part, lanes), jnp.float32) + bias[layer:layer + 1, lane]
                for k in range(ntaps):
                    first = start + c0 + k - reach
                    total = total + taps[layer, k:k + 1, lane] * gated[b, first:first + part, :]
                cv[layer, cb_own, c0:c0 + part, lane] = total.astype(jnp.bfloat16)
                return carry

            lax.fori_loop(0, per_side, lane_block, 0)

    def activate(layer, i):
        r0, size = piece(layer, i)
        block = 2 * grain if size % (2 * grain) == 0 else grain
        parts = [(b, c) for b in range(tp) for c in range(per_side)]

        def load(b, c, r):
            lane = slice(c * lanes, (c + 1) * lanes)
            return (cv[layer, b, r, lane] if layer < last else cv2[b, r, lane]).astype(jnp.float32)

        def sums(r):
            s1 = jnp.zeros((block, lanes), jnp.float32)
            s2 = jnp.zeros((block, lanes), jnp.float32)
            for b, c in parts:
                v = load(b, c, r)
                s1 = s1 + v
                s2 = s2 + v * v
            rowa[r, :] = s1
            rowb[r, :] = s2

        def apply(r):
            scale, shift = rowa[r, :], rowb[r, :]
            for b, c in parts:
                lane = slice(c * lanes, (c + 1) * lanes)
                u = (load(b, c, r) - shift) * scale
                u = 0.5 * (u * lng[b, layer:layer + 1, lane] + lns[b, layer:layer + 1, lane])
                act[r, b * lch + c * lanes:b * lch + (c + 1) * lanes] = (u + u * jnp.tanh(u)).astype(jnp.bfloat16)

        over_rows(r0, size, block, sums)
        rows_ = slice(r0, r0 + size)
        average = jnp.sum(rowa[rows_, :], axis=-1, keepdims=True) / chans
        spread_ = jnp.sum(rowb[rows_, :], axis=-1, keepdims=True) / chans - average * average
        rowa[rows_, :] = jnp.broadcast_to(lax.rsqrt(spread_ + norm_floor), (size, lanes))
        rowb[rows_, :] = jnp.broadcast_to(average, (size, lanes))
        over_rows(r0, size, block, apply)

    def expand_wait(layer, s):
        for flag, slot, zs in groups(s):
            sem = d_recv.at[layers + layer * slots + slot]
            guarded(flag, lambda sem=sem: arrived(wo.at[layer, 0], d_send.at[0], sem))

    def expand(layer, s, pieces=(0, 1)):
        for flag, slot, zs in groups(s):
            def go(slot=slot, zs=zs):
                def step(j, carry):
                    c = pl.ds(pl.multiple_of((2 * zs + j) * ocols, ocols), ocols)
                    for i in pieces:
                        r0, size = piece(layer, i)
                        w0 = grain * (layer + 1) + r0
                        add = jnp.dot(act[r0:r0 + size, :], wo[layer, 2 * zs + j], preferred_element_type=jnp.float32)
                        stream[w0:w0 + size, c] = (stream[w0:w0 + size, c].astype(jnp.float32) + add).astype(jnp.bfloat16)
                    return carry

                lax.fori_loop(0, 2, step, 0)
            guarded(flag, go)

    def finish(i):
        r0, size = piece(last, i)
        for j in range(per_out):
            c = slice(j * ocols, (j + 1) * ocols)
            add = jnp.dot(act[r0:r0 + size, :], wo[last, per_out * t + j], preferred_element_type=jnp.float32)
            out[r0:r0 + size, c] = (resid[r0:r0 + size, c].astype(jnp.float32) + add).astype(jnp.bfloat16)

    barrier = pltpu.get_barrier_semaphore()
    for l in range(layers):
        for k in range(3):
            if k < 2:
                when(same)(lambda l=l, k=k: local_copy(l, k).start())
            else:
                local_copy(l, k).start()
    for ds in range(2):
        for j in range(tp):
            if ds or j:
                pl.semaphore_signal(barrier, inc=1, device_id=((sp, spn)[ds], lax.rem(t + j, tp)), device_id_type=MESH)
    for flag, step in ((has_up, 2), (has_down, -2)):
        @when(flag)
        def _(step=step):
            for c in range(2):
                pl.semaphore_signal(barrier, inc=1, device_id=(sp + step, 2 * x + c), device_id_type=MESH)
    pl.semaphore_wait(barrier, 2 * tp - 1 + 2 * (has_up + has_down))

    def pre_start(l):
        for k in range(2):
            when(1 - same)(lambda k=k: pre_copy(l, k).start())

    pre_start(0)
    when(zh_to)(lambda: zh_copy().start())
    tok_starts()
    halo_pass()
    tok_copy(2).start()
    params_start()
    own_start(0, 0)
    own_start(0, 1)
    z_recv_step(0, 0, 1)
    tok_relay()
    z_recv_step(0, 1, 1)
    own_start(0, 2)
    halo_pass_on()
    z_recv_step(0, 0, 2)
    tok_relay_late()
    pre_start(1)
    z_recv_step(0, 1, 2)
    spread(0, 0)
    z_recv_step(0, 2, 1)
    tok_waits()
    ih_copy().start()
    halo_waits()
    ih_wait()
    normalize(0, 0)
    normalize(0, 1)
    params_wait()
    z_recv_step(0, 0, 3)
    z_recv_step(0, 1, 3)
    own_start(1, 0)
    own_start(1, 1)
    spread(0, 1)
    need_v(0)
    for i in range(2):
        project(0, i)
        convolve(0, i)
        cv_start(0, i)
        if i == 0:
            a_step(0, 0)
            z_recv_step(0, 2, 2)
    pre_start(2)

    for layer in range(last):
        after = layer + 1
        cv_relay(layer, 0)
        cv_relay(layer, 1)
        spread(layer, 2)
        z_recv_step(layer, 2, 3)
        spread(layer, 3)
        z_recv_step(after, 0, 1)
        b_step(layer, 0)
        a_step(layer, 1)
        z_recv_step(after, 1, 1)
        for i in range(2):
            cv_waits(layer, i)
            activate(layer, i)
        z_recv_step(after, 0, 2)
        r_step(layer, 0)
        a_step(layer, 2)
        z_recv_step(after, 1, 2)
        own_start(after, 2)
        if layer == 0:
            stream_sent()
        expand_wait(layer, 0)
        expand(layer, 0)
        b_step(layer, 1)
        a_step(layer, 3)
        r_step(layer, 1)
        spread(after, 0)
        z_recv_step(after, 0, 3)
        expand_wait(layer, 1)
        expand(layer, 1)
        b_step(layer, 2)
        z_recv_step(after, 1, 3)
        if after < last:
            own_start(after + 1, 0)
            own_start(after + 1, 1)
        r_step(layer, 2)
        expand_wait(layer, 2)
        expand(layer, 2)
        b_step(layer, 3)
        need_v(after)
        r_step(layer, 3)
        z_recv_step(after, 2, 1)
        spread(after, 1)
        expand_wait(layer, 3)
        for i in range(2):
            expand(layer, 3, (i,))
            normalize(after, i)
            project(after, i)
            convolve(after, i)
            if after < last:
                cv_start(after, i)
                if i == 0:
                    a_step(after, 0)
            else:
                last_start(i)
        z_recv_step(after, 2, 2)
    res_start()
    last_relay(0)
    last_relay(1)
    spread(last, 2)
    z_recv_step(last, 2, 3)
    spread(last, 3)
    res_wait()
    last_waits(0)
    activate(last, 0)
    last_waits(1)
    activate(last, 1)
    need_last()
    finish(0)
    finish(1)
    weights_sent()
    plane_sent()
    small_sent()
    conv_sent()
    when(same)(lambda: res_copy().wait_send())


def fused_call(mesh, *args):
    tokens, norm_gain, w_value, w_gate, conv_taps, conv_bias, ln_gain, ln_shift, w_out = args
    n, tp = mesh.shape["sp"], mesh.shape["tp"]
    layers, ntaps, lch = conv_taps.shape
    rows, feats = tokens.shape
    width, chans = feats * tp, lch * tp
    planes = n // 2
    slots = 2 * planes - 1
    halo = 16 * layers
    window = rows + 2 * halo
    most = window - 32
    dims = (n, tp, layers, ntaps, rows, width, chans)
    vmem = pl.BlockSpec(memory_space=pltpu.VMEM)
    anys = pl.BlockSpec(memory_space=pl.ANY)
    bf, f32 = jnp.bfloat16, jnp.float32
    dma = lambda k: pltpu.SemaphoreType.DMA((k,))
    pairs = lambda k: [dma(k), dma(k)]
    wide = (layers - 1) * slots
    return pl.pallas_call(
        functools.partial(fused, dims),
        out_shape=jax.ShapeDtypeStruct((rows, feats), bf),
        in_specs=[vmem, vmem, anys, anys, anys, vmem, vmem, vmem, vmem],
        out_specs=vmem,
        scratch_shapes=[
            pltpu.VMEM((layers, 2, width, lch), bf),
            pltpu.VMEM((layers, n, chans, width // n), bf),
            pltpu.VMEM(conv_taps.shape, f32),
            pltpu.VMEM(conv_bias.shape, f32),
            pltpu.VMEM((tp,) + ln_gain.shape, f32),
            pltpu.VMEM((tp,) + ln_shift.shape, f32),
            pltpu.VMEM((window, width), bf),
            pltpu.VMEM((window, width), bf),
            pltpu.VMEM((lch // 128, window, 128), f32),
            pltpu.VMEM((layers, tp, most, lch), bf),
            pltpu.VMEM((tp, rows, lch), bf),
            pltpu.VMEM((most, chans), bf),
            pltpu.VMEM((rows, feats), bf),
            pltpu.VMEM((window, 128), f32),
            pltpu.VMEM((window, 128), f32),
            dma(3 * layers),
            *pairs(2 * layers),
            *pairs(2 * layers * 3 * (planes - 1)),
            dma(layers * 3 * slots * 2), dma(layers * (1 + slots)),
            *pairs(wide), *pairs(wide), *pairs(wide),
            *pairs(2 * slots),
            *pairs(tp + 1), *pairs(tp), *pairs(3), *pairs(1),
            *pairs(2), dma(6), dma(2 * tp),
            *pairs(2 * layers), *pairs(2 * layers), *pairs(2 * layers),
            *pairs(6), *pairs(2 * tp), *pairs(1),
        ],
        compiler_params=pltpu.CompilerParams(
            collective_id=0, has_side_effects=True, vmem_limit_bytes=60 * 1024 * 1024),
    )(tokens, norm_gain, w_value, w_gate, w_out, conv_taps, conv_bias, ln_gain, ln_shift)


def fits(mesh, tokens, conv_taps, w_out):
    n, tp = mesh.shape["sp"], mesh.shape["tp"]
    layers, ntaps, lch = conv_taps.shape
    rows, feats = tokens.shape
    return (tp == 4 and n == 2 * tp and ntaps % 2 == 1 and ntaps // 2 < 16 and layers > 1
            and w_out.shape[2] % 128 == 0 and lch % 128 == 0 and feats % 128 == 0
            and feats == 2 * w_out.shape[2]
            and rows % 64 == 0 and rows >= 32 * layers and rows <= 512
            and layers * w_out.shape[1] * w_out.shape[2] * n * 12 <= 20 * 1024 * 1024)


def solution(mesh):
    placed = (
        P("sp", "tp"),
        P(),
        P(None, "sp", "tp"),
        P(None, "sp", "tp"),
        P(None, None, "tp"),
        P(None, "tp"),
        P(None, "tp"),
        P(None, "tp"),
        P(None, "tp", "sp"),
    )

    def run(*args):
        if fits(mesh, args[0], args[4], args[8]):
            return fused_call(mesh, *args)
        return body(*args)

    return jax.shard_map(run, mesh=mesh, in_specs=placed, out_specs=P("sp", "tp"), check_vma=False)
```

```python
import functools

import jax
import jax.numpy as jnp
from jax import lax
from jax.experimental import pallas as pl
from jax.experimental.pallas import tpu as pltpu
from jax.sharding import PartitionSpec as P

MESH = pl.DeviceIdType.MESH

norm_floor = 0.01


def with_halo(array, sides, width):
    for axis, dim in sides:
        size, length = (lax.axis_size(axis), array.shape[dim])
        up = [(i, (i + 1) % size) for i in range(size - 1)]
        down = [(j, i) for i, j in up]
        last = lax.slice_in_dim(array, length - width, length, axis=dim)
        first = lax.slice_in_dim(array, 0, width, axis=dim)
        before = lax.ppermute(last, axis, up)
        after = lax.ppermute(first, axis, down)
        array = jnp.concatenate([before, array, after], axis=dim)
    return array


def body(tokens, norm_gain, w_value, w_gate, conv_taps, conv_bias, ln_gain, ln_shift, w_out):
    stream = tokens
    layer_count = w_value.shape[0]
    reach = conv_taps.shape[1] // 2
    local_channels = w_value.shape[2]
    channels = local_channels * lax.axis_size("tp")
    tok_rows = tokens.shape[0]
    whole_value, whole_gate = (
        lax.all_gather(w_value, "sp", axis=1, tiled=True),
        lax.all_gather(w_gate, "sp", axis=1, tiled=True),
    )
    whole_out = lax.all_gather(w_out, "sp", axis=2, tiled=True)
    for layer_index in range(layer_count):
        whole_rows = lax.all_gather(stream, "tp", axis=1, tiled=True)
        rows_f32 = whole_rows.astype(jnp.float32)
        scale_rows = lax.rsqrt(jnp.mean(rows_f32 * rows_f32, axis=-1, keepdims=True) + norm_floor)
        normed = (rows_f32 * scale_rows * norm_gain[layer_index]).astype(jnp.bfloat16)
        value_rows = jnp.dot(normed, whole_value[layer_index], preferred_element_type=jnp.float32)
        gate_rows = jnp.dot(normed, whole_gate[layer_index], preferred_element_type=jnp.float32)
        gated_input = (value_rows * jax.nn.sigmoid(gate_rows)).astype(jnp.bfloat16)
        padded = with_halo(gated_input, (("sp", 0),), reach)
        padded = padded.astype(jnp.float32)
        convolved = jnp.zeros((tok_rows, local_channels), jnp.float32) + conv_bias[layer_index]
        for offset in range(2 * reach + 1):
            convolved = (
                convolved + conv_taps[layer_index, offset] * padded[offset : offset + tok_rows]
            )
        moments = lax.psum(
            (
                jnp.sum(convolved, axis=-1, keepdims=True),
                jnp.sum(convolved * convolved, axis=-1, keepdims=True),
            ),
            "tp",
        )
        average = moments[0] / channels
        spread = moments[1] / channels - average * average
        activated = jax.nn.silu(
            (convolved - average) * lax.rsqrt(spread + norm_floor) * ln_gain[layer_index]
            + ln_shift[layer_index]
        ).astype(jnp.bfloat16)
        partial_rows = jnp.dot(
            activated, whole_out[layer_index], preferred_element_type=jnp.float32
        )
        summed = lax.psum_scatter(
            partial_rows.astype(jnp.bfloat16), "tp", scatter_dimension=1, tiled=True
        ).astype(jnp.float32)
        stream = (stream.astype(jnp.float32) + summed).astype(jnp.bfloat16)
    return stream


def fused(
    dims,
    tok_in, gain_hbm, wv_in, wg_in, wo_in, taps_in, bias_in, lng_in, lns_in,
    out,
    tok, gain_in, result, wvg, wo, taps, bias, lng, lns, stream, normed, gated, cv, cv2, act, resid, rowa, rowb,
    loc_sem, in_sem, out_sem, pre_send, pre_recv, z_send, z_recv, d_send, d_recv,
    a_send, a_recv, b_send, b_recv, r_send, r_recv, o_send, o_recv, op_send,
    tok_send, tok_recv, zh_send, zh_recv, hp_send, hp_recv, ih_send, ih_recv,
    par_send, par_recv, ln_send, ln_recv,
    ca_send, ca_recv, cb_send, cb_recv, cr_send, cr_recv,
    l_send, l_recv, p_send, p_recv, res_send, res_recv,
):
    n, tp, layers, ntaps, rows, width, chans = dims
    planes = n // 2
    feats = width // tp
    lch = chans // tp
    krows = width // n
    ocols = width // n
    reach = ntaps // 2
    grain = 16
    halo = grain * layers
    window = rows + 2 * halo
    slots = 2 * planes - 1
    last = layers - 1
    lanes = 128
    per_side = lch // lanes
    per_out = feats // ocols
    swapped = 1

    sp = lax.axis_index("sp")
    t = lax.axis_index("tp")
    z, y = sp // 2, lax.rem(sp, 2)
    x, h = t // 2, lax.rem(t, 2)
    xn, yn, hn = 1 - x, 1 - y, 1 - h
    same = 1 - (y + h - 2 * y * h)
    spn = 2 * z + yn
    has_up, has_down = 1 - (z + 1) // planes, jnp.minimum(z, 1)

    partner = (sp, 2 * x + hn)
    xdev = (sp, 2 * xn + h)
    ydev = (spn, t)
    ax, ay = hn * xn + h * x, hn * y + h * yn
    bx, by = hn * x + h * xn, hn * yn + h * y
    adev = (2 * z + ay, 2 * ax + h)
    bdev = (2 * z + by, 2 * bx + h)

    def route(l, slot):
        if (slot + 1) // 2 < swapped:
            if l == 0:
                return (x, yn), ydev, (xn, y), xdev
            return (xn, y), xdev, (x, yn), ydev
        return (ax, ay), adev, (bx, by), bdev

    def rcopy(src, dst, ssem, rsem, dev):
        return pltpu.make_async_remote_copy(
            src_ref=src, dst_ref=dst, send_sem=ssem, recv_sem=rsem,
            device_id=dev, device_id_type=MESH)

    def arrived(ref, ssem, rsem):
        rcopy(ref, ref, ssem, rsem, partner).wait_recv()

    def when(flag):
        return pl.when(flag == 1)

    def vblock(l, k, zs, c):
        r = pl.ds(pl.multiple_of((2 * zs + c) * krows, krows), krows)
        return wvg.at[l, k, r, :]

    def oblock(l, zs, yy, cb):
        r = pl.ds(pl.multiple_of(cb * lch, lch), lch)
        return wo.at[l, 2 * zs + yy, r, :]

    def item(l, k, zs):
        return vblock(l, k, zs, h) if k < 2 else oblock(l, zs, y, t)

    def local_copy(l, k):
        src = (wv_in, wg_in, wo_in)[k].at[l]
        return pltpu.make_async_copy(src, item(l, k, z), loc_sem.at[3 * l + k])

    def pre_copy(l, k):
        src = (wv_in, wg_in)[k].at[l]
        i = 2 * l + k
        return rcopy(src, vblock(l, k, z, y), pre_send.at[i], pre_recv.at[i], (spn, 2 * x + hn))

    def z_copy(l, k, d, s):
        zs = z - s if d == 0 else z + s
        ref = item(l, k, zs)
        i = ((d * layers + l) * 3 + k) * (planes - 1) + s
        return rcopy(ref, ref, z_send.at[i], z_recv.at[i], (sp + (2 if d == 0 else -2), t))

    def z_wait(l, k, d, s):
        zs = z - s if d == 0 else z + s
        i = ((d * layers + l) * 3 + k) * (planes - 1) + s - 1
        arrived(item(l, k, zs), z_send.at[i], z_recv.at[i])

    def d_copy(l, k, src_kind, slot, ref):
        i = ((l * 3 + k) * slots + slot) if src_kind == 0 else (
            layers * 3 * slots + ((l * 3) + src_kind - 1) * slots + slot)
        return rcopy(ref, ref, d_send.at[i], d_recv.at[l if k < 2 else layers + l * slots + slot], partner)

    def a_copy(l, slot, zs):
        ref, i = oblock(l, zs, y, t), l * slots + slot
        return rcopy(ref, ref, a_send.at[i], a_recv.at[i], route(l, slot)[1])

    def b_copy(l, slot, zs):
        ref, i = oblock(l, zs, y, t), l * slots + slot
        return rcopy(ref, ref, b_send.at[i], b_recv.at[i], route(l, slot)[3])

    def from_a(l, slot, zs):
        px, py = route(l, slot)[0]
        return oblock(l, zs, py, 2 * px + h)

    def from_b(l, slot, zs):
        px, py = route(l, slot)[2]
        return oblock(l, zs, py, 2 * px + h)

    def r_copy(l, slot, zs):
        ref, i = from_a(l, slot, zs), l * slots + slot
        return rcopy(ref, ref, r_send.at[i], r_recv.at[i], route(l, slot)[3])

    def o_copy(slot, rel, zs):
        ref, i = oblock(last, zs, y, t), 2 * slot + rel
        return rcopy(ref, ref, o_send.at[i], o_recv.at[2 * t + rel],
                     (sp if rel == 0 else spn, zs))

    def differs(a, b):
        return jnp.minimum(jnp.abs(a - b), 1)

    def to_partner(l, k, slot, zs):
        if k < 2 or l < last:
            d_copy(l, k, 0, slot, item(l, k, zs)).start()

    def spread(l, s):
        for flag, slot, zs in groups(s):
            def go(slot=slot, zs=zs):
                if l < last:
                    a_copy(l, slot, zs).start()
                    b_copy(l, slot, zs).start()
                else:
                    when(differs(zs, t))(lambda: o_copy(slot, 0, zs).start())
                    when(1 - differs(zs // 2, x))(lambda: o_copy(slot, 1, zs).start())
            guarded(flag, go)

    def o_pass(c):
        owner = 2 * xn + c
        ref = oblock(last, t, y, owner)
        return rcopy(ref, ref, op_send.at[c], o_recv.at[2 * owner + 1], ydev)

    def o_relay(s):
        @when(1 - differs(jnp.abs(z - t), s))
        def _():
            for c in range(2):
                owner = 2 * xn + c
                arrived(oblock(last, t, y, owner), o_send.at[0], o_recv.at[2 * owner])
                o_pass(c).start()

    def spread_sent(l, k, slot, zs):
        if k < 2:
            d_copy(l, k, 0, slot, item(l, k, zs)).wait_send()
        elif l < last:
            a_copy(l, slot, zs).wait_send()
            b_copy(l, slot, zs).wait_send()
            d_copy(l, k, 0, slot, item(l, k, zs)).wait_send()
        else:
            when(differs(zs, t))(lambda: o_copy(slot, 0, zs).wait_send())
            when(1 - differs(zs // 2, x))(lambda: o_copy(slot, 1, zs).wait_send())

    def own_start(l, k):
        if k < 2:
            when(same)(lambda: local_copy(l, k).wait())

            @when(1 - same)
            def _():
                i = 2 * l + k
                arrived(item(l, k, z), pre_send.at[i], pre_recv.at[i])
        else:
            local_copy(l, k).wait()
        when(has_up)(lambda: z_copy(l, k, 0, 0).start())
        when(has_down)(lambda: z_copy(l, k, 1, 0).start())
        to_partner(l, k, 0, z)

    def below(s):
        return jnp.minimum(z // s, 1)

    def above(s):
        return jnp.minimum((planes - 1 - z) // s, 1)

    def groups(s):
        if s == 0:
            return [(None, 0, z)]
        return [(below(s), 2 * s - 1, z - s), (above(s), 2 * s, z + s)]

    def guarded(flag, f):
        if flag is None:
            f()
        else:
            when(flag)(f)

    def z_recv_step(l, k, s):
        for d, (flag, slot, zs) in enumerate(groups(s)):
            def go(d=d, slot=slot, zs=zs):
                z_wait(l, k, d, s)
                if s < planes - 1:
                    when((has_up, has_down)[d])(lambda: z_copy(l, k, d, s).start())
                to_partner(l, k, slot, zs)
            guarded(flag, go)

    def a_step(l, s):
        for flag, slot, zs in groups(s):
            def go(slot=slot, zs=zs):
                i = l * slots + slot
                ref = from_a(l, slot, zs)
                arrived(ref, a_send.at[i], a_recv.at[i])
                r_copy(l, slot, zs).start()
                d_copy(l, 2, 1, slot, ref).start()
            guarded(flag, go)

    def b_step(l, s):
        for flag, slot, zs in groups(s):
            def go(slot=slot, zs=zs):
                i = l * slots + slot
                ref = from_b(l, slot, zs)
                arrived(ref, b_send.at[i], b_recv.at[i])
                d_copy(l, 2, 2, slot, ref).start()
            guarded(flag, go)

    def r_step(l, s):
        for flag, slot, zs in groups(s):
            def go(slot=slot, zs=zs):
                i = l * slots + slot
                ref = oblock(l, zs, yn, 2 * xn + h)
                arrived(ref, r_send.at[i], r_recv.at[i])
                d_copy(l, 2, 3, slot, ref).start()
            guarded(flag, go)

    def need_v(l):
        arrived(wvg.at[l, :, pl.ds(0, width // 2), :], d_send.at[0], d_recv.at[l])

    def need_last():
        mate = 2 * x + hn
        arrived(oblock(last, t, y, mate), o_send.at[0], o_recv.at[2 * mate])
        for j in range(tp):
            other = lax.rem(t + j, tp)
            arrived(oblock(last, t, yn, other), o_send.at[0], o_recv.at[2 * other + 1])

    def weights_sent():
        for l in range(layers):
            for k in range(3):
                if k < 2:
                    when(1 - same)(lambda l=l, k=k: pre_copy(l, k).wait_send())
                for s in range(planes - 1):
                    for d, flag in enumerate((has_up, has_down)):
                        ok = flag if s == 0 else flag * (below(s), above(s))[d]
                        when(ok)(lambda l=l, k=k, d=d, s=s: z_copy(l, k, d, s).wait_send())
                for s in range(planes):
                    for flag, slot, zs in groups(s):
                        guarded(flag, lambda l=l, k=k, slot=slot, zs=zs: spread_sent(l, k, slot, zs))

    def plane_sent():
        for c in range(2):
            o_pass(c).wait_send()
        for l in range(last):
            for s in range(planes):
                for flag, slot, zs in groups(s):
                    def go(l=l, slot=slot, zs=zs):
                        r_copy(l, slot, zs).wait_send()
                        d_copy(l, 2, 1, slot, from_a(l, slot, zs)).wait_send()
                        d_copy(l, 2, 2, slot, from_b(l, slot, zs)).wait_send()
                        d_copy(l, 2, 3, slot, oblock(l, zs, yn, 2 * xn + h)).wait_send()
                    guarded(flag, go)

    def cols(owner):
        return pl.ds(pl.multiple_of(owner * feats, feats), feats)

    tcols = cols(t)

    half_rows = rows // 2

    def hcols(owner, part):
        return stream.at[pl.ds(halo + part * half_rows, half_rows), cols(owner)]

    def tok_copy(j, p):
        dev = ((sp, 2 * x + y), (sp, 2 * xn + y), (spn, 2 * x + y))[j]
        return rcopy(tok.at[pl.ds(p * half_rows, half_rows), :], hcols(t, p),
                     tok_send.at[2 * j + p], tok_recv.at[2 * t + p], dev)

    def tok_start(j):
        tok_copy(j, 0).start()
        tok_copy(j, 1).start()

    def tok_pass(j):
        owner, p, dev = (
            (2 * xn + yn, 0, ydev), (2 * x + yn, 0, xdev),
            (2 * x + yn, 1, xdev), (2 * x + y, 1, xdev))[j]
        ref = hcols(owner, p)
        return rcopy(ref, ref, tok_send.at[6 + j], tok_recv.at[2 * owner + p], dev)

    def tok_starts():
        when(1 - same)(lambda: tok_start(0))
        tok_start(1)

        @when(same)
        def _():
            stream[pl.ds(halo, rows), tcols] = tok[...]

    def tok_arrived(owner, p):
        arrived(hcols(owner, p), tok_send.at[0], tok_recv.at[2 * owner + p])

    def tok_relay(step):
        @when(same)
        def _():
            if step == 0:
                tok_arrived(2 * xn + yn, 0)
                tok_pass(0).start()

        @when(1 - same)
        def _():
            if step == 0:
                tok_arrived(2 * x + yn, 0)
                tok_pass(1).start()
            elif step == 1:
                tok_arrived(2 * x + yn, 1)
                tok_pass(2).start()
            else:
                tok_arrived(2 * x + y, 1)
                tok_pass(3).start()

    def tok_waits():
        @when(same)
        def _():
            tok_arrived(2 * xn + yn, 1)
            for p in range(2):
                tok_arrived(2 * x + hn, p)
                tok_arrived(2 * xn + y, p)

        @when(1 - same)
        def _():
            tok_arrived(2 * x + y, 0)
            for p in range(2):
                tok_arrived(2 * xn + yn, p)
                tok_arrived(2 * xn + y, p)

    zh_to = y * has_up + yn * has_down
    zh_from = hn * has_down + h * has_up

    def edge(owner_cols, side):
        r = pl.ds(pl.multiple_of(side * (halo + rows), grain), halo)
        return stream.at[r, owner_cols]

    def zh_copy():
        src = tok.at[pl.ds(pl.multiple_of(y * (rows - halo), grain), halo), :]
        return rcopy(src, edge(tcols, yn), zh_send.at[0], zh_recv.at[t],
                     (sp + 4 * y - 2, 2 * x + yn))

    def half_cols(xx):
        return pl.ds(pl.multiple_of(xx * 2 * feats, feats), 2 * feats)

    def hp_copy(j):
        ref = edge(half_cols(xn if j == 2 else x), h)
        return rcopy(ref, ref, hp_send.at[j], hp_recv.at[j], xdev if j == 0 else ydev)

    def halo_pass():
        @when(zh_from * (1 - same))
        def _():
            for c in range(2):
                arrived(edge(cols(2 * x + c), h), zh_send.at[0], zh_recv.at[2 * x + c])
            hp_copy(0).start()
            hp_copy(1).start()

        @when(1 - zh_from)
        def _():
            stream[pl.ds(pl.multiple_of(h * (halo + rows), grain), halo), :] = jnp.zeros((halo, width), jnp.bfloat16)

    def halo_pass_on():
        @when(zh_from * (1 - same))
        def _():
            arrived(edge(half_cols(xn), h), hp_send.at[0], hp_recv.at[0])
            hp_copy(2).start()

    def halo_waits():
        @when(zh_from * same)
        def _():
            arrived(edge(half_cols(x), h), hp_send.at[0], hp_recv.at[1])
            arrived(edge(half_cols(xn), h), hp_send.at[0], hp_recv.at[2])

    def ih_copy():
        src = stream.at[pl.ds(pl.multiple_of(hn * rows + h * halo, grain), halo), :]
        dst = stream.at[pl.ds(pl.multiple_of(h * (halo + rows), grain), halo), :]
        return rcopy(src, dst, ih_send.at[0], ih_recv.at[0], partner)

    def ih_wait():
        ref = stream.at[pl.ds(pl.multiple_of(hn * (halo + rows), grain), halo), :]
        arrived(ref, ih_send.at[0], ih_recv.at[0])

    def par_copy(i):
        a, b = ((taps_in, taps), (bias_in, bias))[i]
        return rcopy(a, b, par_send.at[i], par_recv.at[i], partner)

    def ln_copy(i, j):
        a, b = ((lng_in, lng), (lns_in, lns))[i]
        return rcopy(a, b.at[t], ln_send.at[3 * i + j - 1], ln_recv.at[tp * i + t],
                     (sp, lax.rem(t + j, tp)))

    def params_start():
        for i in range(2):
            when(same)(lambda i=i: par_copy(i).start())
            for j in range(1, tp):
                ln_copy(i, j).start()


    def in_copies():
        return [
            pltpu.make_async_copy(a, b, in_sem.at[i])
            for i, (a, b) in enumerate((
                (tok_in, tok), (gain_hbm, gain_in), (lng_in, lng.at[t]), (lns_in, lns.at[t]),
                (taps_in, taps), (bias_in, bias)))
        ]

    def in_start():
        for i, c in enumerate(in_copies()):
            if i < 4:
                c.start()
            else:
                when(same)(lambda c=c: c.start())

    def out_copy(i):
        r0, size = piece(last, i)
        r = pl.ds(r0, size)
        return pltpu.make_async_copy(result.at[r, :], out.at[r, :], out_sem.at[i])

    def params_wait():
        for i, c in enumerate(in_copies()):
            if i >= 4:
                when(same)(lambda c=c: c.wait())
            elif i > 0:
                c.wait()
        for i, ref in enumerate((taps, bias)):
            when(1 - same)(lambda i=i, ref=ref: arrived(ref, par_send.at[i], par_recv.at[i]))
        for i, ref in enumerate((lng, lns)):
            for j in range(1, tp):
                other = lax.rem(t + j, tp)
                arrived(ref.at[other], ln_send.at[0], ln_recv.at[tp * i + other])

    def small_sent():
        for p in range(2):
            when(1 - same)(lambda p=p: tok_copy(0, p).wait_send())
            tok_copy(1, p).wait_send()
            tok_copy(2, p).wait_send()
        when(zh_to)(lambda: zh_copy().wait_send())
        for i in range(2):
            when(same)(lambda i=i: par_copy(i).wait_send())
            for j in range(1, tp):
                ln_copy(i, j).wait_send()

    def stream_sent():
        when(same)(lambda: tok_pass(0).wait_send())

        @when(1 - same)
        def _():
            for j in range(1, 4):
                tok_pass(j).wait_send()

        @when(zh_from * (1 - same))
        def _():
            for j in range(3):
                hp_copy(j).wait_send()
        ih_copy().wait_send()

    cb_own = 2 * x + y
    cb_a, cb_b, cb_d = 2 * ax + ay, 2 * bx + by, 2 * xn + yn

    def piece(l, i):
        total = window - 2 * grain * (l + 1)
        first = total - rows // 2
        return i * first, total - first if i else first

    def cblock(l, i, cb):
        r0, size = piece(l, i)
        return cv.at[l, cb, pl.ds(r0, size), :]

    def cv_copy(l, i, j):
        ref = cblock(l, i, cb_a if j == 2 else cb_own)
        s, r = ((ca_send, ca_recv), (cb_send, cb_recv), (cr_send, cr_recv))[j]
        return rcopy(ref, ref, s.at[2 * l + i], r.at[2 * l + i], adev if j == 0 else bdev)

    def cv_start(l, i):
        cv_copy(l, i, 0).start()
        cv_copy(l, i, 1).start()

    def cv_relay(l, i):
        arrived(cblock(l, i, cb_a), ca_send.at[2 * l + i], ca_recv.at[2 * l + i])
        cv_copy(l, i, 2).start()

    def cv_waits(l, i):
        arrived(cblock(l, i, cb_b), cb_send.at[2 * l + i], cb_recv.at[2 * l + i])
        arrived(cblock(l, i, cb_d), cr_send.at[2 * l + i], cr_recv.at[2 * l + i])

    def lblock(i, cb):
        r0, size = piece(last, i)
        return cv2.at[cb, pl.ds(r0, size), :]

    def l_copy(i, j):
        src, cb, dev = (
            (cblock(last, i, cb_own), cb_own, ydev),
            (cblock(last, i, cb_own), cb_own, xdev),
            (lblock(i, 2 * x + yn), 2 * x + yn, xdev),
        )[j]
        return rcopy(src, lblock(i, cb), l_send.at[3 * i + j], l_recv.at[3 * i + j], dev)

    def p_copy(i, j):
        cb = (cb_own, 2 * x + yn, 2 * xn + y, 2 * xn + yn)[j]
        src = cblock(last, i, cb) if j == 0 else lblock(i, cb)
        return rcopy(src, lblock(i, cb), p_send.at[tp * i + j], p_recv.at[tp * i + j], partner)

    def last_start(i):
        r0, size = piece(last, i)
        when(1 - same)(lambda: l_copy(i, 0).start())

        @when(same)
        def _():
            l_copy(i, 1).start()
            p_copy(i, 0).start()
            cv2[cb_own, r0:r0 + size, :] = cv[last, cb_own, r0:r0 + size, :]

    def last_relay(i):
        @when(same)
        def _():
            arrived(lblock(i, 2 * x + yn), l_send.at[0], l_recv.at[3 * i])
            l_copy(i, 2).start()
            p_copy(i, 1).start()

    def last_waits(i):
        @when(same)
        def _():
            for j in (1, 2):
                cb = 2 * xn + (y if j == 1 else yn)
                arrived(lblock(i, cb), l_send.at[0], l_recv.at[3 * i + j])
                p_copy(i, j + 1).start()

        @when(1 - same)
        def _():
            for j, cb in enumerate((2 * x + yn, 2 * x + y, 2 * xn + yn, 2 * xn + y)):
                arrived(lblock(i, cb), p_send.at[0], p_recv.at[tp * i + j])

    def conv_sent():
        for i in range(2):
            for l in range(last):
                for j in range(3):
                    cv_copy(l, i, j).wait_send()
            when(1 - same)(lambda i=i: l_copy(i, 0).wait_send())

            @when(same)
            def _(i=i):
                l_copy(i, 1).wait_send()
                l_copy(i, 2).wait_send()
                for j in range(tp):
                    p_copy(i, j).wait_send()

    def res_copy():
        src = stream.at[pl.ds(halo, rows), cols(2 * x + hn)]
        return rcopy(src, resid, res_send.at[0], res_recv.at[0], partner)

    def res_start():
        @when(same)
        def _():
            res_copy().start()
            resid[...] = stream[pl.ds(halo, rows), tcols]

    def res_wait():
        when(1 - same)(lambda: arrived(resid, res_send.at[0], res_recv.at[0]))

    first_row = (2 * z + h) * rows - halo
    total_rows = n * rows

    def over_rows(start, size, block, f):
        def step(i, carry):
            f(pl.ds(pl.multiple_of(start + i * block, grain), block))
            return carry

        lax.fori_loop(0, size // block, step, 0)

    def chunk(layer, i):
        r0, size = piece(layer - 1, i)
        return grain * layer + r0, size

    def normalize(layer, i):
        w0, size = chunk(layer, i)
        block = 2 * grain

        def squares(r):
            total = jnp.zeros((block, lanes), jnp.float32)
            for c in range(width // lanes):
                v = stream[r, c * lanes:(c + 1) * lanes].astype(jnp.float32)
                total = total + v * v
            rowa[r, :] = total

        def scaled(r):
            scale = rowa[r, :]
            for c in range(width // lanes):
                lane = slice(c * lanes, (c + 1) * lanes)
                v = stream[r, lane].astype(jnp.float32)
                normed[r, lane] = (v * scale * gain_in[layer:layer + 1, lane]).astype(jnp.bfloat16)

        over_rows(w0, size, block, squares)
        mean = jnp.sum(rowa[w0:w0 + size, :], axis=-1, keepdims=True) / width
        rowa[w0:w0 + size, :] = jnp.broadcast_to(lax.rsqrt(mean + norm_floor), (size, lanes))
        over_rows(w0, size, block, scaled)

    def project(layer, i):
        w0, size = chunk(layer, i)
        value = jnp.dot(normed[w0:w0 + size, :], wvg[layer, 0], preferred_element_type=jnp.float32)
        gate = jnp.dot(normed[w0:w0 + size, :], wvg[layer, 1], preferred_element_type=jnp.float32)
        g = (value * (0.5 + 0.5 * jnp.tanh(0.5 * gate))).astype(jnp.bfloat16).astype(jnp.float32)
        row = lax.broadcasted_iota(jnp.int32, (size, lch), 0) + (first_row + w0)
        g = jnp.where(jnp.logical_and(row >= 0, row < total_rows), g, 0.0)
        for b in range(per_side):
            gated[b, w0:w0 + size, :] = g[:, b * lanes:(b + 1) * lanes]

    def convolve(layer, i):
        r0, size = piece(layer, i)
        start = grain * (layer + 1)
        cut = -(-size // 2 // grain) * grain
        for c0, part in ((r0, cut), (r0 + cut, size - cut)):
            def lane_block(b, carry, c0=c0, part=part):
                lane = pl.ds(pl.multiple_of(b * lanes, lanes), lanes)
                total = jnp.zeros((part, lanes), jnp.float32) + bias[layer:layer + 1, lane]
                for k in range(ntaps):
                    first = start + c0 + k - reach
                    total = total + taps[layer, k:k + 1, lane] * gated[b, first:first + part, :]
                cv[layer, cb_own, c0:c0 + part, lane] = total.astype(jnp.bfloat16)
                return carry

            lax.fori_loop(0, per_side, lane_block, 0)

    def activate(layer, i):
        r0, size = piece(layer, i)
        block = 2 * grain if size % (2 * grain) == 0 else grain
        parts = [(b, c) for b in range(tp) for c in range(per_side)]

        def load(b, c, r):
            lane = slice(c * lanes, (c + 1) * lanes)
            return (cv[layer, b, r, lane] if layer < last else cv2[b, r, lane]).astype(jnp.float32)

        def sums(r):
            s1 = jnp.zeros((block, lanes), jnp.float32)
            s2 = jnp.zeros((block, lanes), jnp.float32)
            for b, c in parts:
                v = load(b, c, r)
                s1 = s1 + v
                s2 = s2 + v * v
            rowa[r, :] = s1
            rowb[r, :] = s2

        def apply(r):
            scale, shift = rowa[r, :], rowb[r, :]
            for b, c in parts:
                lane = slice(c * lanes, (c + 1) * lanes)
                u = (load(b, c, r) - shift) * scale
                u = 0.5 * (u * lng[b, layer:layer + 1, lane] + lns[b, layer:layer + 1, lane])
                act[r, b * lch + c * lanes:b * lch + (c + 1) * lanes] = (u + u * jnp.tanh(u)).astype(jnp.bfloat16)

        over_rows(r0, size, block, sums)
        rows_ = slice(r0, r0 + size)
        average = jnp.sum(rowa[rows_, :], axis=-1, keepdims=True) / chans
        spread_ = jnp.sum(rowb[rows_, :], axis=-1, keepdims=True) / chans - average * average
        rowa[rows_, :] = jnp.broadcast_to(lax.rsqrt(spread_ + norm_floor), (size, lanes))
        rowb[rows_, :] = jnp.broadcast_to(average, (size, lanes))
        over_rows(r0, size, block, apply)

    def expand_wait(layer, s):
        for flag, slot, zs in groups(s):
            sem = d_recv.at[layers + layer * slots + slot]
            guarded(flag, lambda sem=sem: arrived(wo.at[layer, 0], d_send.at[0], sem))

    def expand(layer, s, pieces=(0, 1)):
        for flag, slot, zs in groups(s):
            def go(slot=slot, zs=zs):
                def step(j, carry):
                    c = pl.ds(pl.multiple_of((2 * zs + j) * ocols, ocols), ocols)
                    for i in pieces:
                        r0, size = piece(layer, i)
                        w0 = grain * (layer + 1) + r0
                        add = jnp.dot(act[r0:r0 + size, :], wo[layer, 2 * zs + j], preferred_element_type=jnp.float32)
                        stream[w0:w0 + size, c] = (stream[w0:w0 + size, c].astype(jnp.float32) + add).astype(jnp.bfloat16)
                    return carry

                lax.fori_loop(0, 2, step, 0)
            guarded(flag, go)

    def finish(i):
        r0, size = piece(last, i)
        for j in range(per_out):
            c = slice(j * ocols, (j + 1) * ocols)
            add = jnp.dot(act[r0:r0 + size, :], wo[last, per_out * t + j], preferred_element_type=jnp.float32)
            result[r0:r0 + size, c] = (resid[r0:r0 + size, c].astype(jnp.float32) + add).astype(jnp.bfloat16)

    barrier = pltpu.get_barrier_semaphore()
    in_start()
    for l in range(layers):
        for k in range(3):
            if k < 2:
                when(same)(lambda l=l, k=k: local_copy(l, k).start())
            else:
                local_copy(l, k).start()
    for ds in range(2):
        for j in range(tp):
            if ds or j:
                pl.semaphore_signal(barrier, inc=1, device_id=((sp, spn)[ds], lax.rem(t + j, tp)), device_id_type=MESH)
    for flag, step in ((has_up, 2), (has_down, -2)):
        @when(flag)
        def _(step=step):
            for c in range(2):
                pl.semaphore_signal(barrier, inc=1, device_id=(sp + step, 2 * x + c), device_id_type=MESH)
    pl.semaphore_wait(barrier, 2 * tp - 1 + 2 * (has_up + has_down))
    in_copies()[0].wait()

    def pre_start(l):
        for k in range(2):
            when(1 - same)(lambda k=k: pre_copy(l, k).start())

    pre_start(0)
    when(zh_to)(lambda: zh_copy().start())
    tok_starts()
    halo_pass()
    when(1 - same)(lambda: tok_start(2))
    params_start()
    own_start(0, 0)
    own_start(0, 1)
    z_recv_step(0, 0, 1)
    when(same)(lambda: tok_start(2))
    z_recv_step(0, 1, 1)
    tok_relay(0)
    own_start(0, 2)
    halo_pass_on()
    tok_relay(1)
    z_recv_step(0, 0, 2)
    tok_relay(2)
    pre_start(1)
    z_recv_step(0, 1, 2)
    spread(0, 0)
    z_recv_step(0, 2, 1)
    tok_waits()
    ih_copy().start()
    halo_waits()
    ih_wait()
    params_wait()
    normalize(0, 0)
    normalize(0, 1)
    z_recv_step(0, 0, 3)
    z_recv_step(0, 1, 3)
    own_start(1, 0)
    own_start(1, 1)
    spread(0, 1)
    need_v(0)
    for i in range(2):
        project(0, i)
        convolve(0, i)
        cv_start(0, i)
        if i == 0:
            a_step(0, 0)
            z_recv_step(0, 2, 2)

    for layer in range(last):
        after = layer + 1
        z_recv_step(after, 0, 1)
        cv_relay(layer, 0)
        z_recv_step(after, 1, 1)
        cv_relay(layer, 1)
        spread(layer, 2)
        z_recv_step(layer, 2, 3)
        spread(layer, 3)
        if layer == 0:
            pre_start(2)
        z_recv_step(after, 0, 2)
        b_step(layer, 0)
        a_step(layer, 1)
        cv_waits(layer, 0)
        activate(layer, 0)
        z_recv_step(after, 1, 2)
        own_start(after, 2)
        cv_waits(layer, 1)
        activate(layer, 1)
        r_step(layer, 0)
        a_step(layer, 2)
        if layer == 0:
            stream_sent()
        expand_wait(layer, 0)
        expand(layer, 0)
        z_recv_step(after, 0, 3)
        b_step(layer, 1)
        a_step(layer, 3)
        r_step(layer, 1)
        spread(after, 0)
        z_recv_step(after, 1, 3)
        z_recv_step(after, 2, 1)
        if after < last:
            own_start(after + 1, 0)
            own_start(after + 1, 1)
        expand_wait(layer, 1)
        expand(layer, 1)
        b_step(layer, 2)
        if after == last:
            spread(last, 1)
            o_relay(0)
        r_step(layer, 2)
        expand_wait(layer, 2)
        expand(layer, 2)
        b_step(layer, 3)
        need_v(after)
        r_step(layer, 3)
        if after < last:
            spread(after, 1)
            z_recv_step(after, 2, 2)
        else:
            o_relay(1)
        expand_wait(layer, 3)
        for i in range(2):
            expand(layer, 3, (i,))
            normalize(after, i)
            project(after, i)
            convolve(after, i)
            if after < last:
                cv_start(after, i)
                if i == 0:
                    a_step(after, 0)
            else:
                last_start(i)
                if i == 0:
                    z_recv_step(last, 2, 2)
                    spread(last, 2)
    res_start()
    last_relay(0)
    z_recv_step(last, 2, 3)
    last_relay(1)
    spread(last, 3)
    o_relay(2)
    res_wait()
    last_waits(0)
    activate(last, 0)
    last_waits(1)
    o_relay(3)
    activate(last, 1)
    need_last()
    for i in range(2):
        finish(i)
        out_copy(i).start()
    weights_sent()
    plane_sent()
    small_sent()
    conv_sent()
    when(same)(lambda: res_copy().wait_send())
    for i in range(2):
        out_copy(i).wait()


def fused_call(mesh, *args):
    tokens, norm_gain, w_value, w_gate, conv_taps, conv_bias, ln_gain, ln_shift, w_out = args
    n, tp = mesh.shape["sp"], mesh.shape["tp"]
    layers, ntaps, lch = conv_taps.shape
    rows, feats = tokens.shape
    width, chans = feats * tp, lch * tp
    planes = n // 2
    slots = 2 * planes - 1
    halo = 16 * layers
    window = rows + 2 * halo
    most = window - 32
    dims = (n, tp, layers, ntaps, rows, width, chans)
    anys = pl.BlockSpec(memory_space=pl.ANY)
    bf, f32 = jnp.bfloat16, jnp.float32
    dma = lambda k: pltpu.SemaphoreType.DMA((k,))
    pairs = lambda k: [dma(k), dma(k)]
    wide = (layers - 1) * slots
    return pl.pallas_call(
        functools.partial(fused, dims),
        out_shape=jax.ShapeDtypeStruct((rows, feats), bf),
        in_specs=[anys] * 9,
        out_specs=anys,
        scratch_shapes=[
            pltpu.VMEM((rows, feats), bf),
            pltpu.VMEM(norm_gain.shape, f32),
            pltpu.VMEM((rows, feats), bf),
            pltpu.VMEM((layers, 2, width, lch), bf),
            pltpu.VMEM((layers, n, chans, width // n), bf),
            pltpu.VMEM(conv_taps.shape, f32),
            pltpu.VMEM(conv_bias.shape, f32),
            pltpu.VMEM((tp,) + ln_gain.shape, f32),
            pltpu.VMEM((tp,) + ln_shift.shape, f32),
            pltpu.VMEM((window, width), bf),
            pltpu.VMEM((window, width), bf),
            pltpu.VMEM((lch // 128, window, 128), f32),
            pltpu.VMEM((layers, tp, most, lch), bf),
            pltpu.VMEM((tp, rows, lch), bf),
            pltpu.VMEM((most, chans), bf),
            pltpu.VMEM((rows, feats), bf),
            pltpu.VMEM((window, 128), f32),
            pltpu.VMEM((window, 128), f32),
            dma(3 * layers), dma(6), dma(2),
            *pairs(2 * layers),
            *pairs(2 * layers * 3 * (planes - 1)),
            dma(layers * 3 * slots * 2), dma(layers * (1 + slots)),
            *pairs(wide), *pairs(wide), *pairs(wide),
            *pairs(2 * slots), dma(2),
            dma(10), dma(2 * tp), *pairs(tp), *pairs(3), *pairs(1),
            *pairs(2), dma(6), dma(2 * tp),
            *pairs(2 * layers), *pairs(2 * layers), *pairs(2 * layers),
            *pairs(6), *pairs(2 * tp), *pairs(1),
        ],
        compiler_params=pltpu.CompilerParams(
            collective_id=0, has_side_effects=True, vmem_limit_bytes=60 * 1024 * 1024),
    )(tokens, norm_gain, w_value, w_gate, w_out, conv_taps, conv_bias, ln_gain, ln_shift)


def fits(mesh, tokens, conv_taps, w_out):
    n, tp = mesh.shape["sp"], mesh.shape["tp"]
    layers, ntaps, lch = conv_taps.shape
    rows, feats = tokens.shape
    return (tp == 4 and n == 2 * tp and ntaps % 2 == 1 and ntaps // 2 < 16 and layers > 1
            and w_out.shape[2] % 128 == 0 and lch % 128 == 0 and feats % 128 == 0
            and feats == 2 * w_out.shape[2]
            and rows % 64 == 0 and rows >= 32 * layers and rows <= 512
            and layers * w_out.shape[1] * w_out.shape[2] * n * 12 <= 20 * 1024 * 1024)


def solution(mesh):
    placed = (
        P("sp", "tp"),
        P(),
        P(None, "sp", "tp"),
        P(None, "sp", "tp"),
        P(None, None, "tp"),
        P(None, "tp"),
        P(None, "tp"),
        P(None, "tp"),
        P(None, "tp", "sp"),
    )

    def run(*args):
        if fits(mesh, args[0], args[4], args[8]):
            return fused_call(mesh, *args)
        return body(*args)

    return jax.shard_map(run, mesh=mesh, in_specs=placed, out_specs=P("sp", "tp"), check_vma=False)
```

```python
import functools

import jax
import jax.numpy as jnp
from jax import lax
from jax.experimental import pallas as pl
from jax.experimental.pallas import tpu as pltpu
from jax.sharding import PartitionSpec as P

MESH = pl.DeviceIdType.MESH

norm_floor = 0.01


def with_halo(array, sides, width):
    for axis, dim in sides:
        size, length = (lax.axis_size(axis), array.shape[dim])
        up = [(i, (i + 1) % size) for i in range(size - 1)]
        down = [(j, i) for i, j in up]
        last = lax.slice_in_dim(array, length - width, length, axis=dim)
        first = lax.slice_in_dim(array, 0, width, axis=dim)
        before = lax.ppermute(last, axis, up)
        after = lax.ppermute(first, axis, down)
        array = jnp.concatenate([before, array, after], axis=dim)
    return array


def body(tokens, norm_gain, w_value, w_gate, conv_taps, conv_bias, ln_gain, ln_shift, w_out):
    stream = tokens
    layer_count = w_value.shape[0]
    reach = conv_taps.shape[1] // 2
    local_channels = w_value.shape[2]
    channels = local_channels * lax.axis_size("tp")
    tok_rows = tokens.shape[0]
    whole_value, whole_gate = (
        lax.all_gather(w_value, "sp", axis=1, tiled=True),
        lax.all_gather(w_gate, "sp", axis=1, tiled=True),
    )
    whole_out = lax.all_gather(w_out, "sp", axis=2, tiled=True)
    for layer_index in range(layer_count):
        whole_rows = lax.all_gather(stream, "tp", axis=1, tiled=True)
        rows_f32 = whole_rows.astype(jnp.float32)
        scale_rows = lax.rsqrt(jnp.mean(rows_f32 * rows_f32, axis=-1, keepdims=True) + norm_floor)
        normed = (rows_f32 * scale_rows * norm_gain[layer_index]).astype(jnp.bfloat16)
        value_rows = jnp.dot(normed, whole_value[layer_index], preferred_element_type=jnp.float32)
        gate_rows = jnp.dot(normed, whole_gate[layer_index], preferred_element_type=jnp.float32)
        gated_input = (value_rows * jax.nn.sigmoid(gate_rows)).astype(jnp.bfloat16)
        padded = with_halo(gated_input, (("sp", 0),), reach)
        padded = padded.astype(jnp.float32)
        convolved = jnp.zeros((tok_rows, local_channels), jnp.float32) + conv_bias[layer_index]
        for offset in range(2 * reach + 1):
            convolved = (
                convolved + conv_taps[layer_index, offset] * padded[offset : offset + tok_rows]
            )
        moments = lax.psum(
            (
                jnp.sum(convolved, axis=-1, keepdims=True),
                jnp.sum(convolved * convolved, axis=-1, keepdims=True),
            ),
            "tp",
        )
        average = moments[0] / channels
        spread = moments[1] / channels - average * average
        activated = jax.nn.silu(
            (convolved - average) * lax.rsqrt(spread + norm_floor) * ln_gain[layer_index]
            + ln_shift[layer_index]
        ).astype(jnp.bfloat16)
        partial_rows = jnp.dot(
            activated, whole_out[layer_index], preferred_element_type=jnp.float32
        )
        summed = lax.psum_scatter(
            partial_rows.astype(jnp.bfloat16), "tp", scatter_dimension=1, tiled=True
        ).astype(jnp.float32)
        stream = (stream.astype(jnp.float32) + summed).astype(jnp.bfloat16)
    return stream


def fused(
    dims,
    tok_in, gain_hbm, wv_in, wg_in, wo_in, taps_in, bias_in, lng_in, lns_in,
    out,
    tok, gain_in, result, wvg, wo, taps, bias, lng, lns, stream, normed, gated, cv, cv2, act, resid, rowa, rowb,
    loc_sem, in_sem, out_sem, pre_send, pre_recv, z_send, z_recv, d_send, d_recv,
    a_send, a_recv, b_send, b_recv, r_send, r_recv, o_send, o_recv, op_send,
    tok_send, tok_recv, zh_send, zh_recv, hp_send, hp_recv, ih_send, ih_recv,
    par_send, par_recv, ln_send, ln_recv,
    ca_send, ca_recv, cb_send, cb_recv, cr_send, cr_recv,
    l_send, l_recv, p_send, p_recv, res_send, res_recv,
):
    n, tp, layers, ntaps, rows, width, chans = dims
    planes = n // 2
    feats = width // tp
    lch = chans // tp
    krows = width // n
    ocols = width // n
    reach = ntaps // 2
    grain = 16
    halo = grain * layers
    window = rows + 2 * halo
    slots = 2 * planes - 1
    last = layers - 1
    lanes = 128
    per_side = lch // lanes
    per_out = feats // ocols
    swapped = 0

    sp = lax.axis_index("sp")
    t = lax.axis_index("tp")
    z, y = sp // 2, lax.rem(sp, 2)
    x, h = t // 2, lax.rem(t, 2)
    xn, yn, hn = 1 - x, 1 - y, 1 - h
    same = 1 - (y + h - 2 * y * h)
    spn = 2 * z + yn
    has_up, has_down = 1 - (z + 1) // planes, jnp.minimum(z, 1)

    partner = (sp, 2 * x + hn)
    xdev = (sp, 2 * xn + h)
    ydev = (spn, t)
    ax, ay = hn * xn + h * x, hn * y + h * yn
    bx, by = hn * x + h * xn, hn * yn + h * y
    adev = (2 * z + ay, 2 * ax + h)
    bdev = (2 * z + by, 2 * bx + h)

    def route(l, slot):
        if (slot + 1) // 2 < swapped:
            return (x, yn), ydev, (xn, y), xdev
        return (ax, ay), adev, (bx, by), bdev

    def rcopy(src, dst, ssem, rsem, dev):
        return pltpu.make_async_remote_copy(
            src_ref=src, dst_ref=dst, send_sem=ssem, recv_sem=rsem,
            device_id=dev, device_id_type=MESH)

    def arrived(ref, ssem, rsem):
        rcopy(ref, ref, ssem, rsem, partner).wait_recv()

    def when(flag):
        return pl.when(flag == 1)

    def vblock(l, k, zs, c):
        r = pl.ds(pl.multiple_of((2 * zs + c) * krows, krows), krows)
        return wvg.at[l, k, r, :]

    def oblock(l, zs, yy, cb):
        r = pl.ds(pl.multiple_of(cb * lch, lch), lch)
        return wo.at[l, 2 * zs + yy, r, :]

    def item(l, k, zs):
        return vblock(l, k, zs, h) if k < 2 else oblock(l, zs, y, t)

    def local_copy(l, k):
        src = (wv_in, wg_in, wo_in)[k].at[l]
        return pltpu.make_async_copy(src, item(l, k, z), loc_sem.at[3 * l + k])

    def pre_copy(l, k):
        src = (wv_in, wg_in)[k].at[l]
        i = 2 * l + k
        return rcopy(src, vblock(l, k, z, y), pre_send.at[i], pre_recv.at[i], (spn, 2 * x + hn))

    def z_copy(l, k, d, s):
        zs = z - s if d == 0 else z + s
        ref = item(l, k, zs)
        i = ((d * layers + l) * 3 + k) * (planes - 1) + s
        return rcopy(ref, ref, z_send.at[i], z_recv.at[i], (sp + (2 if d == 0 else -2), t))

    def z_wait(l, k, d, s):
        zs = z - s if d == 0 else z + s
        i = ((d * layers + l) * 3 + k) * (planes - 1) + s - 1
        arrived(item(l, k, zs), z_send.at[i], z_recv.at[i])

    def d_copy(l, k, src_kind, slot, ref):
        i = ((l * 3 + k) * slots + slot) if src_kind == 0 else (
            layers * 3 * slots + ((l * 3) + src_kind - 1) * slots + slot)
        return rcopy(ref, ref, d_send.at[i], d_recv.at[l if k < 2 else layers + l * slots + slot], partner)

    def a_copy(l, slot, zs):
        ref, i = oblock(l, zs, y, t), l * slots + slot
        return rcopy(ref, ref, a_send.at[i], a_recv.at[i], route(l, slot)[1])

    def b_copy(l, slot, zs):
        ref, i = oblock(l, zs, y, t), l * slots + slot
        return rcopy(ref, ref, b_send.at[i], b_recv.at[i], route(l, slot)[3])

    def from_a(l, slot, zs):
        px, py = route(l, slot)[0]
        return oblock(l, zs, py, 2 * px + h)

    def from_b(l, slot, zs):
        px, py = route(l, slot)[2]
        return oblock(l, zs, py, 2 * px + h)

    def r_copy(l, slot, zs):
        ref, i = from_a(l, slot, zs), l * slots + slot
        return rcopy(ref, ref, r_send.at[i], r_recv.at[i], route(l, slot)[3])

    def o_copy(slot, rel, zs):
        ref, i = oblock(last, zs, y, t), 2 * slot + rel
        return rcopy(ref, ref, o_send.at[i], o_recv.at[2 * t + rel],
                     (sp if rel == 0 else spn, zs))

    def differs(a, b):
        return jnp.minimum(jnp.abs(a - b), 1)

    def to_partner(l, k, slot, zs):
        if k < 2 or l < last:
            d_copy(l, k, 0, slot, item(l, k, zs)).start()

    def spread(l, s):
        for flag, slot, zs in groups(s):
            def go(slot=slot, zs=zs):
                if l < last:
                    a_copy(l, slot, zs).start()
                    b_copy(l, slot, zs).start()
                else:
                    when(differs(zs, t))(lambda: o_copy(slot, 0, zs).start())
                    far = 1 if s == planes - 1 else 1 - differs(zs // 2, x)
                    when(far)(lambda: o_copy(slot, 1, zs).start())
            guarded(flag, go)

    def o_pass(c):
        owner = 2 * xn + c
        ref = oblock(last, t, y, owner)
        return rcopy(ref, ref, op_send.at[c], o_recv.at[2 * owner + 1], ydev)

    def o_relay(s):
        @when(1 - differs(jnp.abs(z - t), s))
        def _():
            for c in range(2):
                owner = 2 * xn + c
                arrived(oblock(last, t, y, owner), o_send.at[0], o_recv.at[2 * owner])
                if s < planes - 1:
                    o_pass(c).start()

    def spread_sent(l, k, slot, zs):
        if k < 2:
            d_copy(l, k, 0, slot, item(l, k, zs)).wait_send()
        elif l < last:
            a_copy(l, slot, zs).wait_send()
            b_copy(l, slot, zs).wait_send()
            d_copy(l, k, 0, slot, item(l, k, zs)).wait_send()
        else:
            when(differs(zs, t))(lambda: o_copy(slot, 0, zs).wait_send())
            far = 1 if slot > slots - 3 else 1 - differs(zs // 2, x)
            when(far)(lambda: o_copy(slot, 1, zs).wait_send())

    def own_start(l, k):
        if k < 2:
            when(same)(lambda: local_copy(l, k).wait())

            @when(1 - same)
            def _():
                i = 2 * l + k
                arrived(item(l, k, z), pre_send.at[i], pre_recv.at[i])
        else:
            local_copy(l, k).wait()
        when(has_up)(lambda: z_copy(l, k, 0, 0).start())
        when(has_down)(lambda: z_copy(l, k, 1, 0).start())
        to_partner(l, k, 0, z)

    def below(s):
        return jnp.minimum(z // s, 1)

    def above(s):
        return jnp.minimum((planes - 1 - z) // s, 1)

    def groups(s):
        if s == 0:
            return [(None, 0, z)]
        return [(below(s), 2 * s - 1, z - s), (above(s), 2 * s, z + s)]

    def guarded(flag, f):
        if flag is None:
            f()
        else:
            when(flag)(f)

    def z_recv_step(l, k, s):
        for d, (flag, slot, zs) in enumerate(groups(s)):
            def go(d=d, slot=slot, zs=zs):
                z_wait(l, k, d, s)
                if s < planes - 1:
                    when((has_up, has_down)[d])(lambda: z_copy(l, k, d, s).start())
                to_partner(l, k, slot, zs)
            guarded(flag, go)

    def a_step(l, s):
        for flag, slot, zs in groups(s):
            def go(slot=slot, zs=zs):
                i = l * slots + slot
                ref = from_a(l, slot, zs)
                arrived(ref, a_send.at[i], a_recv.at[i])
                r_copy(l, slot, zs).start()
                d_copy(l, 2, 1, slot, ref).start()
            guarded(flag, go)

    def b_step(l, s):
        for flag, slot, zs in groups(s):
            def go(slot=slot, zs=zs):
                i = l * slots + slot
                ref = from_b(l, slot, zs)
                arrived(ref, b_send.at[i], b_recv.at[i])
                d_copy(l, 2, 2, slot, ref).start()
            guarded(flag, go)

    def r_step(l, s):
        for flag, slot, zs in groups(s):
            def go(slot=slot, zs=zs):
                i = l * slots + slot
                ref = oblock(l, zs, yn, 2 * xn + h)
                arrived(ref, r_send.at[i], r_recv.at[i])
                d_copy(l, 2, 3, slot, ref).start()
            guarded(flag, go)

    def need_v(l):
        arrived(wvg.at[l, :, pl.ds(0, width // 2), :], d_send.at[0], d_recv.at[l])

    def need_last():
        mate = 2 * x + hn
        arrived(oblock(last, t, y, mate), o_send.at[0], o_recv.at[2 * mate])
        for j in range(tp):
            other = lax.rem(t + j, tp)
            arrived(oblock(last, t, yn, other), o_send.at[0], o_recv.at[2 * other + 1])

    def weights_sent(some):
        for l in some:
            for k in range(3):
                if k < 2:
                    when(1 - same)(lambda l=l, k=k: pre_copy(l, k).wait_send())
                for s in range(planes - 1):
                    for d, flag in enumerate((has_up, has_down)):
                        ok = flag if s == 0 else flag * (below(s), above(s))[d]
                        when(ok)(lambda l=l, k=k, d=d, s=s: z_copy(l, k, d, s).wait_send())
                for s in range(planes):
                    for flag, slot, zs in groups(s):
                        guarded(flag, lambda l=l, k=k, slot=slot, zs=zs: spread_sent(l, k, slot, zs))

    def passes_sent():
        @when(differs(jnp.abs(z - t), planes - 1))
        def _():
            for c in range(2):
                o_pass(c).wait_send()

    def plane_sent():
        for l in range(last):
            for s in range(planes):
                for flag, slot, zs in groups(s):
                    def go(l=l, slot=slot, zs=zs):
                        r_copy(l, slot, zs).wait_send()
                        d_copy(l, 2, 1, slot, from_a(l, slot, zs)).wait_send()
                        d_copy(l, 2, 2, slot, from_b(l, slot, zs)).wait_send()
                        d_copy(l, 2, 3, slot, oblock(l, zs, yn, 2 * xn + h)).wait_send()
                    guarded(flag, go)

    def cols(owner):
        return pl.ds(pl.multiple_of(owner * feats, feats), feats)

    tcols = cols(t)

    half_rows = rows // 2

    def hcols(owner, part):
        return stream.at[pl.ds(halo + part * half_rows, half_rows), cols(owner)]

    def tok_copy(j, p):
        dev = ((sp, 2 * x + y), (sp, 2 * xn + y), (spn, 2 * x + y))[j]
        return rcopy(tok.at[pl.ds(p * half_rows, half_rows), :], hcols(t, p),
                     tok_send.at[2 * j + p], tok_recv.at[2 * t + p], dev)

    def tok_start(j):
        tok_copy(j, 0).start()
        tok_copy(j, 1).start()

    def tok_pass(j):
        owner, p, dev = (
            (2 * xn + yn, 0, ydev), (2 * x + yn, 0, xdev),
            (2 * x + yn, 1, xdev), (2 * x + y, 1, xdev))[j]
        ref = hcols(owner, p)
        return rcopy(ref, ref, tok_send.at[6 + j], tok_recv.at[2 * owner + p], dev)

    def tok_starts():
        when(1 - same)(lambda: tok_start(0))
        tok_start(1)

        @when(same)
        def _():
            stream[pl.ds(halo, rows), tcols] = tok[...]

    def tok_arrived(owner, p):
        arrived(hcols(owner, p), tok_send.at[0], tok_recv.at[2 * owner + p])

    def tok_relay(step):
        @when(same)
        def _():
            if step == 0:
                tok_arrived(2 * xn + yn, 0)
                tok_pass(0).start()

        @when(1 - same)
        def _():
            if step == 0:
                tok_arrived(2 * x + yn, 0)
                tok_pass(1).start()
            elif step == 1:
                tok_arrived(2 * x + yn, 1)
                tok_pass(2).start()
            else:
                tok_arrived(2 * x + y, 1)
                tok_pass(3).start()

    def tok_waits():
        @when(same)
        def _():
            tok_arrived(2 * xn + yn, 1)
            for p in range(2):
                tok_arrived(2 * x + hn, p)
                tok_arrived(2 * xn + y, p)

        @when(1 - same)
        def _():
            tok_arrived(2 * x + y, 0)
            for p in range(2):
                tok_arrived(2 * xn + yn, p)
                tok_arrived(2 * xn + y, p)

    zh_to = y * has_up + yn * has_down
    zh_from = hn * has_down + h * has_up

    def edge(owner_cols, side):
        r = pl.ds(pl.multiple_of(side * (halo + rows), grain), halo)
        return stream.at[r, owner_cols]

    def zh_copy():
        src = tok.at[pl.ds(pl.multiple_of(y * (rows - halo), grain), halo), :]
        return rcopy(src, edge(tcols, yn), zh_send.at[0], zh_recv.at[t],
                     (sp + 4 * y - 2, 2 * x + yn))

    def half_cols(xx):
        return pl.ds(pl.multiple_of(xx * 2 * feats, feats), 2 * feats)

    def hp_copy(j):
        ref = edge(half_cols(xn if j == 2 else x), h)
        return rcopy(ref, ref, hp_send.at[j], hp_recv.at[j], xdev if j == 0 else ydev)

    def halo_pass():
        @when(zh_from * (1 - same))
        def _():
            for c in range(2):
                arrived(edge(cols(2 * x + c), h), zh_send.at[0], zh_recv.at[2 * x + c])
            hp_copy(0).start()
            hp_copy(1).start()

        @when(1 - zh_from)
        def _():
            stream[pl.ds(pl.multiple_of(h * (halo + rows), grain), halo), :] = jnp.zeros((halo, width), jnp.bfloat16)

    def halo_pass_on():
        @when(zh_from * (1 - same))
        def _():
            arrived(edge(half_cols(xn), h), hp_send.at[0], hp_recv.at[0])
            hp_copy(2).start()

    def halo_waits():
        @when(zh_from * same)
        def _():
            arrived(edge(half_cols(x), h), hp_send.at[0], hp_recv.at[1])
            arrived(edge(half_cols(xn), h), hp_send.at[0], hp_recv.at[2])

    def ih_copy():
        src = stream.at[pl.ds(pl.multiple_of(hn * rows + h * halo, grain), halo), :]
        dst = stream.at[pl.ds(pl.multiple_of(h * (halo + rows), grain), halo), :]
        return rcopy(src, dst, ih_send.at[0], ih_recv.at[0], partner)

    def ih_wait():
        ref = stream.at[pl.ds(pl.multiple_of(hn * (halo + rows), grain), halo), :]
        arrived(ref, ih_send.at[0], ih_recv.at[0])

    def par_copy(i):
        a, b = ((taps_in, taps), (bias_in, bias))[i]
        return rcopy(a, b, par_send.at[i], par_recv.at[i], partner)

    def ln_copy(i, j):
        a, b = ((lng_in, lng), (lns_in, lns))[i]
        return rcopy(a, b.at[t], ln_send.at[3 * i + j - 1], ln_recv.at[tp * i + t],
                     (sp, lax.rem(t + j, tp)))

    def params_start():
        for i in range(2):
            when(same)(lambda i=i: par_copy(i).start())
            for j in range(1, tp):
                ln_copy(i, j).start()


    def in_copies():
        return [
            pltpu.make_async_copy(a, b, in_sem.at[i])
            for i, (a, b) in enumerate((
                (tok_in, tok), (gain_hbm, gain_in), (lng_in, lng.at[t]), (lns_in, lns.at[t]),
                (taps_in, taps), (bias_in, bias)))
        ]

    def in_start():
        for i, c in enumerate(in_copies()):
            if i < 4:
                c.start()
            else:
                when(same)(lambda c=c: c.start())

    def out_copy(i):
        r0, size = piece(last, i)
        r = pl.ds(r0, size)
        return pltpu.make_async_copy(result.at[r, :], out.at[r, :], out_sem.at[i])

    def params_wait():
        for i, c in enumerate(in_copies()):
            if i >= 4:
                when(same)(lambda c=c: c.wait())
            elif i > 0:
                c.wait()
        for i, ref in enumerate((taps, bias)):
            when(1 - same)(lambda i=i, ref=ref: arrived(ref, par_send.at[i], par_recv.at[i]))
        for i, ref in enumerate((lng, lns)):
            for j in range(1, tp):
                other = lax.rem(t + j, tp)
                arrived(ref.at[other], ln_send.at[0], ln_recv.at[tp * i + other])

    def small_sent():
        for p in range(2):
            when(1 - same)(lambda p=p: tok_copy(0, p).wait_send())
            tok_copy(1, p).wait_send()
            tok_copy(2, p).wait_send()
        when(zh_to)(lambda: zh_copy().wait_send())
        for i in range(2):
            when(same)(lambda i=i: par_copy(i).wait_send())
            for j in range(1, tp):
                ln_copy(i, j).wait_send()

    def stream_sent():
        when(same)(lambda: tok_pass(0).wait_send())

        @when(1 - same)
        def _():
            for j in range(1, 4):
                tok_pass(j).wait_send()

        @when(zh_from * (1 - same))
        def _():
            for j in range(3):
                hp_copy(j).wait_send()
        ih_copy().wait_send()

    cb_own = 2 * x + y
    cb_a, cb_b, cb_d = 2 * ax + ay, 2 * bx + by, 2 * xn + yn

    def piece(l, i):
        total = window - 2 * grain * (l + 1)
        first = total - rows // 2
        return i * first, total - first if i else first

    def cblock(l, i, cb):
        r0, size = piece(l, i)
        return cv.at[l, cb, pl.ds(r0, size), :]

    def cv_copy(l, i, j):
        ref = cblock(l, i, cb_a if j == 2 else cb_own)
        s, r = ((ca_send, ca_recv), (cb_send, cb_recv), (cr_send, cr_recv))[j]
        return rcopy(ref, ref, s.at[2 * l + i], r.at[2 * l + i], adev if j == 0 else bdev)

    def cv_start(l, i):
        cv_copy(l, i, 0).start()
        cv_copy(l, i, 1).start()

    def cv_relay(l, i):
        arrived(cblock(l, i, cb_a), ca_send.at[2 * l + i], ca_recv.at[2 * l + i])
        cv_copy(l, i, 2).start()

    def cv_waits(l, i):
        arrived(cblock(l, i, cb_b), cb_send.at[2 * l + i], cb_recv.at[2 * l + i])
        arrived(cblock(l, i, cb_d), cr_send.at[2 * l + i], cr_recv.at[2 * l + i])

    def lblock(i, cb):
        r0, size = piece(last, i)
        return cv2.at[cb, pl.ds(r0, size), :]

    def l_copy(i, j):
        src, cb, dev = (
            (cblock(last, i, cb_own), cb_own, ydev),
            (cblock(last, i, cb_own), cb_own, xdev),
            (lblock(i, 2 * x + yn), 2 * x + yn, xdev),
        )[j]
        return rcopy(src, lblock(i, cb), l_send.at[3 * i + j], l_recv.at[3 * i + j], dev)

    def p_copy(i, j):
        cb = (cb_own, 2 * x + yn, 2 * xn + y, 2 * xn + yn)[j]
        src = cblock(last, i, cb) if j == 0 else lblock(i, cb)
        return rcopy(src, lblock(i, cb), p_send.at[tp * i + j], p_recv.at[tp * i + j], partner)

    def last_start(i):
        r0, size = piece(last, i)
        when(1 - same)(lambda: l_copy(i, 0).start())

        @when(same)
        def _():
            l_copy(i, 1).start()
            p_copy(i, 0).start()
            cv2[cb_own, r0:r0 + size, :] = cv[last, cb_own, r0:r0 + size, :]

    def last_relay(i):
        @when(same)
        def _():
            arrived(lblock(i, 2 * x + yn), l_send.at[0], l_recv.at[3 * i])
            l_copy(i, 2).start()
            p_copy(i, 1).start()

    def last_waits(i):
        @when(same)
        def _():
            for j in (1, 2):
                cb = 2 * xn + (y if j == 1 else yn)
                arrived(lblock(i, cb), l_send.at[0], l_recv.at[3 * i + j])
                p_copy(i, j + 1).start()

        @when(1 - same)
        def _():
            for j, cb in enumerate((2 * x + yn, 2 * x + y, 2 * xn + yn, 2 * xn + y)):
                arrived(lblock(i, cb), p_send.at[0], p_recv.at[tp * i + j])

    def conv_sent():
        for i in range(2):
            for l in range(last):
                for j in range(3):
                    cv_copy(l, i, j).wait_send()

    def last_sent():
        for i in range(2):
            when(1 - same)(lambda i=i: l_copy(i, 0).wait_send())

            @when(same)
            def _(i=i):
                l_copy(i, 1).wait_send()
                l_copy(i, 2).wait_send()
                for j in range(tp):
                    p_copy(i, j).wait_send()

    def res_copy():
        src = stream.at[pl.ds(halo, rows), cols(2 * x + hn)]
        return rcopy(src, resid, res_send.at[0], res_recv.at[0], partner)

    def res_start():
        @when(same)
        def _():
            res_copy().start()
            resid[...] = stream[pl.ds(halo, rows), tcols]

    def res_wait():
        when(1 - same)(lambda: arrived(resid, res_send.at[0], res_recv.at[0]))

    first_row = (2 * z + h) * rows - halo
    total_rows = n * rows

    def over_rows(start, size, block, f):
        def step(i, carry):
            f(pl.ds(pl.multiple_of(start + i * block, grain), block))
            return carry

        lax.fori_loop(0, size // block, step, 0)

    def chunk(layer, i):
        r0, size = piece(layer - 1, i)
        return grain * layer + r0, size

    def normalize(layer, i):
        w0, size = chunk(layer, i)
        block = 2 * grain

        def squares(r):
            total = jnp.zeros((block, lanes), jnp.float32)
            for c in range(width // lanes):
                v = stream[r, c * lanes:(c + 1) * lanes].astype(jnp.float32)
                total = total + v * v
            rowa[r, :] = total

        def scaled(r):
            scale = rowa[r, :]
            for c in range(width // lanes):
                lane = slice(c * lanes, (c + 1) * lanes)
                v = stream[r, lane].astype(jnp.float32)
                normed[r, lane] = (v * scale * gain_in[layer:layer + 1, lane]).astype(jnp.bfloat16)

        over_rows(w0, size, block, squares)
        mean = jnp.sum(rowa[w0:w0 + size, :], axis=-1, keepdims=True) / width
        rowa[w0:w0 + size, :] = jnp.broadcast_to(lax.rsqrt(mean + norm_floor), (size, lanes))
        over_rows(w0, size, block, scaled)

    def project(layer, i):
        w0, size = chunk(layer, i)
        value = jnp.dot(normed[w0:w0 + size, :], wvg[layer, 0], preferred_element_type=jnp.float32)
        gate = jnp.dot(normed[w0:w0 + size, :], wvg[layer, 1], preferred_element_type=jnp.float32)
        g = (value * (0.5 + 0.5 * jnp.tanh(0.5 * gate))).astype(jnp.bfloat16).astype(jnp.float32)
        row = lax.broadcasted_iota(jnp.int32, (size, lch), 0) + (first_row + w0)
        g = jnp.where(jnp.logical_and(row >= 0, row < total_rows), g, 0.0)
        for b in range(per_side):
            gated[b, w0:w0 + size, :] = g[:, b * lanes:(b + 1) * lanes]

    def convolve(layer, i):
        r0, size = piece(layer, i)
        start = grain * (layer + 1)
        cut = -(-size // 2 // grain) * grain
        for c0, part in ((r0, cut), (r0 + cut, size - cut)):
            def lane_block(b, carry, c0=c0, part=part):
                lane = pl.ds(pl.multiple_of(b * lanes, lanes), lanes)
                total = jnp.zeros((part, lanes), jnp.float32) + bias[layer:layer + 1, lane]
                for k in range(ntaps):
                    first = start + c0 + k - reach
                    total = total + taps[layer, k:k + 1, lane] * gated[b, first:first + part, :]
                cv[layer, cb_own, c0:c0 + part, lane] = total.astype(jnp.bfloat16)
                return carry

            lax.fori_loop(0, per_side, lane_block, 0)

    def activate(layer, i):
        r0, size = piece(layer, i)
        block = 2 * grain if size % (2 * grain) == 0 else grain
        parts = [(b, c) for b in range(tp) for c in range(per_side)]

        def load(b, c, r):
            lane = slice(c * lanes, (c + 1) * lanes)
            return (cv[layer, b, r, lane] if layer < last else cv2[b, r, lane]).astype(jnp.float32)

        def sums(r):
            s1 = jnp.zeros((block, lanes), jnp.float32)
            s2 = jnp.zeros((block, lanes), jnp.float32)
            for b, c in parts:
                v = load(b, c, r)
                s1 = s1 + v
                s2 = s2 + v * v
            rowa[r, :] = s1
            rowb[r, :] = s2

        def apply(r):
            scale, shift = rowa[r, :], rowb[r, :]
            for b, c in parts:
                lane = slice(c * lanes, (c + 1) * lanes)
                u = (load(b, c, r) - shift) * scale
                u = 0.5 * (u * lng[b, layer:layer + 1, lane] + lns[b, layer:layer + 1, lane])
                act[r, b * lch + c * lanes:b * lch + (c + 1) * lanes] = (u + u * jnp.tanh(u)).astype(jnp.bfloat16)

        over_rows(r0, size, block, sums)
        rows_ = slice(r0, r0 + size)
        average = jnp.sum(rowa[rows_, :], axis=-1, keepdims=True) / chans
        spread_ = jnp.sum(rowb[rows_, :], axis=-1, keepdims=True) / chans - average * average
        rowa[rows_, :] = jnp.broadcast_to(lax.rsqrt(spread_ + norm_floor), (size, lanes))
        rowb[rows_, :] = jnp.broadcast_to(average, (size, lanes))
        over_rows(r0, size, block, apply)

    def expand_wait(layer, s):
        for flag, slot, zs in groups(s):
            sem = d_recv.at[layers + layer * slots + slot]
            guarded(flag, lambda sem=sem: arrived(wo.at[layer, 0], d_send.at[0], sem))

    def expand(layer, s, pieces=(0, 1)):
        for flag, slot, zs in groups(s):
            def go(slot=slot, zs=zs):
                def step(j, carry):
                    c = pl.ds(pl.multiple_of((2 * zs + j) * ocols, ocols), ocols)
                    for i in pieces:
                        r0, size = piece(layer, i)
                        w0 = grain * (layer + 1) + r0
                        add = jnp.dot(act[r0:r0 + size, :], wo[layer, 2 * zs + j], preferred_element_type=jnp.float32)
                        stream[w0:w0 + size, c] = (stream[w0:w0 + size, c].astype(jnp.float32) + add).astype(jnp.bfloat16)
                    return carry

                lax.fori_loop(0, 2, step, 0)
            guarded(flag, go)

    def finish(i):
        r0, size = piece(last, i)
        for j in range(per_out):
            c = slice(j * ocols, (j + 1) * ocols)
            add = jnp.dot(act[r0:r0 + size, :], wo[last, per_out * t + j], preferred_element_type=jnp.float32)
            result[r0:r0 + size, c] = (resid[r0:r0 + size, c].astype(jnp.float32) + add).astype(jnp.bfloat16)

    barrier = pltpu.get_barrier_semaphore()
    in_start()
    for l in range(layers):
        for k in range(3):
            if k < 2:
                when(same)(lambda l=l, k=k: local_copy(l, k).start())
            else:
                local_copy(l, k).start()
    for ds in range(2):
        for j in range(tp):
            if ds or j:
                pl.semaphore_signal(barrier, inc=1, device_id=((sp, spn)[ds], lax.rem(t + j, tp)), device_id_type=MESH)
    for flag, step in ((has_up, 2), (has_down, -2)):
        @when(flag)
        def _(step=step):
            for c in range(2):
                pl.semaphore_signal(barrier, inc=1, device_id=(sp + step, 2 * x + c), device_id_type=MESH)
    pl.semaphore_wait(barrier, 2 * tp - 1 + 2 * (has_up + has_down))
    in_copies()[0].wait()

    def pre_start(l):
        for k in range(2):
            when(1 - same)(lambda k=k: pre_copy(l, k).start())

    pre_start(0)
    when(zh_to)(lambda: zh_copy().start())
    tok_starts()
    halo_pass()
    when(1 - same)(lambda: tok_start(2))
    params_start()
    own_start(0, 0)
    own_start(0, 1)
    when(same)(lambda: own_start(0, 2))
    z_recv_step(0, 0, 1)
    when(same)(lambda: tok_start(2))
    z_recv_step(0, 1, 1)
    tok_relay(0)
    when(1 - same)(lambda: own_start(0, 2))
    halo_pass_on()
    tok_relay(1)
    z_recv_step(0, 0, 2)
    tok_relay(2)
    pre_start(1)
    z_recv_step(0, 1, 2)
    spread(0, 0)
    z_recv_step(0, 2, 1)
    tok_waits()
    ih_copy().start()
    halo_waits()
    ih_wait()
    params_wait()
    normalize(0, 0)
    normalize(0, 1)
    z_recv_step(0, 0, 3)
    z_recv_step(0, 1, 3)
    own_start(1, 0)
    own_start(1, 1)
    spread(0, 1)
    need_v(0)
    for i in range(2):
        project(0, i)
        convolve(0, i)
        cv_start(0, i)
        if i == 0:
            a_step(0, 0)
            z_recv_step(0, 2, 2)

    def layer_end(layer):
        after = layer + 1
        expand_wait(layer, 3)
        for i in range(2):
            expand(layer, 3, (i,))
            normalize(after, i)
            project(after, i)
            convolve(after, i)
            if after < last:
                cv_start(after, i)
            else:
                last_start(i)

    for layer in range(last - 1):
        after = layer + 1
        beyond = layer + 2
        z_recv_step(after, 0, 1)
        cv_relay(layer, 0)
        z_recv_step(after, 1, 1)
        cv_relay(layer, 1)
        spread(layer, 2)
        z_recv_step(layer, 2, 3)
        spread(layer, 3)
        if layer == 0:
            pre_start(2)
        z_recv_step(after, 0, 2)
        b_step(layer, 0)
        a_step(layer, 1)
        cv_waits(layer, 0)
        activate(layer, 0)
        z_recv_step(after, 1, 2)
        own_start(after, 2)
        cv_waits(layer, 1)
        activate(layer, 1)
        r_step(layer, 0)
        a_step(layer, 2)
        if layer == 0:
            stream_sent()
        expand_wait(layer, 0)
        expand(layer, 0)
        z_recv_step(after, 0, 3)
        b_step(layer, 1)
        a_step(layer, 3)
        z_recv_step(after, 1, 3)
        r_step(layer, 1)
        spread(after, 0)
        z_recv_step(after, 2, 1)
        own_start(beyond, 2)
        own_start(beyond, 0)
        own_start(beyond, 1)
        expand_wait(layer, 1)
        expand(layer, 1)
        b_step(layer, 2)
        r_step(layer, 2)
        expand_wait(layer, 2)
        expand(layer, 2)
        b_step(layer, 3)
        need_v(after)
        r_step(layer, 3)
        spread(after, 1)
        z_recv_step(after, 2, 2)
        layer_end(layer)
        a_step(after, 0)

    layer = last - 1
    z_recv_step(layer, 2, 3)
    z_recv_step(last, 2, 1)
    cv_relay(layer, 0)
    z_recv_step(last, 0, 1)
    cv_relay(layer, 1)
    spread(layer, 2)
    spread(layer, 3)
    z_recv_step(last, 2, 2)
    b_step(layer, 0)
    a_step(layer, 1)
    z_recv_step(last, 1, 1)
    cv_waits(layer, 0)
    activate(layer, 0)
    z_recv_step(last, 0, 2)
    cv_waits(layer, 1)
    activate(layer, 1)
    r_step(layer, 0)
    a_step(layer, 2)
    z_recv_step(last, 2, 3)
    expand_wait(layer, 0)
    expand(layer, 0)
    z_recv_step(last, 1, 2)
    b_step(layer, 1)
    a_step(layer, 3)
    r_step(layer, 1)
    spread(last, 0)
    spread(last, 1)
    z_recv_step(last, 0, 3)
    expand_wait(layer, 1)
    expand(layer, 1)
    spread(last, 2)
    spread(last, 3)
    b_step(layer, 2)
    r_step(layer, 2)
    z_recv_step(last, 1, 3)
    o_relay(0)
    expand_wait(layer, 2)
    expand(layer, 2)
    b_step(layer, 3)
    need_v(last)
    o_relay(1)
    r_step(layer, 3)
    layer_end(layer)
    res_start()
    o_relay(2)
    last_relay(0)
    last_relay(1)
    res_wait()
    weights_sent(range(last))
    plane_sent()
    small_sent()
    conv_sent()
    last_waits(0)
    activate(last, 0)
    last_waits(1)
    o_relay(3)
    activate(last, 1)
    need_last()
    for i in range(2):
        finish(i)
        out_copy(i).start()
    weights_sent([last])
    passes_sent()
    last_sent()
    when(same)(lambda: res_copy().wait_send())
    for i in range(2):
        out_copy(i).wait()


def fused_call(mesh, *args):
    tokens, norm_gain, w_value, w_gate, conv_taps, conv_bias, ln_gain, ln_shift, w_out = args
    n, tp = mesh.shape["sp"], mesh.shape["tp"]
    layers, ntaps, lch = conv_taps.shape
    rows, feats = tokens.shape
    width, chans = feats * tp, lch * tp
    planes = n // 2
    slots = 2 * planes - 1
    halo = 16 * layers
    window = rows + 2 * halo
    most = window - 32
    dims = (n, tp, layers, ntaps, rows, width, chans)
    anys = pl.BlockSpec(memory_space=pl.ANY)
    bf, f32 = jnp.bfloat16, jnp.float32
    dma = lambda k: pltpu.SemaphoreType.DMA((k,))
    pairs = lambda k: [dma(k), dma(k)]
    wide = (layers - 1) * slots
    return pl.pallas_call(
        functools.partial(fused, dims),
        out_shape=jax.ShapeDtypeStruct((rows, feats), bf),
        in_specs=[anys] * 9,
        out_specs=anys,
        scratch_shapes=[
            pltpu.VMEM((rows, feats), bf),
            pltpu.VMEM(norm_gain.shape, f32),
            pltpu.VMEM((rows, feats), bf),
            pltpu.VMEM((layers, 2, width, lch), bf),
            pltpu.VMEM((layers, n, chans, width // n), bf),
            pltpu.VMEM(conv_taps.shape, f32),
            pltpu.VMEM(conv_bias.shape, f32),
            pltpu.VMEM((tp,) + ln_gain.shape, f32),
            pltpu.VMEM((tp,) + ln_shift.shape, f32),
            pltpu.VMEM((window, width), bf),
            pltpu.VMEM((window, width), bf),
            pltpu.VMEM((lch // 128, window, 128), f32),
            pltpu.VMEM((layers, tp, most, lch), bf),
            pltpu.VMEM((tp, rows, lch), bf),
            pltpu.VMEM((most, chans), bf),
            pltpu.VMEM((rows, feats), bf),
            pltpu.VMEM((window, 128), f32),
            pltpu.VMEM((window, 128), f32),
            dma(3 * layers), dma(6), dma(2),
            *pairs(2 * layers),
            *pairs(2 * layers * 3 * (planes - 1)),
            dma(layers * 3 * slots * 2), dma(layers * (1 + slots)),
            *pairs(wide), *pairs(wide), *pairs(wide),
            *pairs(2 * slots), dma(2),
            dma(10), dma(2 * tp), *pairs(tp), *pairs(3), *pairs(1),
            *pairs(2), dma(6), dma(2 * tp),
            *pairs(2 * layers), *pairs(2 * layers), *pairs(2 * layers),
            *pairs(6), *pairs(2 * tp), *pairs(1),
        ],
        compiler_params=pltpu.CompilerParams(
            collective_id=0, has_side_effects=True, vmem_limit_bytes=60 * 1024 * 1024),
    )(tokens, norm_gain, w_value, w_gate, w_out, conv_taps, conv_bias, ln_gain, ln_shift)


def fits(mesh, tokens, conv_taps, w_out):
    n, tp = mesh.shape["sp"], mesh.shape["tp"]
    layers, ntaps, lch = conv_taps.shape
    rows, feats = tokens.shape
    return (tp == 4 and n == 2 * tp and ntaps % 2 == 1 and ntaps // 2 < 16 and layers > 1
            and w_out.shape[2] % 128 == 0 and lch % 128 == 0 and feats % 128 == 0
            and feats == 2 * w_out.shape[2]
            and rows % 64 == 0 and rows >= 32 * layers and rows <= 512
            and layers * w_out.shape[1] * w_out.shape[2] * n * 12 <= 20 * 1024 * 1024)


def solution(mesh):
    placed = (
        P("sp", "tp"),
        P(),
        P(None, "sp", "tp"),
        P(None, "sp", "tp"),
        P(None, None, "tp"),
        P(None, "tp"),
        P(None, "tp"),
        P(None, "tp"),
        P(None, "tp", "sp"),
    )

    def run(*args):
        if fits(mesh, args[0], args[4], args[8]):
            return fused_call(mesh, *args)
        return body(*args)

    return jax.shard_map(run, mesh=mesh, in_specs=placed, out_specs=P("sp", "tp"), check_vma=False)
```

```python
import functools

import jax
import jax.numpy as jnp
from jax import lax
from jax.experimental import pallas as pl
from jax.experimental.pallas import tpu as pltpu
from jax.sharding import PartitionSpec as P

MESH = pl.DeviceIdType.MESH

norm_floor = 0.01


def with_halo(array, sides, width):
    for axis, dim in sides:
        size, length = (lax.axis_size(axis), array.shape[dim])
        up = [(i, (i + 1) % size) for i in range(size - 1)]
        down = [(j, i) for i, j in up]
        last = lax.slice_in_dim(array, length - width, length, axis=dim)
        first = lax.slice_in_dim(array, 0, width, axis=dim)
        before = lax.ppermute(last, axis, up)
        after = lax.ppermute(first, axis, down)
        array = jnp.concatenate([before, array, after], axis=dim)
    return array


def body(tokens, norm_gain, w_value, w_gate, conv_taps, conv_bias, ln_gain, ln_shift, w_out):
    stream = tokens
    layer_count = w_value.shape[0]
    reach = conv_taps.shape[1] // 2
    local_channels = w_value.shape[2]
    channels = local_channels * lax.axis_size("tp")
    tok_rows = tokens.shape[0]
    whole_value, whole_gate = (
        lax.all_gather(w_value, "sp", axis=1, tiled=True),
        lax.all_gather(w_gate, "sp", axis=1, tiled=True),
    )
    whole_out = lax.all_gather(w_out, "sp", axis=2, tiled=True)
    for layer_index in range(layer_count):
        whole_rows = lax.all_gather(stream, "tp", axis=1, tiled=True)
        rows_f32 = whole_rows.astype(jnp.float32)
        scale_rows = lax.rsqrt(jnp.mean(rows_f32 * rows_f32, axis=-1, keepdims=True) + norm_floor)
        normed = (rows_f32 * scale_rows * norm_gain[layer_index]).astype(jnp.bfloat16)
        value_rows = jnp.dot(normed, whole_value[layer_index], preferred_element_type=jnp.float32)
        gate_rows = jnp.dot(normed, whole_gate[layer_index], preferred_element_type=jnp.float32)
        gated_input = (value_rows * jax.nn.sigmoid(gate_rows)).astype(jnp.bfloat16)
        padded = with_halo(gated_input, (("sp", 0),), reach)
        padded = padded.astype(jnp.float32)
        convolved = jnp.zeros((tok_rows, local_channels), jnp.float32) + conv_bias[layer_index]
        for offset in range(2 * reach + 1):
            convolved = (
                convolved + conv_taps[layer_index, offset] * padded[offset : offset + tok_rows]
            )
        moments = lax.psum(
            (
                jnp.sum(convolved, axis=-1, keepdims=True),
                jnp.sum(convolved * convolved, axis=-1, keepdims=True),
            ),
            "tp",
        )
        average = moments[0] / channels
        spread = moments[1] / channels - average * average
        activated = jax.nn.silu(
            (convolved - average) * lax.rsqrt(spread + norm_floor) * ln_gain[layer_index]
            + ln_shift[layer_index]
        ).astype(jnp.bfloat16)
        partial_rows = jnp.dot(
            activated, whole_out[layer_index], preferred_element_type=jnp.float32
        )
        summed = lax.psum_scatter(
            partial_rows.astype(jnp.bfloat16), "tp", scatter_dimension=1, tiled=True
        ).astype(jnp.float32)
        stream = (stream.astype(jnp.float32) + summed).astype(jnp.bfloat16)
    return stream


def fused(
    dims,
    tok_in, gain_hbm, wv_in, wg_in, wo_in, taps_in, bias_in, lng_in, lns_in,
    out,
    tok, gain_in, result, wvg, wo, taps, bias, lng, lns, stream, normed, gated, cv, cv2, act, resid, rowa, rowb,
    loc_sem, in_sem, out_sem, pre_send, pre_recv, z_send, z_recv, d_send, d_recv,
    a_send, a_recv, b_send, b_recv, r_send, r_recv, o_send, o_recv,
    tok_send, tok_recv, zh_send, zh_recv, hp_send, hp_recv, ih_send, ih_recv,
    par_send, par_recv, ln_send, ln_recv,
    cv_send, ca_recv, cb_recv, cr_recv,
    l_send, l_recv, p_send, p_recv, res_send, res_recv,
):
    n, tp, layers, ntaps, rows, width, chans = dims
    planes = n // 2
    feats = width // tp
    lch = chans // tp
    krows = width // n
    ocols = width // n
    reach = ntaps // 2
    grain = 16
    halo = grain * layers
    window = rows + 2 * halo
    last = layers - 1
    lanes = 128
    per_side = lch // lanes
    per_out = feats // ocols

    sp = lax.axis_index("sp")
    t = lax.axis_index("tp")
    z, y = sp // 2, lax.rem(sp, 2)
    x, h = t // 2, lax.rem(t, 2)
    xn, yn, hn = 1 - x, 1 - y, 1 - h
    same = 1 - (y + h - 2 * y * h)
    spn = 2 * z + yn
    has_up, has_down = 1 - (z + 1) // planes, jnp.minimum(z, 1)

    partner = (sp, 2 * x + hn)
    xdev = (sp, 2 * xn + h)
    ydev = (spn, t)
    ax, ay = hn * xn + h * x, hn * y + h * yn
    bx, by = hn * x + h * xn, hn * yn + h * y
    adev = (2 * z + ay, 2 * ax + h)
    bdev = (2 * z + by, 2 * bx + h)

    def rcopy(src, dst, ssem, rsem, dev):
        return pltpu.make_async_remote_copy(
            src_ref=src, dst_ref=dst, send_sem=ssem, recv_sem=rsem,
            device_id=dev, device_id_type=MESH)

    def arrived(ref, ssem, rsem):
        rcopy(ref, ref, ssem, rsem, partner).wait_recv()

    def sent(ref, ssem):
        rcopy(ref, ref, ssem, ssem, partner).wait_send()

    def when(flag):
        return pl.when(flag == 1)

    def vblock(l, k, zs, c):
        r = pl.ds(pl.multiple_of((2 * zs + c) * krows, krows), krows)
        return wvg.at[l, k, r, :]

    def oblock(l, zs, yy, cb):
        r = pl.ds(pl.multiple_of(cb * lch, lch), lch)
        return wo.at[l, 2 * zs + yy, r, :]

    def item(l, k, zs):
        return vblock(l, k, zs, h) if k < 2 else oblock(l, zs, y, t)

    def local_copy(l, k):
        src = (wv_in, wg_in, wo_in)[k].at[l]
        return pltpu.make_async_copy(src, item(l, k, z), loc_sem.at[3 * l + k])

    def pre_copy(l, k):
        src = (wv_in, wg_in)[k].at[l]
        i = 2 * l + k
        return rcopy(src, vblock(l, k, z, y), pre_send.at[0], pre_recv.at[i], (spn, 2 * x + hn))

    def z_parts(l, k, d, s):
        zs = z - s if d == 0 else z + s
        return item(l, k, zs), z_recv.at[(l * 3 + k) * (planes - 1) + zs - d]

    def z_copy(l, k, d, s):
        ref, rsem = z_parts(l, k, d, s)
        return rcopy(ref, ref, z_send.at[d * (planes - 1) + s], rsem, (sp + (2 if d == 0 else -2), t))

    def z_wait(l, k, d, s):
        ref, rsem = z_parts(l, k, d, s)
        arrived(ref, z_send.at[0], rsem)

    def d_copy(l, k, zs, ref):
        i, j = (l, l) if k < 2 else (layers + l, layers + l * planes + zs)
        return rcopy(ref, ref, d_send.at[i], d_recv.at[j], partner)

    def a_copy(l, zs):
        ref = oblock(l, zs, y, t)
        return rcopy(ref, ref, a_send.at[l], a_recv.at[l * planes + zs], adev)

    def b_copy(l, zs):
        ref = oblock(l, zs, y, t)
        return rcopy(ref, ref, b_send.at[l], b_recv.at[l * planes + zs], bdev)

    def from_a(l, zs):
        return oblock(l, zs, ay, 2 * ax + h)

    def from_b(l, zs):
        return oblock(l, zs, by, 2 * bx + h)

    def r_copy(l, zs):
        ref = from_a(l, zs)
        return rcopy(ref, ref, r_send.at[l], r_recv.at[l * planes + zs], bdev)

    def o_copy(rel, zs):
        ref = oblock(last, zs, y, t)
        return rcopy(ref, ref, o_send.at[rel], o_recv.at[2 * t + rel],
                     (sp if rel == 0 else spn, zs))

    def differs(a, b):
        return jnp.minimum(jnp.abs(a - b), 1)

    def to_partner(l, k, zs):
        if k < 2 or l < last:
            d_copy(l, k, zs, item(l, k, zs)).start()

    def spread(l, s):
        for flag, zs in groups(s):
            def go(zs=zs):
                if l < last:
                    a_copy(l, zs).start()
                    b_copy(l, zs).start()
                else:
                    when(differs(zs, t))(lambda: o_copy(0, zs).start())
                    far = 1 if s == planes - 1 else 1 - differs(zs // 2, x)
                    when(far)(lambda: o_copy(1, zs).start())
            guarded(flag, go)

    def o_pass(c):
        owner = 2 * xn + c
        ref = oblock(last, t, y, owner)
        return rcopy(ref, ref, o_send.at[2], o_recv.at[2 * owner + 1], ydev)

    def o_relay(s):
        @when(1 - differs(jnp.abs(z - t), s))
        def _():
            for c in range(2):
                owner = 2 * xn + c
                arrived(oblock(last, t, y, owner), o_send.at[0], o_recv.at[2 * owner])
                if s < planes - 1:
                    o_pass(c).start()

    def own_start(l, k):
        if k < 2:
            when(same)(lambda: local_copy(l, k).wait())

            @when(1 - same)
            def _():
                i = 2 * l + k
                arrived(item(l, k, z), pre_send.at[0], pre_recv.at[i])
        else:
            local_copy(l, k).wait()
        when(has_up)(lambda: z_copy(l, k, 0, 0).start())
        when(has_down)(lambda: z_copy(l, k, 1, 0).start())
        to_partner(l, k, z)

    def below(s):
        return jnp.minimum(z // s, 1)

    def above(s):
        return jnp.minimum((planes - 1 - z) // s, 1)

    def groups(s):
        if s == 0:
            return [(None, z)]
        return [(below(s), z - s), (above(s), z + s)]

    def guarded(flag, f):
        if flag is None:
            f()
        else:
            when(flag)(f)

    def z_recv_step(l, k, s):
        for d, (flag, zs) in enumerate(groups(s)):
            def go(d=d, zs=zs):
                z_wait(l, k, d, s)
                if s < planes - 1:
                    when((has_up, has_down)[d])(lambda: z_copy(l, k, d, s).start())
                to_partner(l, k, zs)
            guarded(flag, go)

    def a_step(l, s):
        for flag, zs in groups(s):
            def go(zs=zs):
                ref = from_a(l, zs)
                arrived(ref, a_send.at[0], a_recv.at[l * planes + zs])
                r_copy(l, zs).start()
                d_copy(l, 2, zs, ref).start()
            guarded(flag, go)

    def b_step(l, s):
        for flag, zs in groups(s):
            def go(zs=zs):
                ref = from_b(l, zs)
                arrived(ref, b_send.at[0], b_recv.at[l * planes + zs])
                d_copy(l, 2, zs, ref).start()
            guarded(flag, go)

    def r_step(l, s):
        for flag, zs in groups(s):
            def go(zs=zs):
                ref = oblock(l, zs, yn, 2 * xn + h)
                arrived(ref, r_send.at[0], r_recv.at[l * planes + zs])
                d_copy(l, 2, zs, ref).start()
            guarded(flag, go)

    def v_half(l):
        return wvg.at[l, :, pl.ds(0, width // 2), :]

    def need_v(l):
        arrived(v_half(l), d_send.at[0], d_recv.at[l])

    def need_last():
        mate = 2 * x + hn
        arrived(oblock(last, t, y, mate), o_send.at[0], o_recv.at[2 * mate])
        for j in range(tp):
            other = lax.rem(t + j, tp)
            arrived(oblock(last, t, yn, other), o_send.at[0], o_recv.at[2 * other + 1])

    def v_sent():
        when(1 - same)(lambda: sent(wvg.at[:, :, pl.ds(0, krows), :], pre_send.at[0]))
        for l in range(layers):
            sent(v_half(l), d_send.at[l])
        for s in range(planes - 1):
            for d, flag in enumerate((has_up, has_down)):
                ok = flag if s == 0 else flag * (below(s), above(s))[d]
                ref = wvg.at[:, :, pl.ds(0, 3 * krows // 2), :]
                when(ok)(lambda d=d, s=s, ref=ref: sent(ref, z_send.at[d * (planes - 1) + s]))

    def o_sent():
        for l in range(last):
            sent(wo.at[l, pl.ds(0, planes)], d_send.at[layers + l])
            for sem in (a_send, b_send, r_send):
                sent(wo.at[l, 0], sem.at[l])

    def o_last_sent():
        def some(i, count):
            sent(wo.at[last, 0, pl.ds(0, count * lch), :], o_send.at[i])

        at_end = 1 - differs(jnp.abs(planes - 1 - 2 * z), planes - 1)
        extra = at_end * differs((planes - 1 - z) // 2, x)
        some(0, tp - 1)
        when(extra)(lambda: some(1, 3))
        when(1 - extra)(lambda: some(1, 2))
        when(differs(jnp.abs(z - t), planes - 1))(lambda: some(2, 2))

    def cols(owner):
        return pl.ds(pl.multiple_of(owner * feats, feats), feats)

    tcols = cols(t)

    half_rows = rows // 2

    def hcols(owner, part):
        return stream.at[pl.ds(halo + part * half_rows, half_rows), cols(owner)]

    def tok_copy(j, p):
        dev = ((sp, 2 * x + y), (sp, 2 * xn + y), (spn, 2 * x + y))[j]
        return rcopy(tok.at[pl.ds(p * half_rows, half_rows), :], hcols(t, p),
                     tok_send.at[min(j, 1)], tok_recv.at[2 * t + p], dev)

    def tok_start(j):
        tok_copy(j, 0).start()
        tok_copy(j, 1).start()

    def tok_pass(j):
        owner, p, dev = (
            (2 * xn + yn, 0, ydev), (2 * x + yn, 0, xdev),
            (2 * x + yn, 1, xdev), (2 * x + y, 1, xdev))[j]
        ref = hcols(owner, p)
        return rcopy(ref, ref, tok_send.at[2], tok_recv.at[2 * owner + p], dev)

    def tok_starts():
        when(1 - same)(lambda: tok_start(0))
        tok_start(1)

        @when(same)
        def _():
            stream[pl.ds(halo, rows), tcols] = tok[...]

    def tok_arrived(owner, p):
        arrived(hcols(owner, p), tok_send.at[0], tok_recv.at[2 * owner + p])

    def tok_relay(step):
        @when(same)
        def _():
            if step == 0:
                tok_arrived(2 * xn + yn, 0)
                tok_pass(0).start()

        @when(1 - same)
        def _():
            if step == 0:
                tok_arrived(2 * x + yn, 0)
                tok_pass(1).start()
            elif step == 1:
                tok_arrived(2 * x + yn, 1)
                tok_pass(2).start()
            else:
                tok_arrived(2 * x + y, 1)
                tok_pass(3).start()

    def tok_waits():
        @when(same)
        def _():
            tok_arrived(2 * xn + yn, 1)
            for p in range(2):
                tok_arrived(2 * x + hn, p)
                tok_arrived(2 * xn + y, p)

        @when(1 - same)
        def _():
            tok_arrived(2 * x + y, 0)
            for p in range(2):
                tok_arrived(2 * xn + yn, p)
                tok_arrived(2 * xn + y, p)

    zh_to = y * has_up + yn * has_down
    zh_from = hn * has_down + h * has_up

    def edge(owner_cols, side):
        r = pl.ds(pl.multiple_of(side * (halo + rows), grain), halo)
        return stream.at[r, owner_cols]

    def zh_copy():
        src = tok.at[pl.ds(pl.multiple_of(y * (rows - halo), grain), halo), :]
        return rcopy(src, edge(tcols, yn), zh_send.at[0], zh_recv.at[0],
                     (sp + 4 * y - 2, 2 * x + yn))

    def half_cols(xx):
        return pl.ds(pl.multiple_of(xx * 2 * feats, feats), 2 * feats)

    def hp_copy(j):
        ref = edge(half_cols(xn if j == 2 else x), h)
        return rcopy(ref, ref, hp_send.at[0], hp_recv.at[j], xdev if j == 0 else ydev)

    def halo_pass():
        @when(zh_from * (1 - same))
        def _():
            arrived(edge(half_cols(x), h), zh_send.at[0], zh_recv.at[0])
            hp_copy(0).start()
            hp_copy(1).start()

        @when(1 - zh_from)
        def _():
            stream[pl.ds(pl.multiple_of(h * (halo + rows), grain), halo), :] = jnp.zeros((halo, width), jnp.bfloat16)

    def halo_pass_on():
        @when(zh_from * (1 - same))
        def _():
            arrived(edge(half_cols(xn), h), hp_send.at[0], hp_recv.at[0])
            hp_copy(2).start()

    def halo_waits():
        @when(zh_from * same)
        def _():
            arrived(edge(half_cols(x), h), hp_send.at[0], hp_recv.at[1])
            arrived(edge(half_cols(xn), h), hp_send.at[0], hp_recv.at[2])

    def ih_copy():
        src = stream.at[pl.ds(pl.multiple_of(hn * rows + h * halo, grain), halo), :]
        dst = stream.at[pl.ds(pl.multiple_of(h * (halo + rows), grain), halo), :]
        return rcopy(src, dst, ih_send.at[0], ih_recv.at[0], partner)

    def ih_wait():
        ref = stream.at[pl.ds(pl.multiple_of(hn * (halo + rows), grain), halo), :]
        arrived(ref, ih_send.at[0], ih_recv.at[0])

    def par_copy(i):
        a, b = ((taps_in, taps), (bias_in, bias))[i]
        return rcopy(a, b, par_send.at[i], par_recv.at[i], partner)

    def ln_copy(i, j):
        a, b = ((lng_in, lng), (lns_in, lns))[i]
        return rcopy(a, b.at[t], ln_send.at[i], ln_recv.at[i],
                     (sp, lax.rem(t + j, tp)))

    def params_start():
        for i in range(2):
            when(same)(lambda i=i: par_copy(i).start())
            for j in range(1, tp):
                ln_copy(i, j).start()


    def in_copies():
        return [
            pltpu.make_async_copy(a, b, in_sem.at[i])
            for i, (a, b) in enumerate((
                (tok_in, tok), (gain_hbm, gain_in), (lng_in, lng.at[t]), (lns_in, lns.at[t]),
                (taps_in, taps), (bias_in, bias)))
        ]

    def in_start():
        for i, c in enumerate(in_copies()):
            if i < 4:
                c.start()
            else:
                when(same)(lambda c=c: c.start())

    def out_copy(i):
        r0, size = piece(last, i)
        r = pl.ds(r0, size)
        return pltpu.make_async_copy(result.at[r, :], out.at[r, :], out_sem.at[i])

    def params_wait():
        for i, c in enumerate(in_copies()):
            if i >= 4:
                when(same)(lambda c=c: c.wait())
            elif i > 0:
                c.wait()
        for i, ref in enumerate((taps, bias)):
            when(1 - same)(lambda i=i, ref=ref: arrived(ref, par_send.at[i], par_recv.at[i]))
        for i, ref in enumerate((lng, lns)):
            arrived(ref.at[pl.ds(0, tp - 1)], ln_send.at[0], ln_recv.at[i])

    def small_sent():
        when(1 - same)(lambda: sent(tok, tok_send.at[0]))
        sent(stream.at[pl.ds(0, rows), pl.ds(0, 2 * feats)], tok_send.at[1])
        when(zh_to)(lambda: zh_copy().wait_send())
        for i, ref in enumerate((lng, lns)):
            when(same)(lambda i=i: par_copy(i).wait_send())
            sent(ref.at[pl.ds(0, tp - 1)], ln_send.at[i])

    def stream_sent():
        for flag, count in ((same, 1), (1 - same, 3)):
            ref = stream.at[pl.ds(0, half_rows), pl.ds(0, count * feats)]
            when(flag)(lambda ref=ref: sent(ref, tok_send.at[2]))
        ref = stream.at[pl.ds(0, 3 * halo), pl.ds(0, 2 * feats)]
        when(zh_from * (1 - same))(lambda: sent(ref, hp_send.at[0]))
        ih_copy().wait_send()

    cb_own = 2 * x + y
    cb_a, cb_b, cb_d = 2 * ax + ay, 2 * bx + by, 2 * xn + yn

    def piece(l, i):
        total = window - 2 * grain * (l + 1)
        first = total - rows // 2
        return i * first, total - first if i else first

    def cblock(l, i, cb):
        r0, size = piece(l, i)
        return cv.at[l, cb, pl.ds(r0, size), :]

    def cv_copy(l, i, j):
        ref = cblock(l, i, cb_a if j == 2 else cb_own)
        r = (ca_recv, cb_recv, cr_recv)[j]
        return rcopy(ref, ref, cv_send.at[l], r.at[2 * l + i], adev if j == 0 else bdev)

    def cv_start(l, i):
        cv_copy(l, i, 0).start()
        cv_copy(l, i, 1).start()

    def cv_relay(l, i):
        arrived(cblock(l, i, cb_a), cv_send.at[0], ca_recv.at[2 * l + i])
        cv_copy(l, i, 2).start()

    def cv_waits(l, i):
        arrived(cblock(l, i, cb_b), cv_send.at[0], cb_recv.at[2 * l + i])
        arrived(cblock(l, i, cb_d), cv_send.at[0], cr_recv.at[2 * l + i])

    def lblock(i, cb):
        r0, size = piece(last, i)
        return cv2.at[cb, pl.ds(r0, size), :]

    def l_copy(i, j):
        src, cb, dev = (
            (cblock(last, i, cb_own), cb_own, ydev),
            (cblock(last, i, cb_own), cb_own, xdev),
            (lblock(i, 2 * x + yn), 2 * x + yn, xdev),
        )[j]
        return rcopy(src, lblock(i, cb), l_send.at[0], l_recv.at[3 * i + j], dev)

    def p_copy(i, j):
        cb = (cb_own, 2 * x + yn, 2 * xn + y, 2 * xn + yn)[j]
        src = cblock(last, i, cb) if j == 0 else lblock(i, cb)
        return rcopy(src, lblock(i, cb), p_send.at[0], p_recv.at[i], partner)

    def last_start(i):
        r0, size = piece(last, i)
        when(1 - same)(lambda: l_copy(i, 0).start())

        @when(same)
        def _():
            l_copy(i, 1).start()
            p_copy(i, 0).start()
            cv2[cb_own, r0:r0 + size, :] = cv[last, cb_own, r0:r0 + size, :]

    def last_relay(i):
        @when(same)
        def _():
            arrived(lblock(i, 2 * x + yn), l_send.at[0], l_recv.at[3 * i])
            l_copy(i, 2).start()
            p_copy(i, 1).start()

    def last_waits(i):
        @when(same)
        def _():
            for j in (1, 2):
                cb = 2 * xn + (y if j == 1 else yn)
                arrived(lblock(i, cb), l_send.at[0], l_recv.at[3 * i + j])
                p_copy(i, j + 1).start()

        r0, size = piece(last, i)
        when(1 - same)(lambda: arrived(cv2.at[:, pl.ds(r0, size), :], p_send.at[0], p_recv.at[i]))

    def conv_sent():
        for l in range(last):
            total = window - 2 * grain * (l + 1)
            sent(cv.at[l, pl.ds(0, 3), pl.ds(0, total), :], cv_send.at[l])

    def last_sent():
        when(1 - same)(lambda: sent(cv2.at[0], l_send.at[0]))

        @when(same)
        def _():
            sent(cv2.at[pl.ds(0, 2)], l_send.at[0])
            sent(cv2, p_send.at[0])

    def res_copy():
        src = stream.at[pl.ds(halo, rows), cols(2 * x + hn)]
        return rcopy(src, resid, res_send.at[0], res_recv.at[0], partner)

    def res_start():
        @when(same)
        def _():
            res_copy().start()
            resid[...] = stream[pl.ds(halo, rows), tcols]

    def res_wait():
        when(1 - same)(lambda: arrived(resid, res_send.at[0], res_recv.at[0]))

    first_row = (2 * z + h) * rows - halo
    total_rows = n * rows

    def over_rows(start, size, block, f):
        def step(i, carry):
            f(pl.ds(pl.multiple_of(start + i * block, grain), block))
            return carry

        lax.fori_loop(0, size // block, step, 0)

    def chunk(layer, i):
        r0, size = piece(layer - 1, i)
        return grain * layer + r0, size

    def normalize(layer, i):
        w0, size = chunk(layer, i)
        block = 2 * grain

        def squares(r):
            total = jnp.zeros((block, lanes), jnp.float32)
            for c in range(width // lanes):
                v = stream[r, c * lanes:(c + 1) * lanes].astype(jnp.float32)
                total = total + v * v
            rowa[r, :] = total

        def scaled(r):
            scale = rowa[r, :]
            for c in range(width // lanes):
                lane = slice(c * lanes, (c + 1) * lanes)
                v = stream[r, lane].astype(jnp.float32)
                normed[r, lane] = (v * scale * gain_in[layer:layer + 1, lane]).astype(jnp.bfloat16)

        over_rows(w0, size, block, squares)
        mean = jnp.sum(rowa[w0:w0 + size, :], axis=-1, keepdims=True) / width
        rowa[w0:w0 + size, :] = jnp.broadcast_to(lax.rsqrt(mean + norm_floor), (size, lanes))
        over_rows(w0, size, block, scaled)

    def project(layer, i):
        w0, size = chunk(layer, i)
        value = jnp.dot(normed[w0:w0 + size, :], wvg[layer, 0], preferred_element_type=jnp.float32)
        gate = jnp.dot(normed[w0:w0 + size, :], wvg[layer, 1], preferred_element_type=jnp.float32)
        g = (value * (0.5 + 0.5 * jnp.tanh(0.5 * gate))).astype(jnp.bfloat16).astype(jnp.float32)
        row = lax.broadcasted_iota(jnp.int32, (size, lch), 0) + (first_row + w0)
        g = jnp.where(jnp.logical_and(row >= 0, row < total_rows), g, 0.0)
        for b in range(per_side):
            gated[b, w0:w0 + size, :] = g[:, b * lanes:(b + 1) * lanes]

    def convolve(layer, i):
        r0, size = piece(layer, i)
        start = grain * (layer + 1)
        cut = -(-size // 2 // grain) * grain
        for c0, part in ((r0, cut), (r0 + cut, size - cut)):
            def lane_block(b, carry, c0=c0, part=part):
                lane = pl.ds(pl.multiple_of(b * lanes, lanes), lanes)
                total = jnp.zeros((part, lanes), jnp.float32) + bias[layer:layer + 1, lane]
                for k in range(ntaps):
                    first = start + c0 + k - reach
                    total = total + taps[layer, k:k + 1, lane] * gated[b, first:first + part, :]
                cv[layer, cb_own, c0:c0 + part, lane] = total.astype(jnp.bfloat16)
                return carry

            lax.fori_loop(0, per_side, lane_block, 0)

    def activate(layer, i):
        r0, size = piece(layer, i)
        block = 2 * grain if size % (2 * grain) == 0 else grain
        parts = [(b, c) for b in range(tp) for c in range(per_side)]

        def load(b, c, r):
            lane = slice(c * lanes, (c + 1) * lanes)
            return (cv[layer, b, r, lane] if layer < last else cv2[b, r, lane]).astype(jnp.float32)

        def sums(r):
            s1 = jnp.zeros((block, lanes), jnp.float32)
            s2 = jnp.zeros((block, lanes), jnp.float32)
            for b, c in parts:
                v = load(b, c, r)
                s1 = s1 + v
                s2 = s2 + v * v
            rowa[r, :] = s1
            rowb[r, :] = s2

        def apply(r):
            scale, shift = rowa[r, :], rowb[r, :]
            for b, c in parts:
                lane = slice(c * lanes, (c + 1) * lanes)
                u = (load(b, c, r) - shift) * scale
                u = 0.5 * (u * lng[b, layer:layer + 1, lane] + lns[b, layer:layer + 1, lane])
                act[r, b * lch + c * lanes:b * lch + (c + 1) * lanes] = (u + u * jnp.tanh(u)).astype(jnp.bfloat16)

        over_rows(r0, size, block, sums)
        rows_ = slice(r0, r0 + size)
        average = jnp.sum(rowa[rows_, :], axis=-1, keepdims=True) / chans
        spread_ = jnp.sum(rowb[rows_, :], axis=-1, keepdims=True) / chans - average * average
        rowa[rows_, :] = jnp.broadcast_to(lax.rsqrt(spread_ + norm_floor), (size, lanes))
        rowb[rows_, :] = jnp.broadcast_to(average, (size, lanes))
        over_rows(r0, size, block, apply)

    def expand_wait(layer, s):
        for flag, zs in groups(s):
            sem = d_recv.at[layers + layer * planes + zs]
            guarded(flag, lambda sem=sem: arrived(wo.at[layer, 0], d_send.at[0], sem))

    def expand(layer, s, pieces=(0, 1)):
        for flag, zs in groups(s):
            def go(zs=zs):
                def step(j, carry):
                    c = pl.ds(pl.multiple_of((2 * zs + j) * ocols, ocols), ocols)
                    for i in pieces:
                        r0, size = piece(layer, i)
                        w0 = grain * (layer + 1) + r0
                        add = jnp.dot(act[r0:r0 + size, :], wo[layer, 2 * zs + j], preferred_element_type=jnp.float32)
                        stream[w0:w0 + size, c] = (stream[w0:w0 + size, c].astype(jnp.float32) + add).astype(jnp.bfloat16)
                    return carry

                lax.fori_loop(0, 2, step, 0)
            guarded(flag, go)

    def finish(i):
        r0, size = piece(last, i)
        for j in range(per_out):
            c = slice(j * ocols, (j + 1) * ocols)
            add = jnp.dot(act[r0:r0 + size, :], wo[last, per_out * t + j], preferred_element_type=jnp.float32)
            result[r0:r0 + size, c] = (resid[r0:r0 + size, c].astype(jnp.float32) + add).astype(jnp.bfloat16)

    barrier = pltpu.get_barrier_semaphore()
    in_start()
    for l in range(layers):
        for k in range(3):
            if k < 2:
                when(same)(lambda l=l, k=k: local_copy(l, k).start())
            else:
                local_copy(l, k).start()
    for ds in range(2):
        for j in range(tp):
            if ds or j:
                pl.semaphore_signal(barrier, inc=1, device_id=((sp, spn)[ds], lax.rem(t + j, tp)), device_id_type=MESH)
    for flag, step in ((has_up, 2), (has_down, -2)):
        @when(flag)
        def _(step=step):
            for c in range(2):
                pl.semaphore_signal(barrier, inc=1, device_id=(sp + step, 2 * x + c), device_id_type=MESH)
    pl.semaphore_wait(barrier, 2 * tp - 1 + 2 * (has_up + has_down))
    in_copies()[0].wait()

    def pre_start(l):
        for k in range(2):
            when(1 - same)(lambda k=k: pre_copy(l, k).start())

    pre_start(0)
    when(zh_to)(lambda: zh_copy().start())
    tok_starts()
    halo_pass()
    when(1 - same)(lambda: tok_start(2))
    params_start()
    own_start(0, 0)
    own_start(0, 1)
    when(same)(lambda: own_start(0, 2))
    z_recv_step(0, 0, 1)
    when(same)(lambda: tok_start(2))
    z_recv_step(0, 1, 1)
    tok_relay(0)
    when(1 - same)(lambda: own_start(0, 2))
    halo_pass_on()
    tok_relay(1)
    z_recv_step(0, 0, 2)
    tok_relay(2)
    pre_start(1)
    z_recv_step(0, 1, 2)
    spread(0, 0)
    z_recv_step(0, 2, 1)
    tok_waits()
    ih_copy().start()
    halo_waits()
    ih_wait()
    params_wait()
    normalize(0, 0)
    normalize(0, 1)
    z_recv_step(0, 0, 3)
    z_recv_step(0, 1, 3)
    own_start(1, 0)
    own_start(1, 1)
    spread(0, 1)
    need_v(0)
    for i in range(2):
        project(0, i)
        convolve(0, i)
        cv_start(0, i)
        if i == 0:
            a_step(0, 0)
            z_recv_step(0, 2, 2)

    def layer_end(layer, between):
        after = layer + 1
        expand_wait(layer, 3)
        for i in range(2):
            expand(layer, 3, (i,))
            normalize(after, i)
            project(after, i)
            convolve(after, i)
            if after < last:
                cv_start(after, i)
            else:
                last_start(i)
            if i == 0:
                between()

    for layer in range(last - 1):
        after = layer + 1
        beyond = layer + 2
        z_recv_step(after, 0, 1)
        cv_relay(layer, 0)
        z_recv_step(after, 1, 1)
        cv_relay(layer, 1)
        spread(layer, 2)
        z_recv_step(layer, 2, 3)
        spread(layer, 3)
        if layer == 0:
            pre_start(2)
        z_recv_step(after, 0, 2)
        b_step(layer, 0)
        a_step(layer, 1)
        cv_waits(layer, 0)
        activate(layer, 0)
        z_recv_step(after, 1, 2)
        own_start(after, 2)
        cv_waits(layer, 1)
        activate(layer, 1)
        r_step(layer, 0)
        a_step(layer, 2)
        if layer == 0:
            stream_sent()
        expand_wait(layer, 0)
        expand(layer, 0)
        z_recv_step(after, 0, 3)
        b_step(layer, 1)
        a_step(layer, 3)
        z_recv_step(after, 1, 3)
        r_step(layer, 1)
        spread(after, 0)
        z_recv_step(after, 2, 1)
        own_start(beyond, 2)
        own_start(beyond, 0)
        own_start(beyond, 1)
        expand_wait(layer, 1)
        expand(layer, 1)
        b_step(layer, 2)
        r_step(layer, 2)
        expand_wait(layer, 2)
        expand(layer, 2)
        b_step(layer, 3)
        need_v(after)
        r_step(layer, 3)
        spread(after, 1)
        layer_end(layer, lambda: z_recv_step(after, 2, 2))
        a_step(after, 0)

    layer = last - 1
    z_recv_step(layer, 2, 3)
    z_recv_step(last, 2, 1)
    cv_relay(layer, 0)
    z_recv_step(last, 0, 1)
    cv_relay(layer, 1)
    spread(layer, 2)
    spread(layer, 3)
    z_recv_step(last, 2, 2)
    b_step(layer, 0)
    a_step(layer, 1)
    z_recv_step(last, 1, 1)
    cv_waits(layer, 0)
    activate(layer, 0)
    z_recv_step(last, 0, 2)
    cv_waits(layer, 1)
    activate(layer, 1)
    r_step(layer, 0)
    a_step(layer, 2)
    z_recv_step(last, 2, 3)
    expand_wait(layer, 0)
    expand(layer, 0)
    z_recv_step(last, 1, 2)
    b_step(layer, 1)
    a_step(layer, 3)
    r_step(layer, 1)
    spread(last, 0)
    spread(last, 1)
    z_recv_step(last, 0, 3)
    expand_wait(layer, 1)
    expand(layer, 1)
    spread(last, 2)
    spread(last, 3)
    b_step(layer, 2)
    r_step(layer, 2)
    z_recv_step(last, 1, 3)
    o_relay(0)
    expand_wait(layer, 2)
    expand(layer, 2)
    b_step(layer, 3)
    need_v(last)
    o_relay(1)
    r_step(layer, 3)
    layer_end(layer, lambda: None)
    res_start()
    o_relay(2)
    last_relay(0)
    last_relay(1)
    res_wait()
    o_sent()
    small_sent()
    conv_sent()
    last_waits(0)
    activate(last, 0)
    last_waits(1)
    o_relay(3)
    activate(last, 1)
    need_last()
    for i in range(2):
        finish(i)
        out_copy(i).start()
    v_sent()
    o_last_sent()
    last_sent()
    when(same)(lambda: res_copy().wait_send())
    for i in range(2):
        out_copy(i).wait()


def fused_call(mesh, *args):
    tokens, norm_gain, w_value, w_gate, conv_taps, conv_bias, ln_gain, ln_shift, w_out = args
    n, tp = mesh.shape["sp"], mesh.shape["tp"]
    layers, ntaps, lch = conv_taps.shape
    rows, feats = tokens.shape
    width, chans = feats * tp, lch * tp
    planes = n // 2
    last = layers - 1
    halo = 16 * layers
    window = rows + 2 * halo
    most = window - 32
    dims = (n, tp, layers, ntaps, rows, width, chans)
    anys = pl.BlockSpec(memory_space=pl.ANY)
    bf, f32 = jnp.bfloat16, jnp.float32
    dma = lambda k: pltpu.SemaphoreType.DMA((k,))
    return pl.pallas_call(
        functools.partial(fused, dims),
        out_shape=jax.ShapeDtypeStruct((rows, feats), bf),
        in_specs=[anys] * 9,
        out_specs=anys,
        scratch_shapes=[
            pltpu.VMEM((rows, feats), bf),
            pltpu.VMEM(norm_gain.shape, f32),
            pltpu.VMEM((rows, feats), bf),
            pltpu.VMEM((layers, 2, width, lch), bf),
            pltpu.VMEM((layers, n, chans, width // n), bf),
            pltpu.VMEM(conv_taps.shape, f32),
            pltpu.VMEM(conv_bias.shape, f32),
            pltpu.VMEM((tp,) + ln_gain.shape, f32),
            pltpu.VMEM((tp,) + ln_shift.shape, f32),
            pltpu.VMEM((window, width), bf),
            pltpu.VMEM((window, width), bf),
            pltpu.VMEM((lch // 128, window, 128), f32),
            pltpu.VMEM((layers, tp, most, lch), bf),
            pltpu.VMEM((tp, rows, lch), bf),
            pltpu.VMEM((most, chans), bf),
            pltpu.VMEM((rows, feats), bf),
            pltpu.VMEM((window, 128), f32),
            pltpu.VMEM((window, 128), f32),
            dma(3 * layers), dma(6), dma(2),
            dma(1), dma(2 * layers),
            dma(2 * (planes - 1)), dma(3 * layers * (planes - 1)),
            dma(layers + last), dma(layers + last * planes),
            *[dma(k) for _ in range(3) for k in (last, last * planes)],
            dma(3), dma(2 * tp),
            dma(3), dma(2 * tp), dma(1), dma(1), dma(1), dma(3), dma(1), dma(1),
            dma(2), dma(2), dma(2), dma(2),
            dma(last), dma(2 * last), dma(2 * last), dma(2 * last),
            dma(1), dma(6), dma(1), dma(2), dma(1), dma(1),
        ],
        compiler_params=pltpu.CompilerParams(
            collective_id=0, has_side_effects=True, vmem_limit_bytes=60 * 1024 * 1024),
    )(tokens, norm_gain, w_value, w_gate, w_out, conv_taps, conv_bias, ln_gain, ln_shift)


def fits(mesh, tokens, conv_taps, w_out):
    n, tp = mesh.shape["sp"], mesh.shape["tp"]
    layers, ntaps, lch = conv_taps.shape
    rows, feats = tokens.shape
    return (tp == 4 and n == 2 * tp and ntaps % 2 == 1 and ntaps // 2 < 16 and layers > 1
            and w_out.shape[2] % 128 == 0 and lch % 128 == 0 and feats % 128 == 0
            and feats == 2 * w_out.shape[2]
            and rows % 64 == 0 and rows >= 32 * layers and rows <= 512
            and layers * w_out.shape[1] * w_out.shape[2] * n * 12 <= 20 * 1024 * 1024)


def solution(mesh):
    placed = (
        P("sp", "tp"),
        P(),
        P(None, "sp", "tp"),
        P(None, "sp", "tp"),
        P(None, None, "tp"),
        P(None, "tp"),
        P(None, "tp"),
        P(None, "tp"),
        P(None, "tp", "sp"),
    )

    def run(*args):
        if fits(mesh, args[0], args[4], args[8]):
            return fused_call(mesh, *args)
        return body(*args)

    return jax.shard_map(run, mesh=mesh, in_specs=placed, out_specs=P("sp", "tp"), check_vma=False)
```

```python
import functools

import jax
import jax.numpy as jnp
from jax import lax
from jax.experimental import pallas as pl
from jax.experimental.pallas import tpu as pltpu
from jax.sharding import PartitionSpec as P

MESH = pl.DeviceIdType.MESH

norm_floor = 0.01


def with_halo(array, sides, width):
    for axis, dim in sides:
        size, length = (lax.axis_size(axis), array.shape[dim])
        up = [(i, (i + 1) % size) for i in range(size - 1)]
        down = [(j, i) for i, j in up]
        last = lax.slice_in_dim(array, length - width, length, axis=dim)
        first = lax.slice_in_dim(array, 0, width, axis=dim)
        before = lax.ppermute(last, axis, up)
        after = lax.ppermute(first, axis, down)
        array = jnp.concatenate([before, array, after], axis=dim)
    return array


def body(tokens, norm_gain, w_value, w_gate, conv_taps, conv_bias, ln_gain, ln_shift, w_out):
    stream = tokens
    layer_count = w_value.shape[0]
    reach = conv_taps.shape[1] // 2
    local_channels = w_value.shape[2]
    channels = local_channels * lax.axis_size("tp")
    tok_rows = tokens.shape[0]
    whole_value, whole_gate = (
        lax.all_gather(w_value, "sp", axis=1, tiled=True),
        lax.all_gather(w_gate, "sp", axis=1, tiled=True),
    )
    whole_out = lax.all_gather(w_out, "sp", axis=2, tiled=True)
    for layer_index in range(layer_count):
        whole_rows = lax.all_gather(stream, "tp", axis=1, tiled=True)
        rows_f32 = whole_rows.astype(jnp.float32)
        scale_rows = lax.rsqrt(jnp.mean(rows_f32 * rows_f32, axis=-1, keepdims=True) + norm_floor)
        normed = (rows_f32 * scale_rows * norm_gain[layer_index]).astype(jnp.bfloat16)
        value_rows = jnp.dot(normed, whole_value[layer_index], preferred_element_type=jnp.float32)
        gate_rows = jnp.dot(normed, whole_gate[layer_index], preferred_element_type=jnp.float32)
        gated_input = (value_rows * jax.nn.sigmoid(gate_rows)).astype(jnp.bfloat16)
        padded = with_halo(gated_input, (("sp", 0),), reach)
        padded = padded.astype(jnp.float32)
        convolved = jnp.zeros((tok_rows, local_channels), jnp.float32) + conv_bias[layer_index]
        for offset in range(2 * reach + 1):
            convolved = (
                convolved + conv_taps[layer_index, offset] * padded[offset : offset + tok_rows]
            )
        moments = lax.psum(
            (
                jnp.sum(convolved, axis=-1, keepdims=True),
                jnp.sum(convolved * convolved, axis=-1, keepdims=True),
            ),
            "tp",
        )
        average = moments[0] / channels
        spread = moments[1] / channels - average * average
        activated = jax.nn.silu(
            (convolved - average) * lax.rsqrt(spread + norm_floor) * ln_gain[layer_index]
            + ln_shift[layer_index]
        ).astype(jnp.bfloat16)
        partial_rows = jnp.dot(
            activated, whole_out[layer_index], preferred_element_type=jnp.float32
        )
        summed = lax.psum_scatter(
            partial_rows.astype(jnp.bfloat16), "tp", scatter_dimension=1, tiled=True
        ).astype(jnp.float32)
        stream = (stream.astype(jnp.float32) + summed).astype(jnp.bfloat16)
    return stream


def fused(
    dims,
    tok_in, gain_hbm, wv_in, wg_in, wo_in, taps_in, bias_in, lng_in, lns_in,
    out,
    tok, gain_in, result, wvg, wo, taps, bias, lng, lns, stream, normed, gated, cv, cv2, act, resid, rowa, rowb,
    loc_sem, in_sem, out_sem, pre_send, pre_recv, z_send, z_recv, d_send, d_recv,
    a_send, a_recv, b_send, b_recv, r_send, r_recv, o_send, o_recv,
    tok_send, tok_recv, zh_send, zh_recv, hp_send, hp_recv, ih_send, ih_recv,
    par_send, par_recv, ln_send, ln_recv,
    cv_send, ca_recv, cb_recv, cr_recv,
    l_send, l_recv, p_send, p_recv, res_send, res_recv,
):
    n, tp, layers, ntaps, rows, width, chans = dims
    planes = n // 2
    feats = width // tp
    lch = chans // tp
    krows = width // n
    ocols = width // n
    reach = ntaps // 2
    grain = 16
    halo = grain * layers
    window = rows + 2 * halo
    last = layers - 1
    lanes = 128
    per_side = lch // lanes
    per_out = feats // ocols

    sp = lax.axis_index("sp")
    t = lax.axis_index("tp")
    z, y = sp // 2, lax.rem(sp, 2)
    x, h = t // 2, lax.rem(t, 2)
    xn, yn, hn = 1 - x, 1 - y, 1 - h
    same = 1 - (y + h - 2 * y * h)
    spn = 2 * z + yn
    has_up, has_down = 1 - (z + 1) // planes, jnp.minimum(z, 1)

    partner = (sp, 2 * x + hn)
    xdev = (sp, 2 * xn + h)
    ydev = (spn, t)
    ax, ay = hn * xn + h * x, hn * y + h * yn
    bx, by = hn * x + h * xn, hn * yn + h * y
    adev = (2 * z + ay, 2 * ax + h)
    bdev = (2 * z + by, 2 * bx + h)

    def rcopy(src, dst, ssem, rsem, dev):
        return pltpu.make_async_remote_copy(
            src_ref=src, dst_ref=dst, send_sem=ssem, recv_sem=rsem,
            device_id=dev, device_id_type=MESH)

    def arrived(ref, ssem, rsem):
        rcopy(ref, ref, ssem, rsem, partner).wait_recv()

    def sent(ref, ssem):
        rcopy(ref, ref, ssem, ssem, partner).wait_send()

    def when(flag):
        return pl.when(flag == 1)

    def vblock(l, k, zs, c):
        r = pl.ds(pl.multiple_of((2 * zs + c) * krows, krows), krows)
        return wvg.at[l, k, r, :]

    def oblock(l, zs, yy, cb):
        r = pl.ds(pl.multiple_of(cb * lch, lch), lch)
        return wo.at[l, 2 * zs + yy, r, :]

    def item(l, k, zs):
        return vblock(l, k, zs, h) if k < 2 else oblock(l, zs, y, t)

    def local_copy(l, k):
        src = (wv_in, wg_in, wo_in)[k].at[l]
        return pltpu.make_async_copy(src, item(l, k, z), loc_sem.at[3 * l + k])

    def pre_copy(l, k):
        src = (wv_in, wg_in)[k].at[l]
        i = 2 * l + k
        return rcopy(src, vblock(l, k, z, y), pre_send.at[0], pre_recv.at[i], (spn, 2 * x + hn))

    def z_parts(l, k, d, s):
        zs = z - s if d == 0 else z + s
        return item(l, k, zs), z_recv.at[(l * 3 + k) * (planes - 1) + zs - d]

    def z_copy(l, k, d, s):
        ref, rsem = z_parts(l, k, d, s)
        return rcopy(ref, ref, z_send.at[d * (planes - 1) + s], rsem, (sp + (2 if d == 0 else -2), t))

    def z_wait(l, k, d, s):
        ref, rsem = z_parts(l, k, d, s)
        arrived(ref, z_send.at[0], rsem)

    def d_copy(l, k, zs, ref):
        i, j = (l, l) if k < 2 else (layers + l, layers + l * planes + zs)
        return rcopy(ref, ref, d_send.at[i], d_recv.at[j], partner)

    def a_copy(l, zs):
        ref = oblock(l, zs, y, t)
        return rcopy(ref, ref, a_send.at[l], a_recv.at[l * planes + zs], adev)

    def b_copy(l, zs):
        ref = oblock(l, zs, y, t)
        return rcopy(ref, ref, b_send.at[l], b_recv.at[l * planes + zs], bdev)

    def from_a(l, zs):
        return oblock(l, zs, ay, 2 * ax + h)

    def from_b(l, zs):
        return oblock(l, zs, by, 2 * bx + h)

    def r_copy(l, zs):
        ref = from_a(l, zs)
        return rcopy(ref, ref, r_send.at[l], r_recv.at[l * planes + zs], bdev)

    def o_copy(rel, zs):
        ref = oblock(last, zs, y, t)
        return rcopy(ref, ref, o_send.at[rel], o_recv.at[2 * t + rel],
                     (sp if rel == 0 else spn, zs))

    def differs(a, b):
        return jnp.minimum(jnp.abs(a - b), 1)

    def to_partner(l, k, zs):
        if k < 2 or l < last:
            d_copy(l, k, zs, item(l, k, zs)).start()

    def spread(l, s):
        for flag, zs in groups(s):
            def go(zs=zs):
                if l < last:
                    a_copy(l, zs).start()
                    b_copy(l, zs).start()
                else:
                    when(differs(zs, t))(lambda: o_copy(0, zs).start())
                    far = 1 if s == planes - 1 else 1 - differs(zs // 2, x)
                    when(far)(lambda: o_copy(1, zs).start())
            guarded(flag, go)

    def o_pass(c):
        owner = 2 * xn + c
        ref = oblock(last, t, y, owner)
        return rcopy(ref, ref, o_send.at[2], o_recv.at[2 * owner + 1], ydev)

    def o_relay(s):
        @when(1 - differs(jnp.abs(z - t), s))
        def _():
            for c in range(2):
                owner = 2 * xn + c
                arrived(oblock(last, t, y, owner), o_send.at[0], o_recv.at[2 * owner])
                if s < planes - 1:
                    o_pass(c).start()

    def own_start(l, k):
        if k < 2:
            when(same)(lambda: local_copy(l, k).wait())

            @when(1 - same)
            def _():
                i = 2 * l + k
                arrived(item(l, k, z), pre_send.at[0], pre_recv.at[i])
        else:
            local_copy(l, k).wait()
        when(has_up)(lambda: z_copy(l, k, 0, 0).start())
        when(has_down)(lambda: z_copy(l, k, 1, 0).start())
        to_partner(l, k, z)

    def below(s):
        return jnp.minimum(z // s, 1)

    def above(s):
        return jnp.minimum((planes - 1 - z) // s, 1)

    def groups(s):
        if s == 0:
            return [(None, z)]
        return [(below(s), z - s), (above(s), z + s)]

    def guarded(flag, f):
        if flag is None:
            f()
        else:
            when(flag)(f)

    def z_recv_step(l, k, s):
        for d, (flag, zs) in enumerate(groups(s)):
            def go(d=d, zs=zs):
                z_wait(l, k, d, s)
                if s < planes - 1:
                    when((has_up, has_down)[d])(lambda: z_copy(l, k, d, s).start())
                to_partner(l, k, zs)
            guarded(flag, go)

    def a_step(l, s):
        for flag, zs in groups(s):
            def go(zs=zs):
                ref = from_a(l, zs)
                arrived(ref, a_send.at[0], a_recv.at[l * planes + zs])
                r_copy(l, zs).start()
                d_copy(l, 2, zs, ref).start()
            guarded(flag, go)

    def b_step(l, s):
        for flag, zs in groups(s):
            def go(zs=zs):
                ref = from_b(l, zs)
                arrived(ref, b_send.at[0], b_recv.at[l * planes + zs])
                d_copy(l, 2, zs, ref).start()
            guarded(flag, go)

    def r_step(l, s):
        for flag, zs in groups(s):
            def go(zs=zs):
                ref = oblock(l, zs, yn, 2 * xn + h)
                arrived(ref, r_send.at[0], r_recv.at[l * planes + zs])
                d_copy(l, 2, zs, ref).start()
            guarded(flag, go)

    def v_half(l):
        return wvg.at[l, :, pl.ds(0, width // 2), :]

    def need_v(l):
        arrived(v_half(l), d_send.at[0], d_recv.at[l])

    def need_last():
        mate = 2 * x + hn
        arrived(oblock(last, t, y, mate), o_send.at[0], o_recv.at[2 * mate])
        for j in range(tp):
            other = lax.rem(t + j, tp)
            arrived(oblock(last, t, yn, other), o_send.at[0], o_recv.at[2 * other + 1])

    def v_sent():
        when(1 - same)(lambda: sent(wvg.at[:, :, pl.ds(0, krows), :], pre_send.at[0]))
        for l in range(layers):
            sent(v_half(l), d_send.at[l])
        for s in range(planes - 1):
            for d, flag in enumerate((has_up, has_down)):
                ok = flag if s == 0 else flag * (below(s), above(s))[d]
                ref = wvg.at[:, :, pl.ds(0, 3 * krows // 2), :]
                when(ok)(lambda d=d, s=s, ref=ref: sent(ref, z_send.at[d * (planes - 1) + s]))

    def o_sent():
        for l in range(last):
            sent(wo.at[l, pl.ds(0, planes)], d_send.at[layers + l])
            for sem in (a_send, b_send, r_send):
                sent(wo.at[l, 0], sem.at[l])

    def o_last_sent():
        def some(i, count):
            sent(wo.at[last, 0, pl.ds(0, count * lch), :], o_send.at[i])

        at_end = 1 - differs(jnp.abs(planes - 1 - 2 * z), planes - 1)
        extra = at_end * differs((planes - 1 - z) // 2, x)
        some(0, tp - 1)
        when(extra)(lambda: some(1, 3))
        when(1 - extra)(lambda: some(1, 2))
        when(differs(jnp.abs(z - t), planes - 1))(lambda: some(2, 2))

    def cols(owner):
        return pl.ds(pl.multiple_of(owner * feats, feats), feats)

    tcols = cols(t)

    half_rows = rows // 2

    def hcols(owner, part):
        return stream.at[pl.ds(halo + part * half_rows, half_rows), cols(owner)]

    def tok_copy(j, p):
        dev = ((sp, 2 * x + y), (sp, 2 * xn + y), (spn, 2 * x + y))[j]
        return rcopy(tok.at[pl.ds(p * half_rows, half_rows), :], hcols(t, p),
                     tok_send.at[min(j, 1)], tok_recv.at[2 * t + p], dev)

    def tok_start(j):
        tok_copy(j, 0).start()
        tok_copy(j, 1).start()

    def tok_pass(j):
        owner, p, dev = (
            (2 * xn + yn, 0, ydev), (2 * x + yn, 0, xdev),
            (2 * x + yn, 1, xdev), (2 * x + y, 1, xdev))[j]
        ref = hcols(owner, p)
        return rcopy(ref, ref, tok_send.at[2], tok_recv.at[2 * owner + p], dev)

    def tok_starts():
        when(1 - same)(lambda: tok_start(0))
        tok_start(1)

        @when(same)
        def _():
            stream[pl.ds(halo, rows), tcols] = tok[...]

    def tok_arrived(owner, p):
        arrived(hcols(owner, p), tok_send.at[0], tok_recv.at[2 * owner + p])

    def tok_relay(step):
        @when(same)
        def _():
            if step == 0:
                tok_arrived(2 * xn + yn, 0)
                tok_pass(0).start()

        @when(1 - same)
        def _():
            if step == 0:
                tok_arrived(2 * x + yn, 0)
                tok_pass(1).start()
            elif step == 1:
                tok_arrived(2 * x + yn, 1)
                tok_pass(2).start()
            else:
                tok_arrived(2 * x + y, 1)
                tok_pass(3).start()

    def tok_waits():
        @when(same)
        def _():
            tok_arrived(2 * xn + yn, 1)
            for p in range(2):
                tok_arrived(2 * x + hn, p)
                tok_arrived(2 * xn + y, p)

        @when(1 - same)
        def _():
            tok_arrived(2 * x + y, 0)
            for p in range(2):
                tok_arrived(2 * xn + yn, p)
                tok_arrived(2 * xn + y, p)

    zh_to = y * has_up + yn * has_down
    zh_from = hn * has_down + h * has_up

    def edge(owner_cols, side):
        r = pl.ds(pl.multiple_of(side * (halo + rows), grain), halo)
        return stream.at[r, owner_cols]

    def zh_copy():
        src = tok.at[pl.ds(pl.multiple_of(y * (rows - halo), grain), halo), :]
        return rcopy(src, edge(tcols, yn), zh_send.at[0], zh_recv.at[0],
                     (sp + 4 * y - 2, 2 * x + yn))

    def half_cols(xx):
        return pl.ds(pl.multiple_of(xx * 2 * feats, feats), 2 * feats)

    def hp_copy(j):
        ref = edge(half_cols(xn if j == 2 else x), h)
        return rcopy(ref, ref, hp_send.at[0], hp_recv.at[j], xdev if j == 0 else ydev)

    def halo_pass():
        @when(zh_from * (1 - same))
        def _():
            arrived(edge(half_cols(x), h), zh_send.at[0], zh_recv.at[0])
            hp_copy(0).start()
            hp_copy(1).start()

        @when(1 - zh_from)
        def _():
            stream[pl.ds(pl.multiple_of(h * (halo + rows), grain), halo), :] = jnp.zeros((halo, width), jnp.bfloat16)

    def halo_pass_on():
        @when(zh_from * (1 - same))
        def _():
            arrived(edge(half_cols(xn), h), hp_send.at[0], hp_recv.at[0])
            hp_copy(2).start()

    def halo_waits():
        @when(zh_from * same)
        def _():
            arrived(edge(half_cols(x), h), hp_send.at[0], hp_recv.at[1])
            arrived(edge(half_cols(xn), h), hp_send.at[0], hp_recv.at[2])

    def ih_copy():
        src = stream.at[pl.ds(pl.multiple_of(hn * rows + h * halo, grain), halo), :]
        dst = stream.at[pl.ds(pl.multiple_of(h * (halo + rows), grain), halo), :]
        return rcopy(src, dst, ih_send.at[0], ih_recv.at[0], partner)

    def ih_wait():
        ref = stream.at[pl.ds(pl.multiple_of(hn * (halo + rows), grain), halo), :]
        arrived(ref, ih_send.at[0], ih_recv.at[0])

    def par_copy(i):
        a, b = ((taps_in, taps), (bias_in, bias))[i]
        return rcopy(a, b, par_send.at[i], par_recv.at[i], partner)

    def ln_copy(i, j):
        a, b = ((lng_in, lng), (lns_in, lns))[i]
        return rcopy(a, b.at[t], ln_send.at[i], ln_recv.at[i],
                     (sp, lax.rem(t + j, tp)))

    def params_start():
        for i in range(2):
            when(same)(lambda i=i: par_copy(i).start())
            for j in range(1, tp):
                ln_copy(i, j).start()


    def in_copies():
        return [
            pltpu.make_async_copy(a, b, in_sem.at[i])
            for i, (a, b) in enumerate((
                (tok_in, tok), (gain_hbm, gain_in), (lng_in, lng.at[t]), (lns_in, lns.at[t]),
                (taps_in, taps), (bias_in, bias)))
        ]

    def in_start():
        for i, c in enumerate(in_copies()):
            if i < 4:
                c.start()
            else:
                when(same)(lambda c=c: c.start())

    def out_copy(i):
        r0, size = piece(last, i)
        r = pl.ds(r0, size)
        return pltpu.make_async_copy(result.at[r, :], out.at[r, :], out_sem.at[i])

    def params_wait():
        for i, c in enumerate(in_copies()):
            if i >= 4:
                when(same)(lambda c=c: c.wait())
            elif i > 0:
                c.wait()
        for i, ref in enumerate((taps, bias)):
            when(1 - same)(lambda i=i, ref=ref: arrived(ref, par_send.at[i], par_recv.at[i]))
        for i, ref in enumerate((lng, lns)):
            arrived(ref.at[pl.ds(0, tp - 1)], ln_send.at[0], ln_recv.at[i])

    def small_sent():
        when(1 - same)(lambda: sent(tok, tok_send.at[0]))
        sent(stream.at[pl.ds(0, rows), pl.ds(0, 2 * feats)], tok_send.at[1])
        when(zh_to)(lambda: zh_copy().wait_send())
        for i, ref in enumerate((lng, lns)):
            when(same)(lambda i=i: par_copy(i).wait_send())
            sent(ref.at[pl.ds(0, tp - 1)], ln_send.at[i])

    def stream_sent():
        for flag, count in ((same, 1), (1 - same, 3)):
            ref = stream.at[pl.ds(0, half_rows), pl.ds(0, count * feats)]
            when(flag)(lambda ref=ref: sent(ref, tok_send.at[2]))
        ref = stream.at[pl.ds(0, 3 * halo), pl.ds(0, 2 * feats)]
        when(zh_from * (1 - same))(lambda: sent(ref, hp_send.at[0]))
        ih_copy().wait_send()

    cb_own = 2 * x + y
    cb_a, cb_b, cb_d = 2 * ax + ay, 2 * bx + by, 2 * xn + yn

    def piece(l, i):
        total = window - 2 * grain * (l + 1)
        first = total - rows // 2
        return i * first, total - first if i else first

    def cblock(l, i, cb):
        r0, size = piece(l, i)
        return cv.at[l, cb, pl.ds(r0, size), :]

    def cv_copy(l, i, j):
        ref = cblock(l, i, cb_a if j == 2 else cb_own)
        r = (ca_recv, cb_recv, cr_recv)[j]
        return rcopy(ref, ref, cv_send.at[l], r.at[2 * l + i], adev if j == 0 else bdev)

    def cv_start(l, i):
        cv_copy(l, i, 0).start()
        cv_copy(l, i, 1).start()

    def cv_relay(l, i):
        arrived(cblock(l, i, cb_a), cv_send.at[0], ca_recv.at[2 * l + i])
        cv_copy(l, i, 2).start()

    def cv_waits(l, i):
        arrived(cblock(l, i, cb_b), cv_send.at[0], cb_recv.at[2 * l + i])
        arrived(cblock(l, i, cb_d), cv_send.at[0], cr_recv.at[2 * l + i])

    def lblock(i, cb):
        r0, size = piece(last, i)
        return cv2.at[cb, pl.ds(r0, size), :]

    def l_copy(i, j):
        src, cb, dev = (
            (cblock(last, i, cb_own), cb_own, ydev),
            (cblock(last, i, cb_own), cb_own, xdev),
            (lblock(i, 2 * x + yn), 2 * x + yn, xdev),
        )[j]
        return rcopy(src, lblock(i, cb), l_send.at[0], l_recv.at[3 * i + j], dev)

    def p_copy(i, j):
        cb = (cb_own, 2 * x + yn, 2 * xn + y, 2 * xn + yn)[j]
        src = cblock(last, i, cb) if j == 0 else lblock(i, cb)
        return rcopy(src, lblock(i, cb), p_send.at[0], p_recv.at[i], partner)

    def last_start(i):
        r0, size = piece(last, i)
        when(1 - same)(lambda: l_copy(i, 0).start())

        @when(same)
        def _():
            l_copy(i, 1).start()
            p_copy(i, 0).start()
            cv2[cb_own, r0:r0 + size, :] = cv[last, cb_own, r0:r0 + size, :]

    def last_relay(i):
        @when(same)
        def _():
            arrived(lblock(i, 2 * x + yn), l_send.at[0], l_recv.at[3 * i])
            l_copy(i, 2).start()
            p_copy(i, 1).start()

    def last_waits(i):
        @when(same)
        def _():
            for j in (1, 2):
                cb = 2 * xn + (y if j == 1 else yn)
                arrived(lblock(i, cb), l_send.at[0], l_recv.at[3 * i + j])
                p_copy(i, j + 1).start()

        r0, size = piece(last, i)
        when(1 - same)(lambda: arrived(cv2.at[:, pl.ds(r0, size), :], p_send.at[0], p_recv.at[i]))

    def conv_sent():
        for l in range(last):
            total = window - 2 * grain * (l + 1)
            sent(cv.at[l, pl.ds(0, 3), pl.ds(0, total), :], cv_send.at[l])

    def last_sent():
        when(1 - same)(lambda: sent(cv2.at[0], l_send.at[0]))

        @when(same)
        def _():
            sent(cv2.at[pl.ds(0, 2)], l_send.at[0])
            sent(cv2, p_send.at[0])

    def res_copy():
        src = stream.at[pl.ds(halo, rows), cols(2 * x + hn)]
        return rcopy(src, resid, res_send.at[0], res_recv.at[0], partner)

    def res_start():
        @when(same)
        def _():
            res_copy().start()
            resid[...] = stream[pl.ds(halo, rows), tcols]

    def res_wait():
        when(1 - same)(lambda: arrived(resid, res_send.at[0], res_recv.at[0]))

    first_row = (2 * z + h) * rows - halo
    total_rows = n * rows

    def over_rows(start, size, block, f):
        def step(i, carry):
            f(pl.ds(pl.multiple_of(start + i * block, grain), block))
            return carry

        lax.fori_loop(0, size // block, step, 0)

    def chunk(layer, i):
        r0, size = piece(layer - 1, i)
        return grain * layer + r0, size

    def normalize(layer, i):
        w0, size = chunk(layer, i)
        block = 2 * grain

        def squares(r):
            total = jnp.zeros((block, lanes), jnp.float32)
            for c in range(width // lanes):
                v = stream[r, c * lanes:(c + 1) * lanes].astype(jnp.float32)
                total = total + v * v
            rowa[r, :] = total

        def scaled(r):
            scale = rowa[r, :]
            for c in range(width // lanes):
                lane = slice(c * lanes, (c + 1) * lanes)
                v = stream[r, lane].astype(jnp.float32)
                normed[r, lane] = (v * scale * gain_in[layer:layer + 1, lane]).astype(jnp.bfloat16)

        over_rows(w0, size, block, squares)
        mean = jnp.sum(rowa[w0:w0 + size, :], axis=-1, keepdims=True) / width
        rowa[w0:w0 + size, :] = jnp.broadcast_to(lax.rsqrt(mean + norm_floor), (size, lanes))
        over_rows(w0, size, block, scaled)

    def project(layer, i):
        w0, size = chunk(layer, i)
        value = jnp.dot(normed[w0:w0 + size, :], wvg[layer, 0], preferred_element_type=jnp.float32)
        gate = jnp.dot(normed[w0:w0 + size, :], wvg[layer, 1], preferred_element_type=jnp.float32)
        g = (value * (0.5 + 0.5 * jnp.tanh(0.5 * gate))).astype(jnp.bfloat16).astype(jnp.float32)
        row = lax.broadcasted_iota(jnp.int32, (size, lch), 0) + (first_row + w0)
        g = jnp.where(jnp.logical_and(row >= 0, row < total_rows), g, 0.0)
        for b in range(per_side):
            gated[b, w0:w0 + size, :] = g[:, b * lanes:(b + 1) * lanes]

    def convolve(layer, i):
        r0, size = piece(layer, i)
        start = grain * (layer + 1)
        cut = -(-size // 2 // grain) * grain
        for c0, part in ((r0, cut), (r0 + cut, size - cut)):
            def lane_block(b, carry, c0=c0, part=part):
                lane = pl.ds(pl.multiple_of(b * lanes, lanes), lanes)
                total = jnp.zeros((part, lanes), jnp.float32) + bias[layer:layer + 1, lane]
                for k in range(ntaps):
                    first = start + c0 + k - reach
                    total = total + taps[layer, k:k + 1, lane] * gated[b, first:first + part, :]
                cv[layer, cb_own, c0:c0 + part, lane] = total.astype(jnp.bfloat16)
                return carry

            lax.fori_loop(0, per_side, lane_block, 0)

    def activate(layer, i):
        r0, size = piece(layer, i)
        block = 2 * grain if size % (2 * grain) == 0 else grain
        parts = [(b, c) for b in range(tp) for c in range(per_side)]

        def load(b, c, r):
            lane = slice(c * lanes, (c + 1) * lanes)
            return (cv[layer, b, r, lane] if layer < last else cv2[b, r, lane]).astype(jnp.float32)

        def sums(r):
            s1 = jnp.zeros((block, lanes), jnp.float32)
            s2 = jnp.zeros((block, lanes), jnp.float32)
            for b, c in parts:
                v = load(b, c, r)
                s1 = s1 + v
                s2 = s2 + v * v
            rowa[r, :] = s1
            rowb[r, :] = s2

        def apply(r):
            scale, shift = rowa[r, :], rowb[r, :]
            for b, c in parts:
                lane = slice(c * lanes, (c + 1) * lanes)
                u = (load(b, c, r) - shift) * scale
                u = 0.5 * (u * lng[b, layer:layer + 1, lane] + lns[b, layer:layer + 1, lane])
                act[r, b * lch + c * lanes:b * lch + (c + 1) * lanes] = (u + u * jnp.tanh(u)).astype(jnp.bfloat16)

        over_rows(r0, size, block, sums)
        rows_ = slice(r0, r0 + size)
        average = jnp.sum(rowa[rows_, :], axis=-1, keepdims=True) / chans
        spread_ = jnp.sum(rowb[rows_, :], axis=-1, keepdims=True) / chans - average * average
        rowa[rows_, :] = jnp.broadcast_to(lax.rsqrt(spread_ + norm_floor), (size, lanes))
        rowb[rows_, :] = jnp.broadcast_to(average, (size, lanes))
        over_rows(r0, size, block, apply)

    def expand_wait(layer, s):
        for flag, zs in groups(s):
            sem = d_recv.at[layers + layer * planes + zs]
            guarded(flag, lambda sem=sem: arrived(wo.at[layer, 0], d_send.at[0], sem))

    def expand(layer, s, pieces=(0, 1)):
        for flag, zs in groups(s):
            def go(zs=zs):
                def step(j, carry):
                    c = pl.ds(pl.multiple_of((2 * zs + j) * ocols, ocols), ocols)
                    for i in pieces:
                        r0, size = piece(layer, i)
                        w0 = grain * (layer + 1) + r0
                        add = jnp.dot(act[r0:r0 + size, :], wo[layer, 2 * zs + j], preferred_element_type=jnp.float32)
                        stream[w0:w0 + size, c] = (stream[w0:w0 + size, c].astype(jnp.float32) + add).astype(jnp.bfloat16)
                    return carry

                lax.fori_loop(0, 2, step, 0)
            guarded(flag, go)

    def finish(i):
        r0, size = piece(last, i)
        for j in range(per_out):
            c = slice(j * ocols, (j + 1) * ocols)
            add = jnp.dot(act[r0:r0 + size, :], wo[last, per_out * t + j], preferred_element_type=jnp.float32)
            result[r0:r0 + size, c] = (resid[r0:r0 + size, c].astype(jnp.float32) + add).astype(jnp.bfloat16)

    barrier = pltpu.get_barrier_semaphore()
    in_start()
    for l in range(layers):
        for k in range(3):
            if k < 2:
                when(same)(lambda l=l, k=k: local_copy(l, k).start())
            else:
                local_copy(l, k).start()
    for ds in range(2):
        for j in range(tp):
            if ds or j:
                pl.semaphore_signal(barrier, inc=1, device_id=((sp, spn)[ds], lax.rem(t + j, tp)), device_id_type=MESH)
    for flag, step in ((has_up, 2), (has_down, -2)):
        @when(flag)
        def _(step=step):
            for c in range(2):
                pl.semaphore_signal(barrier, inc=1, device_id=(sp + step, 2 * x + c), device_id_type=MESH)
    pl.semaphore_wait(barrier, 2 * tp - 1 + 2 * (has_up + has_down))
    in_copies()[0].wait()

    def pre_start(l):
        for k in range(2):
            when(1 - same)(lambda k=k: pre_copy(l, k).start())

    pre_start(0)
    when(zh_to)(lambda: zh_copy().start())
    tok_starts()
    halo_pass()
    when(1 - same)(lambda: tok_start(2))
    params_start()
    own_start(0, 0)
    own_start(0, 1)
    when(same)(lambda: own_start(0, 2))
    z_recv_step(0, 0, 1)
    when(same)(lambda: tok_start(2))
    z_recv_step(0, 1, 1)
    tok_relay(0)
    when(1 - same)(lambda: own_start(0, 2))
    halo_pass_on()
    tok_relay(1)
    z_recv_step(0, 0, 2)
    tok_relay(2)
    pre_start(1)
    z_recv_step(0, 1, 2)
    spread(0, 0)
    z_recv_step(0, 2, 1)
    tok_waits()
    ih_copy().start()

    def first_weights_in():
        z_recv_step(0, 0, 3)
        z_recv_step(0, 1, 3)

    when(same)(first_weights_in)
    halo_waits()
    ih_wait()
    params_wait()
    normalize(0, 0)
    normalize(0, 1)
    when(1 - same)(first_weights_in)
    own_start(1, 0)
    own_start(1, 1)
    spread(0, 1)
    need_v(0)
    for i in range(2):
        project(0, i)
        convolve(0, i)
        cv_start(0, i)
        if i == 0:
            a_step(0, 0)
            z_recv_step(0, 2, 2)

    def layer_end(layer, between):
        after = layer + 1
        expand_wait(layer, 3)
        for i in range(2):
            expand(layer, 3, (i,))
            normalize(after, i)
            project(after, i)
            convolve(after, i)
            if after < last:
                cv_start(after, i)
            else:
                last_start(i)
            if i == 0:
                between()

    for layer in range(last - 1):
        after = layer + 1
        beyond = layer + 2
        z_recv_step(after, 0, 1)
        cv_relay(layer, 0)
        z_recv_step(after, 1, 1)
        cv_relay(layer, 1)
        spread(layer, 2)
        z_recv_step(layer, 2, 3)
        spread(layer, 3)
        if layer == 0:
            pre_start(2)
        z_recv_step(after, 0, 2)
        b_step(layer, 0)
        a_step(layer, 1)
        cv_waits(layer, 0)
        activate(layer, 0)
        z_recv_step(after, 1, 2)
        own_start(after, 2)
        cv_waits(layer, 1)
        activate(layer, 1)
        r_step(layer, 0)
        a_step(layer, 2)
        if layer == 0:
            stream_sent()
        expand_wait(layer, 0)
        expand(layer, 0)
        z_recv_step(after, 0, 3)
        b_step(layer, 1)
        a_step(layer, 3)
        z_recv_step(after, 1, 3)
        r_step(layer, 1)
        spread(after, 0)
        z_recv_step(after, 2, 1)
        own_start(beyond, 2)
        own_start(beyond, 0)
        own_start(beyond, 1)
        expand_wait(layer, 1)
        expand(layer, 1)
        b_step(layer, 2)
        r_step(layer, 2)
        expand_wait(layer, 2)
        expand(layer, 2)
        b_step(layer, 3)
        need_v(after)
        r_step(layer, 3)
        spread(after, 1)
        layer_end(layer, lambda: z_recv_step(after, 2, 2))
        a_step(after, 0)

    layer = last - 1
    z_recv_step(layer, 2, 3)
    z_recv_step(last, 2, 1)
    cv_relay(layer, 0)
    z_recv_step(last, 0, 1)
    cv_relay(layer, 1)
    spread(layer, 2)
    spread(layer, 3)
    z_recv_step(last, 2, 2)
    b_step(layer, 0)
    a_step(layer, 1)
    z_recv_step(last, 1, 1)
    cv_waits(layer, 0)
    activate(layer, 0)
    z_recv_step(last, 0, 2)
    cv_waits(layer, 1)
    activate(layer, 1)
    r_step(layer, 0)
    a_step(layer, 2)
    z_recv_step(last, 2, 3)
    expand_wait(layer, 0)
    expand(layer, 0)
    z_recv_step(last, 1, 2)
    b_step(layer, 1)
    a_step(layer, 3)
    r_step(layer, 1)
    spread(last, 0)
    spread(last, 1)
    spread(last, 2)
    spread(last, 3)
    z_recv_step(last, 0, 3)
    expand_wait(layer, 1)
    expand(layer, 1)
    b_step(layer, 2)
    r_step(layer, 2)
    z_recv_step(last, 1, 3)
    o_relay(0)
    expand_wait(layer, 2)
    expand(layer, 2)
    b_step(layer, 3)
    need_v(last)
    o_relay(1)
    r_step(layer, 3)
    layer_end(layer, lambda: None)
    res_start()
    o_relay(2)
    last_relay(0)
    last_relay(1)
    res_wait()
    o_sent()
    small_sent()
    conv_sent()
    last_waits(0)
    activate(last, 0)
    last_waits(1)
    o_relay(3)
    need_last()
    finish(0)
    out_copy(0).start()
    activate(last, 1)
    finish(1)
    out_copy(1).start()
    v_sent()
    o_last_sent()
    last_sent()
    when(same)(lambda: res_copy().wait_send())
    for i in range(2):
        out_copy(i).wait()


def fused_call(mesh, *args):
    tokens, norm_gain, w_value, w_gate, conv_taps, conv_bias, ln_gain, ln_shift, w_out = args
    n, tp = mesh.shape["sp"], mesh.shape["tp"]
    layers, ntaps, lch = conv_taps.shape
    rows, feats = tokens.shape
    width, chans = feats * tp, lch * tp
    planes = n // 2
    last = layers - 1
    halo = 16 * layers
    window = rows + 2 * halo
    most = window - 32
    dims = (n, tp, layers, ntaps, rows, width, chans)
    anys = pl.BlockSpec(memory_space=pl.ANY)
    bf, f32 = jnp.bfloat16, jnp.float32
    dma = lambda k: pltpu.SemaphoreType.DMA((k,))
    return pl.pallas_call(
        functools.partial(fused, dims),
        out_shape=jax.ShapeDtypeStruct((rows, feats), bf),
        in_specs=[anys] * 9,
        out_specs=anys,
        scratch_shapes=[
            pltpu.VMEM((rows, feats), bf),
            pltpu.VMEM(norm_gain.shape, f32),
            pltpu.VMEM((rows, feats), bf),
            pltpu.VMEM((layers, 2, width, lch), bf),
            pltpu.VMEM((layers, n, chans, width // n), bf),
            pltpu.VMEM(conv_taps.shape, f32),
            pltpu.VMEM(conv_bias.shape, f32),
            pltpu.VMEM((tp,) + ln_gain.shape, f32),
            pltpu.VMEM((tp,) + ln_shift.shape, f32),
            pltpu.VMEM((window, width), bf),
            pltpu.VMEM((window, width), bf),
            pltpu.VMEM((lch // 128, window, 128), f32),
            pltpu.VMEM((layers, tp, most, lch), bf),
            pltpu.VMEM((tp, rows, lch), bf),
            pltpu.VMEM((most, chans), bf),
            pltpu.VMEM((rows, feats), bf),
            pltpu.VMEM((window, 128), f32),
            pltpu.VMEM((window, 128), f32),
            dma(3 * layers), dma(6), dma(2),
            dma(1), dma(2 * layers),
            dma(2 * (planes - 1)), dma(3 * layers * (planes - 1)),
            dma(layers + last), dma(layers + last * planes),
            *[dma(k) for _ in range(3) for k in (last, last * planes)],
            dma(3), dma(2 * tp),
            dma(3), dma(2 * tp), dma(1), dma(1), dma(1), dma(3), dma(1), dma(1),
            dma(2), dma(2), dma(2), dma(2),
            dma(last), dma(2 * last), dma(2 * last), dma(2 * last),
            dma(1), dma(6), dma(1), dma(2), dma(1), dma(1),
        ],
        compiler_params=pltpu.CompilerParams(
            collective_id=0, has_side_effects=True, vmem_limit_bytes=60 * 1024 * 1024),
    )(tokens, norm_gain, w_value, w_gate, w_out, conv_taps, conv_bias, ln_gain, ln_shift)


def fits(mesh, tokens, conv_taps, w_out):
    n, tp = mesh.shape["sp"], mesh.shape["tp"]
    layers, ntaps, lch = conv_taps.shape
    rows, feats = tokens.shape
    return (tp == 4 and n == 2 * tp and ntaps % 2 == 1 and ntaps // 2 < 16 and layers > 1
            and w_out.shape[2] % 128 == 0 and lch % 128 == 0 and feats % 128 == 0
            and feats == 2 * w_out.shape[2]
            and rows % 64 == 0 and rows >= 32 * layers and rows <= 512
            and layers * w_out.shape[1] * w_out.shape[2] * n * 12 <= 20 * 1024 * 1024)


def solution(mesh):
    placed = (
        P("sp", "tp"),
        P(),
        P(None, "sp", "tp"),
        P(None, "sp", "tp"),
        P(None, None, "tp"),
        P(None, "tp"),
        P(None, "tp"),
        P(None, "tp"),
        P(None, "tp", "sp"),
    )

    def run(*args):
        if fits(mesh, args[0], args[4], args[8]):
            return fused_call(mesh, *args)
        return body(*args)

    return jax.shard_map(run, mesh=mesh, in_specs=placed, out_specs=P("sp", "tp"), check_vma=False)
```

```python
import functools

import jax
import jax.numpy as jnp
from jax import lax
from jax.experimental import pallas as pl
from jax.experimental.pallas import tpu as pltpu
from jax.sharding import PartitionSpec as P

MESH = pl.DeviceIdType.MESH

norm_floor = 0.01


def with_halo(array, sides, width):
    for axis, dim in sides:
        size, length = (lax.axis_size(axis), array.shape[dim])
        up = [(i, (i + 1) % size) for i in range(size - 1)]
        down = [(j, i) for i, j in up]
        last = lax.slice_in_dim(array, length - width, length, axis=dim)
        first = lax.slice_in_dim(array, 0, width, axis=dim)
        before = lax.ppermute(last, axis, up)
        after = lax.ppermute(first, axis, down)
        array = jnp.concatenate([before, array, after], axis=dim)
    return array


def body(tokens, norm_gain, w_value, w_gate, conv_taps, conv_bias, ln_gain, ln_shift, w_out):
    stream = tokens
    layer_count = w_value.shape[0]
    reach = conv_taps.shape[1] // 2
    local_channels = w_value.shape[2]
    channels = local_channels * lax.axis_size("tp")
    tok_rows = tokens.shape[0]
    whole_value, whole_gate = (
        lax.all_gather(w_value, "sp", axis=1, tiled=True),
        lax.all_gather(w_gate, "sp", axis=1, tiled=True),
    )
    whole_out = lax.all_gather(w_out, "sp", axis=2, tiled=True)
    for layer_index in range(layer_count):
        whole_rows = lax.all_gather(stream, "tp", axis=1, tiled=True)
        rows_f32 = whole_rows.astype(jnp.float32)
        scale_rows = lax.rsqrt(jnp.mean(rows_f32 * rows_f32, axis=-1, keepdims=True) + norm_floor)
        normed = (rows_f32 * scale_rows * norm_gain[layer_index]).astype(jnp.bfloat16)
        value_rows = jnp.dot(normed, whole_value[layer_index], preferred_element_type=jnp.float32)
        gate_rows = jnp.dot(normed, whole_gate[layer_index], preferred_element_type=jnp.float32)
        gated_input = (value_rows * jax.nn.sigmoid(gate_rows)).astype(jnp.bfloat16)
        padded = with_halo(gated_input, (("sp", 0),), reach)
        padded = padded.astype(jnp.float32)
        convolved = jnp.zeros((tok_rows, local_channels), jnp.float32) + conv_bias[layer_index]
        for offset in range(2 * reach + 1):
            convolved = (
                convolved + conv_taps[layer_index, offset] * padded[offset : offset + tok_rows]
            )
        moments = lax.psum(
            (
                jnp.sum(convolved, axis=-1, keepdims=True),
                jnp.sum(convolved * convolved, axis=-1, keepdims=True),
            ),
            "tp",
        )
        average = moments[0] / channels
        spread = moments[1] / channels - average * average
        activated = jax.nn.silu(
            (convolved - average) * lax.rsqrt(spread + norm_floor) * ln_gain[layer_index]
            + ln_shift[layer_index]
        ).astype(jnp.bfloat16)
        partial_rows = jnp.dot(
            activated, whole_out[layer_index], preferred_element_type=jnp.float32
        )
        summed = lax.psum_scatter(
            partial_rows.astype(jnp.bfloat16), "tp", scatter_dimension=1, tiled=True
        ).astype(jnp.float32)
        stream = (stream.astype(jnp.float32) + summed).astype(jnp.bfloat16)
    return stream


def fused(
    dims,
    tok_in, gain_hbm, wv_in, wg_in, wo_in, taps_in, bias_in, lng_in, lns_in,
    out,
    tok, gain_in, result, wvg, wo, taps, bias, lng, lns, stream, normed, gated, cv, cv2, act, resid, rowa, rowb,
    loc_sem, in_sem, out_sem, pre_send, z_send, z_recv, d_send, d_recv,
    a_send, a_recv, b_send, b_recv, r_send, r_recv, o_send, o_recv,
    tok_send, tok_recv, zh_send, zh_recv, hp_send, hp_recv, ih_send, ih_recv,
    par_send, par_recv, ln_send, ln_recv,
    cv_send, ca_recv, cb_recv, cr_recv,
    l_send, l_recv, p_send, p_recv, res_send, res_recv,
):
    n, tp, layers, ntaps, rows, width, chans = dims
    planes = n // 2
    feats = width // tp
    lch = chans // tp
    krows = width // n
    ocols = width // n
    reach = ntaps // 2
    grain = 16
    halo = grain * layers
    window = rows + 2 * halo
    last = layers - 1
    lanes = 128
    per_side = lch // lanes
    per_out = feats // ocols

    sp = lax.axis_index("sp")
    t = lax.axis_index("tp")
    z, y = sp // 2, lax.rem(sp, 2)
    x, h = t // 2, lax.rem(t, 2)
    xn, yn, hn = 1 - x, 1 - y, 1 - h
    same = 1 - (y + h - 2 * y * h)
    spn = 2 * z + yn
    has_up, has_down = 1 - (z + 1) // planes, jnp.minimum(z, 1)

    partner = (sp, 2 * x + hn)
    xdev = (sp, 2 * xn + h)
    ydev = (spn, t)
    ax, ay = hn * xn + h * x, hn * y + h * yn
    bx, by = hn * x + h * xn, hn * yn + h * y
    adev = (2 * z + ay, 2 * ax + h)
    bdev = (2 * z + by, 2 * bx + h)

    def rcopy(src, dst, ssem, rsem, dev):
        return pltpu.make_async_remote_copy(
            src_ref=src, dst_ref=dst, send_sem=ssem, recv_sem=rsem,
            device_id=dev, device_id_type=MESH)

    def arrived(ref, ssem, rsem):
        rcopy(ref, ref, ssem, rsem, partner).wait_recv()

    def sent(ref, ssem):
        rcopy(ref, ref, ssem, ssem, partner).wait_send()

    def when(flag):
        return pl.when(flag == 1)

    def vblock(l, k, zs, c):
        r = pl.ds(pl.multiple_of((2 * zs + c) * krows, krows), krows)
        return wvg.at[l, k, r, :]

    def oblock(l, zs, yy, cb):
        r = pl.ds(pl.multiple_of(cb * lch, lch), lch)
        return wo.at[l, 2 * zs + yy, r, :]

    def item(l, k, zs):
        return vblock(l, k, zs, h) if k < 2 else oblock(l, zs, y, t)

    def local_copy(l, k):
        src = (wv_in, wg_in, wo_in)[k].at[l]
        return pltpu.make_async_copy(src, item(l, k, z), loc_sem.at[3 * l + k])

    def pre_copy(l, k):
        src = (wv_in, wg_in)[k].at[l]
        return rcopy(src, vblock(l, k, z, y), pre_send.at[0], loc_sem.at[3 * l + k], (spn, 2 * x + hn))

    def z_parts(l, k, d, s):
        zs = z - s if d == 0 else z + s
        return item(l, k, zs), z_recv.at[(l * 3 + k) * (planes - 1) + zs - d]

    def z_copy(l, k, d, s):
        ref, rsem = z_parts(l, k, d, s)
        return rcopy(ref, ref, z_send.at[d * (planes - 1) + s], rsem, (sp + (2 if d == 0 else -2), t))

    def z_wait(l, k, d, s):
        ref, rsem = z_parts(l, k, d, s)
        arrived(ref, z_send.at[0], rsem)

    def d_copy(l, k, zs, ref):
        i, j = (l, l) if k < 2 else (layers + l, layers + l * planes + zs)
        return rcopy(ref, ref, d_send.at[i], d_recv.at[j], partner)

    def a_copy(l, zs):
        ref = oblock(l, zs, y, t)
        return rcopy(ref, ref, a_send.at[l], a_recv.at[l * planes + zs], adev)

    def b_copy(l, zs):
        ref = oblock(l, zs, y, t)
        return rcopy(ref, ref, b_send.at[l], b_recv.at[l * planes + zs], bdev)

    def from_a(l, zs):
        return oblock(l, zs, ay, 2 * ax + h)

    def from_b(l, zs):
        return oblock(l, zs, by, 2 * bx + h)

    def r_copy(l, zs):
        ref = from_a(l, zs)
        return rcopy(ref, ref, r_send.at[l], r_recv.at[l * planes + zs], bdev)

    def o_copy(rel, zs):
        ref = oblock(last, zs, y, t)
        return rcopy(ref, ref, o_send.at[rel], o_recv.at[2 * t + rel],
                     (sp if rel == 0 else spn, zs))

    def differs(a, b):
        return jnp.minimum(jnp.abs(a - b), 1)

    def to_partner(l, k, zs):
        if k < 2 or l < last:
            d_copy(l, k, zs, item(l, k, zs)).start()

    def spread(l, s):
        for flag, zs in groups(s):
            def go(zs=zs):
                if l < last:
                    a_copy(l, zs).start()
                    b_copy(l, zs).start()
                else:
                    when(differs(zs, t))(lambda: o_copy(0, zs).start())
                    far = 1 if s == planes - 1 else 1 - differs(zs // 2, x)
                    when(far)(lambda: o_copy(1, zs).start())
            guarded(flag, go)

    def o_pass(c):
        owner = 2 * xn + c
        ref = oblock(last, t, y, owner)
        return rcopy(ref, ref, o_send.at[2], o_recv.at[2 * owner + 1], ydev)

    def o_relay(s):
        @when(1 - differs(jnp.abs(z - t), s))
        def _():
            for c in range(2):
                owner = 2 * xn + c
                arrived(oblock(last, t, y, owner), o_send.at[0], o_recv.at[2 * owner])
                if s < planes - 1:
                    o_pass(c).start()

    def own_start(l, k):
        if k < 2:
            when(same)(lambda: local_copy(l, k).wait())

            @when(1 - same)
            def _():
                arrived(item(l, k, z), pre_send.at[0], loc_sem.at[3 * l + k])
        else:
            local_copy(l, k).wait()
        when(has_up)(lambda: z_copy(l, k, 0, 0).start())
        when(has_down)(lambda: z_copy(l, k, 1, 0).start())
        to_partner(l, k, z)

    def below(s):
        return jnp.minimum(z // s, 1)

    def above(s):
        return jnp.minimum((planes - 1 - z) // s, 1)

    def groups(s):
        if s == 0:
            return [(None, z)]
        return [(below(s), z - s), (above(s), z + s)]

    def guarded(flag, f):
        if flag is None:
            f()
        else:
            when(flag)(f)

    def z_recv_step(l, k, s):
        for d, (flag, zs) in enumerate(groups(s)):
            def go(d=d, zs=zs):
                z_wait(l, k, d, s)
                if s < planes - 1:
                    when((has_up, has_down)[d])(lambda: z_copy(l, k, d, s).start())
                to_partner(l, k, zs)
            guarded(flag, go)

    def a_step(l, s):
        for flag, zs in groups(s):
            def go(zs=zs):
                ref = from_a(l, zs)
                arrived(ref, a_send.at[0], a_recv.at[l * planes + zs])
                r_copy(l, zs).start()
                d_copy(l, 2, zs, ref).start()
            guarded(flag, go)

    def b_step(l, s):
        for flag, zs in groups(s):
            def go(zs=zs):
                ref = from_b(l, zs)
                arrived(ref, b_send.at[0], b_recv.at[l * planes + zs])
                d_copy(l, 2, zs, ref).start()
            guarded(flag, go)

    def r_step(l, s):
        for flag, zs in groups(s):
            def go(zs=zs):
                ref = oblock(l, zs, yn, 2 * xn + h)
                arrived(ref, r_send.at[0], r_recv.at[l * planes + zs])
                d_copy(l, 2, zs, ref).start()
            guarded(flag, go)

    def v_half(l):
        return wvg.at[l, :, pl.ds(0, width // 2), :]

    def need_v(l):
        arrived(v_half(l), d_send.at[0], d_recv.at[l])

    def need_last():
        mate = 2 * x + hn
        arrived(oblock(last, t, y, mate), o_send.at[0], o_recv.at[2 * mate])
        for j in range(tp):
            other = lax.rem(t + j, tp)
            arrived(oblock(last, t, yn, other), o_send.at[0], o_recv.at[2 * other + 1])

    def v_sent():
        when(1 - same)(lambda: sent(wvg.at[:, :, pl.ds(0, krows), :], pre_send.at[0]))
        for l in range(layers):
            sent(v_half(l), d_send.at[l])
        for s in range(planes - 1):
            for d, flag in enumerate((has_up, has_down)):
                ok = flag if s == 0 else flag * (below(s), above(s))[d]
                ref = wvg.at[:, :, pl.ds(0, 3 * krows // 2), :]
                when(ok)(lambda d=d, s=s, ref=ref: sent(ref, z_send.at[d * (planes - 1) + s]))

    def o_sent():
        for l in range(last):
            sent(wo.at[l, pl.ds(0, planes)], d_send.at[layers + l])
            for sem in (a_send, b_send, r_send):
                sent(wo.at[l, 0], sem.at[l])

    def o_last_sent():
        def some(i, count):
            sent(wo.at[last, 0, pl.ds(0, count * lch), :], o_send.at[i])

        at_end = 1 - differs(jnp.abs(planes - 1 - 2 * z), planes - 1)
        extra = at_end * differs((planes - 1 - z) // 2, x)
        some(0, tp - 1)
        when(extra)(lambda: some(1, 3))
        when(1 - extra)(lambda: some(1, 2))
        when(differs(jnp.abs(z - t), planes - 1))(lambda: some(2, 2))

    def cols(owner):
        return pl.ds(pl.multiple_of(owner * feats, feats), feats)

    tcols = cols(t)

    half_rows = rows // 2

    def hcols(owner, part):
        return stream.at[pl.ds(halo + part * half_rows, half_rows), cols(owner)]

    def tok_copy(j, p):
        dev = ((sp, 2 * x + y), (sp, 2 * xn + y), (spn, 2 * x + y))[j]
        return rcopy(tok.at[pl.ds(p * half_rows, half_rows), :], hcols(t, p),
                     tok_send.at[min(j, 1)], tok_recv.at[2 * t + p], dev)

    def tok_start(j):
        tok_copy(j, 0).start()
        tok_copy(j, 1).start()

    def tok_pass(j):
        owner, p, dev = (
            (2 * xn + yn, 0, ydev), (2 * x + yn, 0, xdev),
            (2 * x + yn, 1, xdev), (2 * x + y, 1, xdev))[j]
        ref = hcols(owner, p)
        return rcopy(ref, ref, tok_send.at[2], tok_recv.at[2 * owner + p], dev)

    def tok_starts():
        when(1 - same)(lambda: tok_start(0))
        tok_start(1)

        @when(same)
        def _():
            stream[pl.ds(halo, rows), tcols] = tok[...]

    def tok_arrived(owner, p):
        arrived(hcols(owner, p), tok_send.at[0], tok_recv.at[2 * owner + p])

    def tok_relay(step):
        @when(same)
        def _():
            if step == 0:
                tok_arrived(2 * xn + yn, 0)
                tok_pass(0).start()

        @when(1 - same)
        def _():
            if step == 0:
                tok_arrived(2 * x + yn, 0)
                tok_pass(1).start()
            elif step == 1:
                tok_arrived(2 * x + yn, 1)
                tok_pass(2).start()
            else:
                tok_arrived(2 * x + y, 1)
                tok_pass(3).start()

    def tok_waits():
        @when(same)
        def _():
            tok_arrived(2 * xn + yn, 1)
            for p in range(2):
                tok_arrived(2 * x + hn, p)
                tok_arrived(2 * xn + y, p)

        @when(1 - same)
        def _():
            tok_arrived(2 * x + y, 0)
            for p in range(2):
                tok_arrived(2 * xn + yn, p)
                tok_arrived(2 * xn + y, p)

    zh_to = y * has_up + yn * has_down
    zh_from = hn * has_down + h * has_up

    def edge(owner_cols, side):
        r = pl.ds(pl.multiple_of(side * (halo + rows), grain), halo)
        return stream.at[r, owner_cols]

    def zh_copy():
        src = tok.at[pl.ds(pl.multiple_of(y * (rows - halo), grain), halo), :]
        return rcopy(src, edge(tcols, yn), zh_send.at[0], zh_recv.at[0],
                     (sp + 4 * y - 2, 2 * x + yn))

    def half_cols(xx):
        return pl.ds(pl.multiple_of(xx * 2 * feats, feats), 2 * feats)

    def hp_copy(j):
        ref = edge(half_cols(xn if j == 2 else x), h)
        return rcopy(ref, ref, hp_send.at[0], hp_recv.at[j], xdev if j == 0 else ydev)

    def halo_pass():
        @when(zh_from * (1 - same))
        def _():
            arrived(edge(half_cols(x), h), zh_send.at[0], zh_recv.at[0])
            hp_copy(0).start()
            hp_copy(1).start()

        @when(1 - zh_from)
        def _():
            stream[pl.ds(pl.multiple_of(h * (halo + rows), grain), halo), :] = jnp.zeros((halo, width), jnp.bfloat16)

    def halo_pass_on():
        @when(zh_from * (1 - same))
        def _():
            arrived(edge(half_cols(xn), h), hp_send.at[0], hp_recv.at[0])
            hp_copy(2).start()

    def halo_waits():
        @when(zh_from * same)
        def _():
            arrived(edge(half_cols(x), h), hp_send.at[0], hp_recv.at[1])
            arrived(edge(half_cols(xn), h), hp_send.at[0], hp_recv.at[2])

    def ih_copy():
        src = stream.at[pl.ds(pl.multiple_of(hn * rows + h * halo, grain), halo), :]
        dst = stream.at[pl.ds(pl.multiple_of(h * (halo + rows), grain), halo), :]
        return rcopy(src, dst, ih_send.at[0], ih_recv.at[0], partner)

    def ih_wait():
        ref = stream.at[pl.ds(pl.multiple_of(hn * (halo + rows), grain), halo), :]
        arrived(ref, ih_send.at[0], ih_recv.at[0])

    def par_copy(i):
        a, b = ((taps_in, taps), (bias_in, bias))[i]
        return rcopy(a, b, par_send.at[i], par_recv.at[i], partner)

    def ln_copy(i, j):
        a, b = ((lng_in, lng), (lns_in, lns))[i]
        return rcopy(a, b.at[t], ln_send.at[i], ln_recv.at[i],
                     (sp, lax.rem(t + j, tp)))

    def params_start():
        for i in range(2):
            when(same)(lambda i=i: par_copy(i).start())
            for j in range(1, tp):
                ln_copy(i, j).start()


    def in_copies():
        return [
            pltpu.make_async_copy(a, b, in_sem.at[i])
            for i, (a, b) in enumerate((
                (tok_in, tok), (gain_hbm, gain_in), (lng_in, lng.at[t]), (lns_in, lns.at[t]),
                (taps_in, taps), (bias_in, bias)))
        ]

    def in_start():
        for i, c in enumerate(in_copies()):
            if i < 4:
                c.start()
            else:
                when(same)(lambda c=c: c.start())

    def out_copy(i):
        r0, size = piece(last, i)
        r = pl.ds(r0, size)
        return pltpu.make_async_copy(result.at[r, :], out.at[r, :], out_sem.at[i])

    def params_wait():
        for i, c in enumerate(in_copies()):
            if i >= 4:
                when(same)(lambda c=c: c.wait())
            elif i > 0:
                c.wait()
        for i, ref in enumerate((taps, bias)):
            when(1 - same)(lambda i=i, ref=ref: arrived(ref, par_send.at[i], par_recv.at[i]))
        for i, ref in enumerate((lng, lns)):
            arrived(ref.at[pl.ds(0, tp - 1)], ln_send.at[0], ln_recv.at[i])

    def small_sent():
        when(1 - same)(lambda: sent(tok, tok_send.at[0]))
        sent(stream.at[pl.ds(0, rows), pl.ds(0, 2 * feats)], tok_send.at[1])
        when(zh_to)(lambda: zh_copy().wait_send())
        for i, ref in enumerate((lng, lns)):
            when(same)(lambda i=i: par_copy(i).wait_send())
            sent(ref.at[pl.ds(0, tp - 1)], ln_send.at[i])

    def stream_sent():
        for flag, count in ((same, 1), (1 - same, 3)):
            ref = stream.at[pl.ds(0, half_rows), pl.ds(0, count * feats)]
            when(flag)(lambda ref=ref: sent(ref, tok_send.at[2]))
        ref = stream.at[pl.ds(0, 3 * halo), pl.ds(0, 2 * feats)]
        when(zh_from * (1 - same))(lambda: sent(ref, hp_send.at[0]))
        ih_copy().wait_send()

    cb_own = 2 * x + y
    cb_a, cb_b, cb_d = 2 * ax + ay, 2 * bx + by, 2 * xn + yn

    def piece(l, i):
        total = window - 2 * grain * (l + 1)
        first = total - rows // 2
        return i * first, total - first if i else first

    def cblock(l, i, cb):
        r0, size = piece(l, i)
        return cv.at[l, cb, pl.ds(r0, size), :]

    def cv_copy(l, i, j):
        ref = cblock(l, i, cb_a if j == 2 else cb_own)
        r = (ca_recv, cb_recv, cr_recv)[j]
        return rcopy(ref, ref, cv_send.at[l], r.at[2 * l + i], adev if j == 0 else bdev)

    def cv_start(l, i):
        cv_copy(l, i, 0).start()
        cv_copy(l, i, 1).start()

    def cv_relay(l, i):
        arrived(cblock(l, i, cb_a), cv_send.at[0], ca_recv.at[2 * l + i])
        cv_copy(l, i, 2).start()

    def cv_waits(l, i):
        arrived(cblock(l, i, cb_b), cv_send.at[0], cb_recv.at[2 * l + i])
        arrived(cblock(l, i, cb_d), cv_send.at[0], cr_recv.at[2 * l + i])

    def lblock(i, cb):
        r0, size = piece(last, i)
        return cv2.at[cb, pl.ds(r0, size), :]

    def l_copy(i, j):
        src, cb, dev = (
            (cblock(last, i, cb_own), cb_own, ydev),
            (cblock(last, i, cb_own), cb_own, xdev),
            (lblock(i, 2 * x + yn), 2 * x + yn, xdev),
        )[j]
        return rcopy(src, lblock(i, cb), l_send.at[0], l_recv.at[3 * i + j], dev)

    def p_copy(i, j):
        cb = (cb_own, 2 * x + yn, 2 * xn + y, 2 * xn + yn)[j]
        src = cblock(last, i, cb) if j == 0 else lblock(i, cb)
        return rcopy(src, lblock(i, cb), p_send.at[0], p_recv.at[i], partner)

    def last_start(i):
        r0, size = piece(last, i)
        when(1 - same)(lambda: l_copy(i, 0).start())

        @when(same)
        def _():
            l_copy(i, 1).start()
            p_copy(i, 0).start()
            cv2[cb_own, r0:r0 + size, :] = cv[last, cb_own, r0:r0 + size, :]

    def last_relay(i):
        @when(same)
        def _():
            arrived(lblock(i, 2 * x + yn), l_send.at[0], l_recv.at[3 * i])
            l_copy(i, 2).start()
            p_copy(i, 1).start()

    def last_waits(i):
        @when(same)
        def _():
            for j in (1, 2):
                cb = 2 * xn + (y if j == 1 else yn)
                arrived(lblock(i, cb), l_send.at[0], l_recv.at[3 * i + j])
                p_copy(i, j + 1).start()

        r0, size = piece(last, i)
        when(1 - same)(lambda: arrived(cv2.at[:, pl.ds(r0, size), :], p_send.at[0], p_recv.at[i]))

    def conv_sent():
        for l in range(last):
            total = window - 2 * grain * (l + 1)
            sent(cv.at[l, pl.ds(0, 3), pl.ds(0, total), :], cv_send.at[l])

    def last_sent():
        when(1 - same)(lambda: sent(cv2.at[0], l_send.at[0]))

        @when(same)
        def _():
            sent(cv2.at[pl.ds(0, 2)], l_send.at[0])
            sent(cv2, p_send.at[0])

    def res_copy():
        src = stream.at[pl.ds(halo, rows), cols(2 * x + hn)]
        return rcopy(src, resid, res_send.at[0], res_recv.at[0], partner)

    def res_start():
        @when(same)
        def _():
            res_copy().start()
            resid[...] = stream[pl.ds(halo, rows), tcols]

    def res_wait():
        when(1 - same)(lambda: arrived(resid, res_send.at[0], res_recv.at[0]))

    first_row = (2 * z + h) * rows - halo
    total_rows = n * rows

    def over_rows(start, size, block, f):
        def step(i, carry):
            f(pl.ds(pl.multiple_of(start + i * block, grain), block))
            return carry

        lax.fori_loop(0, size // block, step, 0)

    def chunk(layer, i):
        r0, size = piece(layer - 1, i)
        return grain * layer + r0, size

    def normalize(layer, i):
        w0, size = chunk(layer, i)
        block = 2 * grain

        def squares(r):
            total = jnp.zeros((block, lanes), jnp.float32)
            for c in range(width // lanes):
                v = stream[r, c * lanes:(c + 1) * lanes].astype(jnp.float32)
                total = total + v * v
            rowa[r, :] = total

        def scaled(r):
            scale = rowa[r, :]
            for c in range(width // lanes):
                lane = slice(c * lanes, (c + 1) * lanes)
                v = stream[r, lane].astype(jnp.float32)
                normed[r, lane] = (v * scale * gain_in[layer:layer + 1, lane]).astype(jnp.bfloat16)

        over_rows(w0, size, block, squares)
        mean = jnp.sum(rowa[w0:w0 + size, :], axis=-1, keepdims=True) / width
        rowa[w0:w0 + size, :] = jnp.broadcast_to(lax.rsqrt(mean + norm_floor), (size, lanes))
        over_rows(w0, size, block, scaled)

    def project(layer, i):
        w0, size = chunk(layer, i)
        value = jnp.dot(normed[w0:w0 + size, :], wvg[layer, 0], preferred_element_type=jnp.float32)
        gate = jnp.dot(normed[w0:w0 + size, :], wvg[layer, 1], preferred_element_type=jnp.float32)
        g = (value * (0.5 + 0.5 * jnp.tanh(0.5 * gate))).astype(jnp.bfloat16).astype(jnp.float32)
        row = lax.broadcasted_iota(jnp.int32, (size, lch), 0) + (first_row + w0)
        g = jnp.where(jnp.logical_and(row >= 0, row < total_rows), g, 0.0)
        for b in range(per_side):
            gated[b, w0:w0 + size, :] = g[:, b * lanes:(b + 1) * lanes]

    def convolve(layer, i):
        r0, size = piece(layer, i)
        start = grain * (layer + 1)
        cut = -(-size // 2 // grain) * grain
        for c0, part in ((r0, cut), (r0 + cut, size - cut)):
            def lane_block(b, carry, c0=c0, part=part):
                lane = pl.ds(pl.multiple_of(b * lanes, lanes), lanes)
                total = jnp.zeros((part, lanes), jnp.float32) + bias[layer:layer + 1, lane]
                for k in range(ntaps):
                    first = start + c0 + k - reach
                    total = total + taps[layer, k:k + 1, lane] * gated[b, first:first + part, :]
                cv[layer, cb_own, c0:c0 + part, lane] = total.astype(jnp.bfloat16)
                return carry

            lax.fori_loop(0, per_side, lane_block, 0)

    def activate(layer, i):
        r0, size = piece(layer, i)
        block = 2 * grain if size % (2 * grain) == 0 else grain
        parts = [(b, c) for b in range(tp) for c in range(per_side)]

        def load(b, c, r):
            lane = slice(c * lanes, (c + 1) * lanes)
            return (cv[layer, b, r, lane] if layer < last else cv2[b, r, lane]).astype(jnp.float32)

        def sums(r):
            s1 = jnp.zeros((block, lanes), jnp.float32)
            s2 = jnp.zeros((block, lanes), jnp.float32)
            for b, c in parts:
                v = load(b, c, r)
                s1 = s1 + v
                s2 = s2 + v * v
            rowa[r, :] = s1
            rowb[r, :] = s2

        def apply(r):
            scale, shift = rowa[r, :], rowb[r, :]
            for b, c in parts:
                lane = slice(c * lanes, (c + 1) * lanes)
                u = (load(b, c, r) - shift) * scale
                u = 0.5 * (u * lng[b, layer:layer + 1, lane] + lns[b, layer:layer + 1, lane])
                act[r, b * lch + c * lanes:b * lch + (c + 1) * lanes] = (u + u * jnp.tanh(u)).astype(jnp.bfloat16)

        over_rows(r0, size, block, sums)
        rows_ = slice(r0, r0 + size)
        average = jnp.sum(rowa[rows_, :], axis=-1, keepdims=True) / chans
        spread_ = jnp.sum(rowb[rows_, :], axis=-1, keepdims=True) / chans - average * average
        rowa[rows_, :] = jnp.broadcast_to(lax.rsqrt(spread_ + norm_floor), (size, lanes))
        rowb[rows_, :] = jnp.broadcast_to(average, (size, lanes))
        over_rows(r0, size, block, apply)

    def expand_wait(layer, s):
        for flag, zs in groups(s):
            sem = d_recv.at[layers + layer * planes + zs]
            guarded(flag, lambda sem=sem: arrived(wo.at[layer, 0], d_send.at[0], sem))

    def expand(layer, s, pieces=(0, 1)):
        for flag, zs in groups(s):
            def go(zs=zs):
                def step(j, carry):
                    c = pl.ds(pl.multiple_of((2 * zs + j) * ocols, ocols), ocols)
                    for i in pieces:
                        r0, size = piece(layer, i)
                        w0 = grain * (layer + 1) + r0
                        add = jnp.dot(act[r0:r0 + size, :], wo[layer, 2 * zs + j], preferred_element_type=jnp.float32)
                        stream[w0:w0 + size, c] = (stream[w0:w0 + size, c].astype(jnp.float32) + add).astype(jnp.bfloat16)
                    return carry

                lax.fori_loop(0, 2, step, 0)
            guarded(flag, go)

    def finish(i):
        r0, size = piece(last, i)
        for j in range(per_out):
            c = slice(j * ocols, (j + 1) * ocols)
            add = jnp.dot(act[r0:r0 + size, :], wo[last, per_out * t + j], preferred_element_type=jnp.float32)
            result[r0:r0 + size, c] = (resid[r0:r0 + size, c].astype(jnp.float32) + add).astype(jnp.bfloat16)

    barrier = pltpu.get_barrier_semaphore()
    in_start()
    for l in range(layers):
        for k in range(3):
            if k < 2:
                when(same)(lambda l=l, k=k: local_copy(l, k).start())
            else:
                local_copy(l, k).start()
    for ds in range(2):
        for j in range(tp):
            if ds or j:
                pl.semaphore_signal(barrier, inc=1, device_id=((sp, spn)[ds], lax.rem(t + j, tp)), device_id_type=MESH)
    for flag, step in ((has_up, 2), (has_down, -2)):
        @when(flag)
        def _(step=step):
            for c in range(2):
                pl.semaphore_signal(barrier, inc=1, device_id=(sp + step, 2 * x + c), device_id_type=MESH)
    pl.semaphore_wait(barrier, 2 * tp - 1 + 2 * (has_up + has_down))
    in_copies()[0].wait()

    def pre_start(l):
        for k in range(2):
            when(1 - same)(lambda k=k: pre_copy(l, k).start())

    pre_start(0)
    when(zh_to)(lambda: zh_copy().start())
    tok_starts()
    halo_pass()
    when(1 - same)(lambda: tok_start(2))
    params_start()
    own_start(0, 0)
    own_start(0, 1)
    when(same)(lambda: own_start(0, 2))
    z_recv_step(0, 0, 1)
    when(same)(lambda: tok_start(2))
    z_recv_step(0, 1, 1)
    tok_relay(0)
    when(1 - same)(lambda: own_start(0, 2))
    halo_pass_on()
    tok_relay(1)
    z_recv_step(0, 0, 2)
    tok_relay(2)
    pre_start(1)
    z_recv_step(0, 1, 2)
    spread(0, 0)
    z_recv_step(0, 2, 1)
    tok_waits()
    ih_copy().start()

    def first_weights_in():
        z_recv_step(0, 0, 3)
        z_recv_step(0, 1, 3)

    when(same)(first_weights_in)
    halo_waits()
    ih_wait()
    params_wait()
    normalize(0, 0)
    normalize(0, 1)
    when(1 - same)(first_weights_in)
    own_start(1, 0)
    own_start(1, 1)
    spread(0, 1)
    need_v(0)
    for i in range(2):
        project(0, i)
        convolve(0, i)
        cv_start(0, i)
        if i == 0:
            a_step(0, 0)
            z_recv_step(0, 2, 2)

    def layer_end(layer, between):
        after = layer + 1
        expand_wait(layer, 3)
        for i in range(2):
            expand(layer, 3, (i,))
            normalize(after, i)
            project(after, i)
            convolve(after, i)
            if after < last:
                cv_start(after, i)
            else:
                last_start(i)
            if i == 0:
                between()

    for layer in range(last - 1):
        after = layer + 1
        beyond = layer + 2
        z_recv_step(after, 0, 1)
        cv_relay(layer, 0)
        z_recv_step(after, 1, 1)
        cv_relay(layer, 1)
        spread(layer, 2)
        z_recv_step(layer, 2, 3)
        spread(layer, 3)
        z_recv_step(after, 0, 2)
        b_step(layer, 0)
        a_step(layer, 1)
        cv_waits(layer, 0)
        activate(layer, 0)
        z_recv_step(after, 1, 2)
        own_start(after, 2)
        if layer == 0:
            pre_start(2)
        cv_waits(layer, 1)
        activate(layer, 1)
        r_step(layer, 0)
        a_step(layer, 2)
        if layer == 0:
            stream_sent()
        expand_wait(layer, 0)
        expand(layer, 0)
        z_recv_step(after, 0, 3)
        b_step(layer, 1)
        a_step(layer, 3)
        z_recv_step(after, 1, 3)
        r_step(layer, 1)
        spread(after, 0)
        z_recv_step(after, 2, 1)
        own_start(beyond, 2)
        own_start(beyond, 0)
        own_start(beyond, 1)
        expand_wait(layer, 1)
        expand(layer, 1)
        b_step(layer, 2)
        r_step(layer, 2)
        expand_wait(layer, 2)
        expand(layer, 2)
        b_step(layer, 3)
        need_v(after)
        r_step(layer, 3)
        spread(after, 1)
        layer_end(layer, lambda: z_recv_step(after, 2, 2))
        a_step(after, 0)

    layer = last - 1
    z_recv_step(layer, 2, 3)
    z_recv_step(last, 2, 1)
    cv_relay(layer, 0)
    z_recv_step(last, 0, 1)
    cv_relay(layer, 1)
    spread(layer, 2)
    spread(layer, 3)
    z_recv_step(last, 2, 2)
    b_step(layer, 0)
    a_step(layer, 1)
    z_recv_step(last, 1, 1)
    cv_waits(layer, 0)
    activate(layer, 0)
    z_recv_step(last, 0, 2)
    cv_waits(layer, 1)
    activate(layer, 1)
    r_step(layer, 0)
    a_step(layer, 2)
    z_recv_step(last, 2, 3)
    expand_wait(layer, 0)
    expand(layer, 0)
    z_recv_step(last, 1, 2)
    b_step(layer, 1)
    a_step(layer, 3)
    r_step(layer, 1)
    spread(last, 0)
    spread(last, 1)
    spread(last, 2)
    spread(last, 3)
    z_recv_step(last, 0, 3)
    expand_wait(layer, 1)
    expand(layer, 1)
    b_step(layer, 2)
    r_step(layer, 2)
    z_recv_step(last, 1, 3)
    o_relay(0)
    expand_wait(layer, 2)
    expand(layer, 2)
    b_step(layer, 3)
    need_v(last)
    o_relay(1)
    r_step(layer, 3)
    layer_end(layer, lambda: None)
    res_start()
    o_relay(2)
    last_relay(0)
    last_relay(1)
    res_wait()
    o_sent()
    small_sent()
    conv_sent()
    last_waits(0)
    activate(last, 0)
    last_waits(1)
    o_relay(3)
    need_last()
    finish(0)
    out_copy(0).start()
    activate(last, 1)
    finish(1)
    out_copy(1).start()
    v_sent()
    o_last_sent()
    last_sent()
    when(same)(lambda: res_copy().wait_send())
    for i in range(2):
        out_copy(i).wait()


def fused_call(mesh, *args):
    tokens, norm_gain, w_value, w_gate, conv_taps, conv_bias, ln_gain, ln_shift, w_out = args
    n, tp = mesh.shape["sp"], mesh.shape["tp"]
    layers, ntaps, lch = conv_taps.shape
    rows, feats = tokens.shape
    width, chans = feats * tp, lch * tp
    planes = n // 2
    last = layers - 1
    halo = 16 * layers
    window = rows + 2 * halo
    most = window - 32
    dims = (n, tp, layers, ntaps, rows, width, chans)
    anys = pl.BlockSpec(memory_space=pl.ANY)
    bf, f32 = jnp.bfloat16, jnp.float32
    dma = lambda k: pltpu.SemaphoreType.DMA((k,))
    return pl.pallas_call(
        functools.partial(fused, dims),
        out_shape=jax.ShapeDtypeStruct((rows, feats), bf),
        in_specs=[anys] * 9,
        out_specs=anys,
        scratch_shapes=[
            pltpu.VMEM((rows, feats), bf),
            pltpu.VMEM(norm_gain.shape, f32),
            pltpu.VMEM((rows, feats), bf),
            pltpu.VMEM((layers, 2, width, lch), bf),
            pltpu.VMEM((layers, n, chans, width // n), bf),
            pltpu.VMEM(conv_taps.shape, f32),
            pltpu.VMEM(conv_bias.shape, f32),
            pltpu.VMEM((tp,) + ln_gain.shape, f32),
            pltpu.VMEM((tp,) + ln_shift.shape, f32),
            pltpu.VMEM((window, width), bf),
            pltpu.VMEM((window, width), bf),
            pltpu.VMEM((lch // 128, window, 128), f32),
            pltpu.VMEM((layers, tp, most, lch), bf),
            pltpu.VMEM((tp, rows, lch), bf),
            pltpu.VMEM((most, chans), bf),
            pltpu.VMEM((rows, feats), bf),
            pltpu.VMEM((window, 128), f32),
            pltpu.VMEM((window, 128), f32),
            dma(3 * layers), dma(6), dma(2),
            dma(1),
            dma(2 * (planes - 1)), dma(3 * layers * (planes - 1)),
            dma(layers + last), dma(layers + last * planes),
            *[dma(k) for _ in range(3) for k in (last, last * planes)],
            dma(3), dma(2 * tp),
            dma(3), dma(2 * tp), dma(1), dma(1), dma(1), dma(3), dma(1), dma(1),
            dma(2), dma(2), dma(2), dma(2),
            dma(last), dma(2 * last), dma(2 * last), dma(2 * last),
            dma(1), dma(6), dma(1), dma(2), dma(1), dma(1),
        ],
        compiler_params=pltpu.CompilerParams(
            collective_id=0, has_side_effects=True, vmem_limit_bytes=60 * 1024 * 1024),
    )(tokens, norm_gain, w_value, w_gate, w_out, conv_taps, conv_bias, ln_gain, ln_shift)


def fits(mesh, tokens, conv_taps, w_out):
    n, tp = mesh.shape["sp"], mesh.shape["tp"]
    layers, ntaps, lch = conv_taps.shape
    rows, feats = tokens.shape
    return (tp == 4 and n == 2 * tp and ntaps % 2 == 1 and ntaps // 2 < 16 and layers > 1
            and w_out.shape[2] % 128 == 0 and lch % 128 == 0 and feats % 128 == 0
            and feats == 2 * w_out.shape[2]
            and rows % 64 == 0 and rows >= 32 * layers and rows <= 512
            and layers * w_out.shape[1] * w_out.shape[2] * n * 12 <= 20 * 1024 * 1024)


def solution(mesh):
    placed = (
        P("sp", "tp"),
        P(),
        P(None, "sp", "tp"),
        P(None, "sp", "tp"),
        P(None, None, "tp"),
        P(None, "tp"),
        P(None, "tp"),
        P(None, "tp"),
        P(None, "tp", "sp"),
    )

    def run(*args):
        if fits(mesh, args[0], args[4], args[8]):
            return fused_call(mesh, *args)
        return body(*args)

    return jax.shard_map(run, mesh=mesh, in_specs=placed, out_specs=P("sp", "tp"), check_vma=False)
```
